32 devices in a mesh: sp: 4 (over x, core), tp: 8 (over z, y).
Axes of the slice: x: 2, y: 2, z: 4, core: 2. Of those that a mesh axis runs over, the one named last changes fastest.
Arguments:
- latent: bfloat16 [512, 4096], P('sp', 'tp'), may hold values from -60 to 60
- context: bfloat16 [64, 4096], P('sp', 'tp'), may hold values from -6 to 6
- conditioning: bfloat16 [4096], P('sp'), may hold values from -6 to 6
- context_prompt_vector: bfloat16 [4096], P('sp'), may hold values from -6 to 6
- shift_matrix: bfloat16 [4096, 4096], P('tp', 'sp'), may hold values from -0.09375 to 0.09375
- scale_matrix: bfloat16 [4096, 4096], P('tp', 'sp'), may hold values from -0.09375 to 0.09375
- residual_gate_matrix: bfloat16 [4096, 4096], P('tp', 'sp'), may hold values from -0.09375 to 0.09375
- query_matrix: bfloat16 [2048, 4096], P('tp'), may hold values from -0.09375 to 0.09375
- key_matrix: bfloat16 [2048, 4096], P('tp'), may hold values from -0.09375 to 0.09375
- value_matrix: bfloat16 [4096, 4096], P('tp'), may hold values from -0.09375 to 0.09375
- gate_matrix: bfloat16 [4096, 4096], P('tp'), may hold values from -0.09375 to 0.09375
- decay_down_factor: bfloat16 [2, 4096, 16], replicated, may hold values from -0.09375 to 0.09375
- decay_up_factor: bfloat16 [2, 16, 2048], replicated, may hold values from -1.5 to 1.5
- decay_key_bias: float32 [2, 2048], replicated, may hold values from -0.5 to 7
- spike_log_decay: float32 [2, 512, 16], P(None, 'sp'), may hold values from -2.8 to 0
- output_gain: float32 [4096], P('tp'), may hold values from 0.1 to 1.9
- output_matrix: bfloat16 [4096, 4096], P('tp'), may hold values from -0.375 to 0.375
Outputs:
- mixed: bfloat16 [512, 4096], P('sp', 'tp')
The draws below stay inside these ranges and needn't reach their ends.
All inputs are finite; a program needn't handle non-finite values.
Results may differ from the reference program's by a relative error of at most 0.013.
Values may be sent and summed in bfloat16 or wider, within the bound.
A program may use at most 64 MiB of HBM per device.

```python
import math
import jax
import jax.numpy as jnp
from jax import lax

D = 4096
HEADS = 16
DK = 128
DV = 256
DECAY_RANK = 16
BLK = 64
VGROUP = 64
SEQ = 512
CTX = 64


def draw_latent(key, part):
    key_one, key_two = jax.random.split(key, 2)
    normal_part = jnp.clip(jax.random.normal(key_one, (SEQ, D), jnp.float32), -5.0, 5.0)
    column_rise = jnp.exp(jnp.linspace(math.log(0.6), math.log(2.0), D))
    jitter = jax.random.uniform(key_two, (1, D), jnp.float32, 0.7, 1.4)
    return (normal_part * column_rise * jitter).astype(jnp.bfloat16)


def draw_decay_key_bias(key, part):
    key_one, key_two, key_three = jax.random.split(key, 3)
    fast_share = 0.5
    fast_heads = jax.random.bernoulli(key_one, fast_share, (2, HEADS, 1))
    fast_rates = jax.random.uniform(key_two, (2, HEADS, DK), jnp.float32, -0.5, 1.5)
    slow_rates = jax.random.uniform(key_three, (2, HEADS, DK), jnp.float32, 5.0, 7.0)
    return jnp.where(fast_heads, fast_rates, slow_rates).reshape(2, HEADS * DK)


def draw_spike_log_decay(key, part):
    key_one, key_two = jax.random.split(key, 2)
    spots = jax.random.randint(key_one, (2, HEADS, 4), 0, SEQ)
    depths = jnp.log(jax.random.uniform(key_two, (2, HEADS, 4), jnp.float32, 0.5, 0.8))
    positions = jnp.arange(SEQ, dtype=jnp.int32)
    hits = (positions[None, None, None, :] == spots[:, :, :, None]).astype(jnp.float32)
    summed = jnp.sum(hits * depths[:, :, :, None], axis=2)
    return jnp.transpose(summed, (0, 2, 1))


def level_of(rng, dims, cuts, least, top_value):
    factor_of, own = 1.0, jax.random.fold_in(rng, 6)
    for position, blocks in cuts:
        heights = jnp.exp(jax.random.uniform(jax.random.fold_in(own, position), (blocks,), jnp.float32, least / len(cuts), top_value / len(cuts)))
        factor_of = factor_of * jnp.repeat(heights, dims[position] // blocks).reshape([-1 if axis == position else 1 for axis in range(len(dims))])
    return factor_of


def centred(own_key, shape, deviation, reach, shards=(), held_as=jnp.bfloat16):
    entries = jax.random.normal(own_key, shape, jnp.float32) * deviation
    if len(shards) > 0:
        entries = level_of(own_key, shape, shards, -0.22, 0.18) * entries
    return jnp.clip(entries, min=-reach, max=reach).astype(held_as)


def setup_inputs(seed: int = 0) -> dict:
    splits = jax.random.split(jax.random.key(seed), 18)
    latent = draw_latent(jax.random.fold_in(splits[17], 71), 0)
    context = centred(splits[1], (CTX, D), 1.0, 6.0, ((0, 4), (1, 8)))
    conditioning = centred(splits[2], (D,), 1.0, 6.0, ((0, 4),))
    context_prompt_vector = centred(splits[3], (D,), 1.0, 6.0, ((0, 4),))
    shift_matrix = centred(splits[4], (D, D), D ** -0.5, 0.09375, ((0, 8), (1, 4)))
    scale_matrix = centred(splits[5], (D, D), D ** -0.5, 0.09375, ((0, 8), (1, 4)))
    residual_gate_matrix = centred(splits[6], (D, D), D ** -0.5, 0.09375, ((0, 8), (1, 4)))
    query_matrix = centred(splits[7], (HEADS * DK, D), D ** -0.5, 0.09375, ((0, 8),))
    key_matrix = centred(splits[8], (HEADS * DK, D), D ** -0.5, 0.09375, ((0, 8),))
    value_matrix = centred(splits[9], (HEADS * DV, D), D ** -0.5, 0.09375, ((0, 8),))
    gate_matrix = centred(splits[10], (HEADS * DV, D), D ** -0.5, 0.09375, ((0, 8),))
    decay_down_factor = centred(splits[11], (2, D, DECAY_RANK), D ** -0.5, 0.09375)
    decay_up_factor = centred(splits[12], (2, DECAY_RANK, HEADS * DK), DECAY_RANK ** -0.5, 1.5)
    decay_key_bias = draw_decay_key_bias(jax.random.fold_in(splits[17], 71), 0)
    spike_log_decay = draw_spike_log_decay(jax.random.fold_in(splits[17], 71), 0)
    output_gain = jnp.clip(1.0 + 0.18 * jax.random.normal(splits[15], (HEADS * DV,), jnp.float32), 0.1, 1.9)
    output_matrix = centred(splits[16], (D, HEADS * DV), (HEADS * DV // 16) ** -0.5, 0.375, ((0, 8),))
    return {"latent": latent, "context": context, "conditioning": conditioning, "context_prompt_vector": context_prompt_vector, "shift_matrix": shift_matrix, "scale_matrix": scale_matrix, "residual_gate_matrix": residual_gate_matrix, "query_matrix": query_matrix, "key_matrix": key_matrix, "value_matrix": value_matrix, "gate_matrix": gate_matrix, "decay_down_factor": decay_down_factor, "decay_up_factor": decay_up_factor, "decay_key_bias": decay_key_bias, "spike_log_decay": spike_log_decay, "output_gain": output_gain, "output_matrix": output_matrix}


epsilon = 1e-05
gate_norm = 16.0
precise = lax.Precision.HIGHEST

def linear(rows, weight):
    return lax.dot_general(rows, weight, (((1,), (1,)), ((), ())), preferred_element_type=jnp.float32)

def modulated(rows, shift_vec, scale_vec):
    rows_f = rows.astype(jnp.float32)
    mean_val = lax.optimization_barrier(jnp.mean(rows_f, axis=-1, keepdims=True))
    variance = lax.optimization_barrier(jnp.mean(rows_f * rows_f, axis=-1, keepdims=True)) - mean_val * mean_val
    return ((rows_f - mean_val) * lax.rsqrt(variance + epsilon) * (1.0 + scale_vec) + shift_vec).astype(jnp.bfloat16)

def reverse_rows(array):
    return jnp.flip(array, axis=0)

def end_state(key_rows, value_rows, log_decay):
    cumulative = jnp.cumsum(log_decay, axis=0)
    totals = cumulative[-1]
    weighted = key_rows * jnp.exp(totals - cumulative)
    return (jnp.exp(totals), jnp.einsum('nhd,nhe->hde', weighted, value_rows, precision=precise))

def blockwise(queries, key_rows, value_rows, log_decay, carried, block_len):
    length, head_count, _ = queries.shape
    value_width = value_rows.shape[-1]
    blocks = length // block_len

    def shaped(array):
        return array.reshape(blocks, block_len, head_count, array.shape[-1])
    triangle = jnp.tril(jnp.ones((block_len, block_len), jnp.float32))

    def advance(state_now, inputs):
        block_q, block_k, block_v, block_a = inputs
        cumulative = jnp.cumsum(block_a, axis=0)
        block_end = cumulative[-1]
        query_dec = block_q * jnp.exp(cumulative)
        scores = jnp.einsum('ihd,jhd->hij', query_dec, block_k * jnp.exp(-cumulative), precision=precise) * triangle
        result = jnp.einsum('hij,jhe->ihe', scores, block_v, precision=precise)
        result = result + jnp.einsum('ihd,hde->ihe', query_dec, state_now, precision=precise)
        state_next = state_now * jnp.exp(block_end)[:, :, None] + jnp.einsum('jhd,jhe->hde', block_k * jnp.exp(block_end - cumulative), block_v, precision=precise)
        return (state_next, result)
    _, outputs = lax.scan(advance, carried, (shaped(queries), shaped(key_rows), shaped(value_rows), shaped(log_decay)))
    return outputs.reshape(length, head_count, value_width)

def reference(latent, context, conditioning, context_prompt_vector, shift_matrix, scale_matrix, residual_gate_matrix, query_matrix, key_matrix, value_matrix, gate_matrix, decay_down_factor, decay_up_factor, decay_key_bias, spike_log_decay, output_gain, output_matrix):
    conds = jax.nn.silu(jnp.stack([conditioning, context_prompt_vector]).astype(jnp.float32)).astype(jnp.bfloat16)
    shifts = linear(conds, shift_matrix)
    scales = linear(conds, scale_matrix)
    gates = linear(conds, residual_gate_matrix)
    latent_normalized = modulated(latent, shifts[0], scales[0])
    normed_ctx = modulated(context, shifts[1], scales[1])

    def project(rows, weight):
        stored = lax.optimization_barrier(linear(rows, weight).astype(jnp.bfloat16))
        return stored.astype(jnp.float32)

    def split_heads(rows, width):
        return rows.reshape(rows.shape[0], HEADS, width)
    queries = split_heads(project(latent_normalized, query_matrix), DK) * DK ** (-0.5)
    key_rows = split_heads(project(latent_normalized, key_matrix), DK)
    value_rows = split_heads(project(latent_normalized, value_matrix), DV)
    gate_rows = project(latent_normalized, gate_matrix)
    ctx_keys = split_heads(project(normed_ctx, key_matrix), DK)
    ctx_values = split_heads(project(normed_ctx, value_matrix), DV)

    def per_head_decay(rows, direction):
        low_rows = jnp.dot(rows, decay_down_factor[direction], preferred_element_type=jnp.float32)
        pre_act = jnp.dot(low_rows, decay_up_factor[direction].astype(jnp.float32), precision=precise) + decay_key_bias[direction]
        return split_heads(jax.nn.log_sigmoid(pre_act) / gate_norm, DK)
    latent_forward = per_head_decay(latent_normalized, 0) + spike_log_decay[0][:, :, None]
    latent_backward = per_head_decay(latent_normalized, 1) + spike_log_decay[1][:, :, None]
    ctx_fwd = per_head_decay(normed_ctx, 0)
    ctx_bwd = per_head_decay(normed_ctx, 1)
    start_fwd = end_state(ctx_keys, ctx_values, ctx_fwd)[1]
    start_bwd = end_state(reverse_rows(ctx_keys), reverse_rows(ctx_values), reverse_rows(ctx_bwd))[1]
    out_fwd = blockwise(queries, key_rows, value_rows, latent_forward, start_fwd, BLK)
    out_bwd = reverse_rows(blockwise(reverse_rows(queries), reverse_rows(key_rows), reverse_rows(value_rows), reverse_rows(latent_backward), start_bwd, BLK))
    grouped = (out_fwd + out_bwd).reshape(SEQ, HEADS * DV // VGROUP, VGROUP)
    grouped = grouped * lax.rsqrt(lax.optimization_barrier(jnp.mean(grouped * grouped, axis=-1, keepdims=True)) + epsilon)
    heads_out = (grouped.reshape(SEQ, HEADS * DV) * output_gain * jax.nn.silu(gate_rows)).astype(jnp.bfloat16)
    branch = linear(heads_out, output_matrix)
    return (latent.astype(jnp.float32) + gates[0] * branch).astype(jnp.bfloat16)
```

```python
import functools
import math

import jax
import jax.numpy as jnp
from jax import lax
from jax.experimental import pallas as pl
from jax.experimental.pallas import tpu as pltpu
from jax.sharding import PartitionSpec as P

D = 4096
HEADS = 16
DK = 128
DECAY_RANK = 16
BLK = 64
VGROUP = 64
MESH = pl.DeviceIdType.MESH


epsilon = 1e-05
gate_norm = 16.0
precise = lax.Precision.HIGHEST


def for_sending(value):

    def short(part):
        return part.astype(jnp.bfloat16) if part.dtype == jnp.float32 else part

    return jax.tree.map(short, value)


def from_partner(value, axis, distance):
    return lax.ppermute(value, axis, [(i, i ^ 1 << distance) for i in range(lax.axis_size(axis))])


def carried_in(value, axis, combine, identity, reverse):
    peers, index = (lax.axis_size(axis), lax.axis_index(axis))
    everything = jax.tree.map(
        lambda part, kind: lax.all_gather(part.astype(kind), axis),
        value,
        (jnp.bfloat16, jnp.bfloat16),
    )
    start = jax.tree.map(
        lambda part, zero: jnp.broadcast_to(jnp.asarray(zero, part.dtype), part.shape),
        value,
        identity,
    )

    def turn(k, before):
        at = peers - 1 - k if reverse else k
        reached = at > index if reverse else at < index
        new = combine(
            before, jax.tree.map(lambda part, own: part[at].astype(own.dtype), everything, value)
        )
        return jax.tree.map(lambda a, b: jnp.where(reached, a, b), new, before)

    return lax.fori_loop(0, peers, turn, start)


def linear(rows, weight):
    return lax.dot_general(
        rows, weight, (((1,), (1,)), ((), ())), preferred_element_type=jnp.float32
    )


def modulated(rows, row_sum, row_squares, shift_vec, scale_vec):
    rows_f = rows.astype(jnp.float32)
    mean_val = row_sum / D
    variance = row_squares / D - mean_val * mean_val
    return (
        (rows_f - mean_val) * lax.rsqrt(variance + epsilon) * (1.0 + scale_vec) + shift_vec
    ).astype(jnp.bfloat16)


def reverse_rows(array):
    return jnp.flip(array, axis=0)


def end_state(key_rows, value_rows, log_decay):
    cumulative = jnp.cumsum(log_decay, axis=0)
    totals = cumulative[-1]
    weighted = key_rows * jnp.exp(totals - cumulative)
    return (jnp.exp(totals), jnp.einsum("nhd,nhe->hde", weighted, value_rows, precision=precise))


def combine(earlier, later):
    return (earlier[0] * later[0], later[0][..., None] * earlier[1] + later[1])


def blockwise(queries, key_rows, value_rows, log_decay, carried, block_len):
    length, head_count, _ = queries.shape
    value_width = value_rows.shape[-1]
    blocks = length // block_len

    def shaped(array):
        return array.reshape(blocks, block_len, head_count, array.shape[-1])

    triangle = jnp.tril(jnp.ones((block_len, block_len), jnp.float32))

    def advance(state_now, inputs):
        block_q, block_k, block_v, block_a = inputs
        cumulative = jnp.cumsum(block_a, axis=0)
        block_end = cumulative[-1]
        query_dec = block_q * jnp.exp(cumulative)
        scores = (
            jnp.einsum("ihd,jhd->hij", query_dec, block_k * jnp.exp(-cumulative), precision=precise)
            * triangle
        )
        result = jnp.einsum("hij,jhe->ihe", scores, block_v, precision=precise)
        result = result + jnp.einsum("ihd,hde->ihe", query_dec, state_now, precision=precise)
        state_next = state_now * jnp.exp(block_end)[:, :, None] + jnp.einsum(
            "jhd,jhe->hde", block_k * jnp.exp(block_end - cumulative), block_v, precision=precise
        )
        return (state_next, result)

    _, outputs = lax.scan(
        advance, carried, (shaped(queries), shaped(key_rows), shaped(value_rows), shaped(log_decay))
    )
    return outputs.reshape(length, head_count, value_width)


def head_channels(pieces, per_head, tp_index):
    for bit_number in range(per_head.bit_length() - 1):
        partner = from_partner(
            (for_sending(pieces[0]), for_sending(pieces[1]), for_sending(pieces[2])),
            "tp",
            bit_number,
        )
        upper = tp_index // (1 << bit_number) % 2 == 1
        pieces = tuple(
            (
                jnp.where(
                    upper,
                    jnp.concatenate([theirs, mine], axis=1),
                    jnp.concatenate([mine, theirs], axis=1),
                )
                for mine, theirs in zip(pieces, partner)
            )
        )
    return pieces


def context_totals(fwd_growth, fwd_state, bwd_growth, bwd_state, identity):

    def absorb(carried, piece):
        return (combine(carried, piece), None)

    total_fwd, _ = lax.scan(absorb, identity, (fwd_growth, fwd_state))
    total_bwd, _ = lax.scan(absorb, identity, (bwd_growth, bwd_state), reverse=True)
    return (total_fwd, total_bwd)


def stored(array):
    return lax.optimization_barrier(array.astype(jnp.bfloat16))


def local(
    latent,
    context,
    conditioning,
    context_prompt_vector,
    shift_matrix,
    scale_matrix,
    residual_gate_matrix,
    query_matrix,
    key_matrix,
    value_matrix,
    gate_matrix,
    decay_down_factor,
    decay_up_factor,
    decay_key_bias,
    spike_log_decay,
    output_gain,
    output_matrix,
):
    tp_count = lax.axis_size("tp")
    tp_index = lax.axis_index("tp")
    per_head = max(tp_count // HEADS, 1)
    heads_per_shard = max(HEADS // tp_count, 1)
    leading_head = tp_index // per_head * heads_per_shard
    tok_rows = latent.shape[0]
    conds = jax.nn.silu(
        jnp.stack([conditioning, context_prompt_vector]).astype(jnp.float32)
    ).astype(jnp.bfloat16)
    shifts, scales, gates = lax.psum(
        (
            linear(conds, shift_matrix),
            linear(conds, scale_matrix),
            linear(conds, residual_gate_matrix),
        ),
        "sp",
    )
    down_both = jnp.concatenate([decay_down_factor[0].T, decay_down_factor[1].T], axis=0)
    lat_weights = (query_matrix, key_matrix, value_matrix, gate_matrix, down_both)
    ctx_weights = (key_matrix, value_matrix, down_both)
    lat_f = latent.astype(jnp.float32)
    ctx_f = context.astype(jnp.float32)
    lat_sum, lat_squares, ctx_sum, ctx_squares = lax.psum(
        (
            jnp.sum(lat_f, axis=1, keepdims=True),
            jnp.sum(lat_f * lat_f, axis=1, keepdims=True),
            jnp.sum(ctx_f, axis=1, keepdims=True),
            jnp.sum(ctx_f * ctx_f, axis=1, keepdims=True),
        ),
        "tp",
    )
    latent_normalized = modulated(latent, lat_sum, lat_squares, shifts[0], scales[0])
    normed_ctx = modulated(context, ctx_sum, ctx_squares, shifts[1], scales[1])
    lat_piece = lax.all_gather(latent_normalized, "tp", axis=1, tiled=True)
    ctx_piece = lax.all_gather(normed_ctx, "tp", axis=1, tiled=True)
    lat_new = tuple((linear(lat_piece, weight) for weight in lat_weights))
    ctx_new = tuple((linear(ctx_piece, weight) for weight in ctx_weights))
    query_part, key_part, value_part, gate_part, low_rank_part = lat_new
    ctx_key_part, ctx_value_part, ctx_low = ctx_new
    query_full, key_full, ctx_key_full = head_channels(
        (stored(query_part), stored(key_part), stored(ctx_key_part)), per_head, tp_index
    )

    def split_heads(rows, width):
        return rows.astype(jnp.float32).reshape(rows.shape[0], heads_per_shard, width)

    value_cols = value_part.shape[1] // heads_per_shard
    queries = split_heads(query_full, DK) * DK ** (-0.5)
    key_rows = split_heads(key_full, DK)
    ctx_keys = split_heads(ctx_key_full, DK)
    values_lat = split_heads(stored(value_part), value_cols)
    values_ctx = split_heads(stored(ctx_value_part), value_cols)
    gate_rows = stored(gate_part).astype(jnp.float32)

    def per_head_decay(low_rows, direction):
        up_part = lax.dynamic_slice_in_dim(
            decay_up_factor[direction], leading_head * DK, heads_per_shard * DK, 1
        ).astype(jnp.float32)
        bias_part = lax.dynamic_slice_in_dim(
            decay_key_bias[direction], leading_head * DK, heads_per_shard * DK, 0
        )
        pre_act = jnp.dot(low_rows, up_part, precision=precise) + bias_part
        return (jax.nn.log_sigmoid(pre_act) / gate_norm).reshape(
            low_rows.shape[0], heads_per_shard, DK
        )

    decay_spikes = lax.dynamic_slice_in_dim(spike_log_decay, leading_head, heads_per_shard, 2)
    latent_forward = per_head_decay(low_rank_part[:, :DECAY_RANK], 0) + decay_spikes[0][:, :, None]
    latent_backward = per_head_decay(low_rank_part[:, DECAY_RANK:], 1) + decay_spikes[1][:, :, None]
    ctx_fwd = per_head_decay(ctx_low[:, :DECAY_RANK], 0)
    ctx_bwd = per_head_decay(ctx_low[:, DECAY_RANK:], 1)
    cf_growth, cf_state = end_state(ctx_keys, values_ctx, ctx_fwd)
    cb_growth, cb_state = end_state(
        reverse_rows(ctx_keys), reverse_rows(values_ctx), reverse_rows(ctx_bwd)
    )
    lf_growth, lf_state = end_state(key_rows, values_lat, latent_forward)
    lb_growth, lb_state = end_state(
        reverse_rows(key_rows), reverse_rows(values_lat), reverse_rows(latent_backward)
    )
    identity = (
        jnp.ones((heads_per_shard, DK), jnp.float32),
        jnp.zeros((heads_per_shard, DK, value_cols), jnp.float32),
    )
    ctx_gathered = (
        lax.all_gather(cf_growth[None].astype(jnp.bfloat16), "sp", axis=0, tiled=True).astype(
            jnp.float32
        ),
        lax.all_gather(cf_state[None].astype(jnp.bfloat16), "sp", axis=0, tiled=True).astype(
            jnp.float32
        ),
        lax.all_gather(cb_growth[None].astype(jnp.bfloat16), "sp", axis=0, tiled=True).astype(
            jnp.float32
        ),
        lax.all_gather(cb_state[None].astype(jnp.bfloat16), "sp", axis=0, tiled=True).astype(
            jnp.float32
        ),
    )
    total_fwd, total_bwd = context_totals(
        ctx_gathered[0], ctx_gathered[1], ctx_gathered[2], ctx_gathered[3], identity
    )
    prefix = carried_in((lf_growth, lf_state), "sp", combine, identity, False)
    suffix = carried_in((lb_growth, lb_state), "sp", combine, identity, True)
    start_fwd = combine(total_fwd, prefix)[1]
    start_bwd = combine(total_bwd, suffix)[1]
    zero_state = jnp.zeros((heads_per_shard, DK, value_cols), jnp.float32)

    def direction_out(query_rows, key_list, value_list, log_decay, start_state):
        local_part = blockwise(query_rows, key_list, value_list, log_decay, zero_state, BLK)
        reach = query_rows * jnp.exp(jnp.cumsum(log_decay, axis=0))
        return local_part + jnp.einsum("nhd,hde->nhe", reach, start_state, precision=precise)

    out_fwd = direction_out(queries, key_rows, values_lat, latent_forward, start_fwd)
    out_bwd = reverse_rows(
        direction_out(
            reverse_rows(queries),
            reverse_rows(key_rows),
            reverse_rows(values_lat),
            reverse_rows(latent_backward),
            start_bwd,
        )
    )
    grouped = (out_fwd + out_bwd).reshape(tok_rows, -1, VGROUP)
    grouped = grouped * lax.rsqrt(jnp.mean(grouped * grouped, axis=-1, keepdims=True) + epsilon)
    heads_out = (grouped.reshape(tok_rows, -1) * output_gain * jax.nn.silu(gate_rows)).astype(
        jnp.bfloat16
    )
    branch = linear(lax.all_gather(heads_out, "tp", axis=1, tiled=True), output_matrix)
    return (latent.astype(jnp.float32) + gates[0] * branch).astype(jnp.bfloat16)


def exact(a, b):
    return lax.dot_general(
        a, b, (((1,), (0,)), ((), ())), precision=precise, preferred_element_type=jnp.float32
    )


def nt(a, b):
    return lax.dot_general(a, b, (((1,), (1,)), ((), ())), preferred_element_type=jnp.float32)


def nn(a, b):
    return lax.dot_general(a, b, (((1,), (0,)), ((), ())), preferred_element_type=jnp.float32)


def tn(a, b):
    return lax.dot_general(a, b, (((0,), (0,)), ((), ())), preferred_element_type=jnp.float32)


def short(value):
    return value.astype(jnp.bfloat16)


def terms(value):
    first = short(value)
    rest = value - first.astype(jnp.float32)
    second = short(rest)
    return first, second, short(rest - second.astype(jnp.float32))


def log_sigmoid(pre):
    return (jnp.minimum(pre, 0.0) - jnp.log1p(jnp.exp(-jnp.abs(pre)))) / gate_norm


def triangle_of(size, upper):
    i = lax.broadcasted_iota(jnp.int32, (size, size), 0)
    j = lax.broadcasted_iota(jnp.int32, (size, size), 1)
    return (j >= i) if upper else (j <= i)


def layer_kernel(
    n,
    s,
    inner,
    rows,
    crows,
    feats,
    heads,
    dv,
    parts,
    hparts,
    latent,
    context,
    conditioning,
    prompt,
    shift_m,
    scale_m,
    gate_m,
    query_m,
    key_m,
    value_m,
    og_m,
    down,
    up,
    bias,
    spike,
    gain,
    out_m,
    out_ref,
    x_all,
    xn,
    acc,
    low_acc,
    mod_w,
    proj_w,
    out_w,
    down_v,
    up_v,
    bias_v,
    spike_v,
    gain_v,
    cond_v,
    mod_own,
    mod_recv,
    mod_all,
    gate_own,
    gate_recv,
    stat_all,
    spike_rows,
    proj,
    ctx_kv,
    ctx_low,
    tot_own,
    tot_recv,
    st_own,
    st_recv,
    local_out,
    ho_all,
    total_out,
    load_sem,
    m1_s,
    m1_r,
    m2_s,
    m2_r,
    mg_s,
    mg_r,
    sa_s,
    sa_r,
    kv_s,
    kv_r,
    lo_s,
    lo_r,
    to_s,
    to_r,
    st_s,
    st_r,
    *gather_sems,
):
    me = lax.axis_index("tp")
    sp = lax.axis_index("sp")
    hk = heads * DK
    hv = heads * dv
    model = n * feats
    both = rows + crows
    width = feats // parts
    hwidth = hv // hparts
    f32 = jnp.float32

    loads = []

    def load(src, dst):
        copy = pltpu.make_async_copy(src, dst, load_sem.at[len(loads)])
        loads.append(copy)
        copy.start()
        return copy

    own_x = []
    for p in range(parts):
        cols = pl.ds(p * width, width)
        own_x.append(
            (
                load(latent.at[:, cols], x_all.at[me * parts + p, pl.ds(0, rows)]),
                load(context.at[:, cols], x_all.at[me * parts + p, pl.ds(rows, crows)]),
            )
        )
    first = [
        load(conditioning, cond_v.at[0]),
        load(prompt, cond_v.at[1]),
        load(shift_m, mod_w.at[0]),
        load(scale_m, mod_w.at[1]),
    ]
    gate_load = load(gate_m, mod_w.at[2])
    head_cols = pl.ds(pl.multiple_of(me * hk, hk), hk)
    small = [
        load(up.at[:, :, head_cols], up_v),
        load(bias.at[:, head_cols], bias_v),
        load(spike, spike_v),
        load(gain, gain_v),
    ]
    weights = [
        load(query_m, proj_w.at[pl.ds(0, hk)]),
        load(key_m, proj_w.at[pl.ds(hk, hk)]),
        load(value_m, proj_w.at[pl.ds(2 * hk, hv)]),
        load(og_m, proj_w.at[pl.ds(2 * hk + hv, hv)]),
        load(down, down_v),
    ]
    last = load(out_m, out_w)

    barrier = pltpu.get_barrier_semaphore()
    for d in range(1, n):
        pl.semaphore_signal(
            barrier, inc=1, device_id={"tp": lax.rem(me + d, n)}, device_id_type=MESH
        )
    for d in range(1, s):
        pl.semaphore_signal(
            barrier, inc=1, device_id={"sp": lax.rem(sp + d, s)}, device_id_type=MESH
        )
    pl.semaphore_wait(barrier, n - 1 + s - 1)

    started = []

    def send(src, dst, send_sem, recv_sem, axis, d):
        index, count = (me, n) if axis == "tp" else (sp, s)
        copy = pltpu.make_async_remote_copy(
            src_ref=src,
            dst_ref=dst,
            send_sem=send_sem,
            recv_sem=recv_sem,
            device_id={axis: lax.rem(index + d, count)},
            device_id_type=MESH,
        )
        copy.start()
        started.append(copy)
        return copy

    line = n // inner
    z, y = lax.div(me, inner), lax.rem(me, inner)
    mate = z + 1 - 2 * lax.rem(z, 2)
    paired = inner > 1 and line % 2 == 0
    at_end = (z == 0) | (z == line - 1)

    def level(i):
        table = []
        for at in range(line):
            order = [at]
            for k in range(1, line):
                order += [b for b in (at - k, at + k) if 0 <= b < line]
            table.append(order[i])
        return sum(jnp.where(z == at, table[at], 0) for at in range(line))

    def block_of(at, column):
        return at * inner + column

    class Gather:
        def __init__(self, ref, pieces, sems):
            self.ref, self.pieces = ref, pieces
            self.lanes = {
                lane: (sems[2 * j], sems[2 * j + 1])
                for j, lane in enumerate(("up", "down", "across", "side"))
            }
            self.turned = tuple(range(pieces // 2, pieces)) if paired else ()

        def copy(self, lane, block, piece, slot, target):
            sends, recvs = self.lanes[lane]
            ref = self.ref.at[block * self.pieces + piece]
            return pltpu.make_async_remote_copy(
                src_ref=ref,
                dst_ref=ref,
                send_sem=sends.at[slot, piece],
                recv_sem=recvs.at[slot, piece],
                device_id={"tp": target},
                device_id_type=MESH,
            )

        def hop(self, lane, at, piece, slot):
            target = {
                "up": block_of(jnp.minimum(z + 1, line - 1), y),
                "down": block_of(jnp.maximum(z - 1, 0), y),
                "across": block_of(z, inner - 1 - y),
            }[lane]
            return self.copy(lane, block_of(at, y), piece, slot, target)

        def sends(self, k, piece, act):
            for lane, at, has, onward, slot, odd in (
                ("up", z - k, z >= k, z + 1 < line, max(2 * k - 1, 0), 0),
                ("down", z + k, z + k < line, z > 0, 2 * k, 1),
            ):
                if k < line - 1:
                    pl.when(has & onward)(lambda: act(self.hop(lane, at, piece, k)))
                if inner > 1 and (k > 0 or lane == "up"):
                    if k == 1 and piece in self.turned:
                        has = has & (lax.rem(z, 2) == odd)
                    pl.when(has)(lambda: act(self.hop("across", at, piece, slot)))

        def start(self, piece):
            self.sends(0, piece, lambda c: c.start())

        def step(self, k, piece):
            for lane, at, has in (("up", z - k, z >= k), ("down", z + k, z + k < line)):
                pl.when(has)(lambda: self.hop(lane, at, piece, k - 1).wait_recv())
            self.sends(k, piece, lambda c: c.start())

        def side(self, piece):
            return self.copy(
                "side", block_of(z, inner - 1 - y), piece, 0, block_of(mate, y)
            )

        def side_start(self, when, piece):
            pl.when(when)(lambda: self.side(piece).start())

        def arrive(self, i, piece):
            at = level(i)
            block = block_of(at, inner - 1 - y)
            slot = jnp.where(at < z, 2 * (z - at) - 1, 2 * (at - z))

            def plain():
                self.copy("across", block, piece, slot, block).wait_recv()

            if i == 0 or piece not in self.turned:
                plain()
                return
            pl.when(at != mate)(plain)
            pl.when(at == mate)(
                lambda: self.copy("side", block, piece, 0, block).wait_recv()
            )

        def drain(self):
            for piece in range(self.pieces):
                for k in range(line):
                    self.sends(k, piece, lambda c: c.wait_send())
                if piece in self.turned:
                    self.side(piece).wait_send()

    def run(events):
        for _, act in sorted(enumerate(events), key=lambda e: (e[1][0], e[0])):
            act[1]()

    xg = Gather(x_all, parts, gather_sems[:8])
    hg = Gather(ho_all, hparts, gather_sems[8:16])

    for copy in own_x[0]:
        copy.wait()
    xg.start(0)
    for pair in own_x[1:]:
        for copy in pair:
            copy.wait()

    ones = jnp.ones((16, width), jnp.bfloat16)
    row_sum = jnp.zeros((16, both), f32)
    row_squares = jnp.zeros((16, both), f32)
    for p in range(parts):
        own = x_all[me * parts + p]
        own_f = own.astype(f32)
        row_sum = row_sum + nt(ones, own)
        for part in terms(own_f * own_f):
            row_squares = row_squares + nt(ones, part)
    stat_all[me] = jnp.zeros(stat_all.shape[1:], f32)
    stat_all[me, 0:1, 0:both] = row_sum[0:1]
    stat_all[me, 1:2, 0:both] = row_squares[0:1]
    sa = [
        send(stat_all.at[me], stat_all.at[me], sa_s.at[d - 1], sa_r.at[d - 1], "tp", d)
        for d in range(1, n)
    ]
    for p in range(1, parts):
        xg.start(p)

    for copy in first:
        copy.wait()

    def one_row(which):
        part = cond_v[which].astype(f32)
        return jnp.concatenate([part[r : r + 1] for r in range(part.shape[0])], axis=1)

    row_of = lax.broadcasted_iota(jnp.int32, (16, shift_m.shape[1]), 0)
    conds = jnp.where(row_of == 0, one_row(0), one_row(1))
    conds = short(conds * lax.logistic(conds))
    for which in range(2):
        mod_own[2 * which : 2 * which + 2, :] = nt(conds, mod_w[which])[0:2]
    m1 = [
        send(mod_own, mod_recv.at[d - 1], m1_s.at[d - 1], m1_r.at[d - 1], "sp", d)
        for d in range(1, s)
    ]

    def exchange_mods():
        for copy in m1:
            copy.wait_recv()
        total = mod_own[...]
        for d in range(1, s):
            total = total + mod_recv[d - 1]
        mod_all[me] = total
        return [
            send(mod_all.at[me], mod_all.at[me], m2_s.at[d - 1], m2_r.at[d - 1], "tp", d)
            for d in range(1, n)
        ]

    held = {}

    def send_mods():
        held["m2"] = exchange_mods()

    def send_gates():
        gate_load.wait()
        gate_own[...] = nt(conds, mod_w[2])[0:2]
        held["mg"] = [
            send(gate_own, gate_recv.at[d - 1], mg_s.at[d - 1], mg_r.at[d - 1], "sp", d)
            for d in range(1, s)
        ]

    def early():
        for copy in small:
            copy.wait()
        slot_head = lax.broadcasted_iota(jnp.int32, (spike_v.shape[1], hk), 0)
        lane_head = lax.broadcasted_iota(jnp.int32, (spike_v.shape[1], hk), 1) // DK
        pick = jnp.where(slot_head == me * heads + lane_head, 1.0, 0.0).astype(jnp.bfloat16)
        for e in range(2):
            spike_rows[:, e * hk : (e + 1) * hk] = sum(
                tn(part, pick) for part in terms(spike_v[e])
            )
        acc[...] = jnp.zeros(acc.shape, f32)
        low_acc[...] = jnp.zeros(low_acc.shape, f32)

    def moments():
        for copy in sa:
            copy.wait_recv()
        stats = sum(stat_all[b] for b in range(n))
        diagonal = lax.broadcasted_iota(jnp.int32, (both, both), 0) == lax.broadcasted_iota(
            jnp.int32, (both, both), 1
        )

        def column_of(row):
            return (
                jnp.sum(
                    jnp.where(diagonal, stats[row : row + 1, 0:both], 0.0), axis=1, keepdims=True
                )
                / model
            )

        mean = column_of(0)
        held["mean"] = mean
        held["spread"] = lax.rsqrt(column_of(1) - mean * mean + epsilon)

    def wait_mods():
        for copy in held["m2"]:
            copy.wait_recv()
        for copy in weights:
            copy.wait()

    tile = math.gcd(2 * hk + 2 * hv, 512)
    columns = acc.shape[1]

    def project_block(block):
        cols = pl.ds(pl.multiple_of(block * feats, feats), feats)
        mean, spread = held["mean"], held["spread"]
        mod = mod_all[block]
        for p in range(parts):
            lanes = slice(p * width, (p + 1) * width)
            x = (x_all[block * parts + p].astype(f32) - mean) * spread
            m = mod[:, lanes]
            xn[0:rows, lanes] = short(x[0:rows] * (1.0 + m[2:3]) + m[0:1])
            xn[rows:, lanes] = short(x[rows:] * (1.0 + m[3:4]) + m[1:2])
        low_acc[...] += nt(xn[...], down_v[:, cols])
        for t in range(columns // tile):
            out = slice(t * tile, (t + 1) * tile)
            acc[:, out] += nt(xn[...], proj_w[out, cols])

    def column_block(i):
        project_block(block_of(level(i), y))

    def other_block(i):
        if i > 0:
            for p in range(parts):
                xg.arrive(i, p)
        project_block(block_of(level(i), inner - 1 - y))

    unit, lag, cost = 0.79, 1.8, 0.68
    arrival = lambda k, p: unit * ((k - 1) * parts + p + 1) + lag
    events = [
        (arrival(1, parts // 2 - 1) + 0.01, send_mods),
        (arrival(1, parts // 2 - 1) + 0.02, send_gates),
        (arrival(1, parts - 1) + 0.05, early),
        (arrival(1, parts - 1) + 0.06, moments),
        (arrival(2, parts // 2) + 0.01, wait_mods),
    ]
    for k in range(1, line):
        for p in range(parts):
            events.append((arrival(k, p), functools.partial(xg.step, k, p)))
    if inner > 1:
        for p in range(parts):
            events.append((arrival(1, p) + 0.03, functools.partial(xg.arrive, 0, p)))
            if p in xg.turned:
                events.append(
                    (arrival(1, p) + 0.04, functools.partial(xg.side_start, at_end, p))
                )
                if line > 2:
                    events.append(
                        (
                            arrival(line - 2, parts - 1) + 0.01,
                            functools.partial(
                                xg.side_start, jnp.logical_not(at_end), p
                            ),
                        )
                    )
    tasks = []
    for i in range(line):
        ready = arrival(i, parts - 1) + 0.02 if i else 0.0
        tasks.append((ready, functools.partial(column_block, i)))
        if inner > 1:
            ready = arrival(max(i, 1), parts - 1) + 0.05 + (lag if i else 0)
            if i == 1 and xg.turned:
                ready = max(ready, arrival(line - 1, parts - 1) + unit * len(xg.turned))
            tasks.append((ready, functools.partial(other_block, i)))
    clock = arrival(2, parts // 2) + 0.02
    for ready, task in sorted(tasks, key=lambda t: t[0]):
        clock = max(clock, ready)
        events.append((clock, task))
        clock += cost
    run(events)
    proj[...] = short(acc[...])

    own_ctx = pl.ds(pl.multiple_of(sp * crows, crows), crows)
    ctx_kv[own_ctx, :] = proj[rows:, hk : 2 * hk + hv]
    ctx_low[own_ctx, :] = jnp.zeros((crows, ctx_low.shape[1]), f32)
    ctx_low[own_ctx, 0 : 2 * DECAY_RANK] = low_acc[rows:]
    kv = [
        send(ctx_kv.at[own_ctx], ctx_kv.at[own_ctx], kv_s.at[d - 1], kv_r.at[d - 1], "sp", d)
        for d in range(1, s)
    ]
    lo = [
        send(ctx_low.at[own_ctx], ctx_low.at[own_ctx], lo_s.at[d - 1], lo_r.at[d - 1], "sp", d)
        for d in range(1, s)
    ]

    none = jnp.zeros((DECAY_RANK, hk), jnp.bfloat16)
    up_both = jnp.concatenate(
        [
            jnp.concatenate([up_v[0], none], axis=1),
            jnp.concatenate([none, up_v[1]], axis=1),
        ],
        axis=0,
    )
    bias_both = jnp.concatenate([bias_v[0:1], bias_v[1:2]], axis=1)

    def logs_of(low):
        return log_sigmoid(sum(nn(part, up_both) for part in terms(low)) + bias_both)

    def running(logs, length, e):
        lanes = slice(e * hk, (e + 1) * hk)
        mask = jnp.where(triangle_of(length, e == 1), 1.0, 0.0).astype(jnp.bfloat16)
        return sum(nn(mask, part) for part in terms(logs[:, lanes]))

    logs = logs_of(low_acc[0:rows]) + spike_rows[...]
    cum = [running(logs, rows, e) for e in range(2)]
    whole = [cum[0][rows - 1 : rows], cum[1][0:1]]
    tot_own[0:1, :] = whole[0]
    tot_own[1:2, :] = whole[1]
    to = [
        send(tot_own, tot_recv.at[d - 1], to_s.at[d - 1], to_r.at[d - 1], "sp", d)
        for d in range(1, s)
    ]

    keys = proj[0:rows, hk : 2 * hk].astype(f32)
    per = hparts // heads
    weighted = [short(keys * jnp.exp(whole[e] - cum[e])) for e in range(2)]
    st = {}
    for h in range(heads):
        for e in range(2):
            state = short(
                tn(
                    weighted[e][:, h * DK : (h + 1) * DK],
                    proj[0:rows, 2 * hk + h * dv : 2 * hk + (h + 1) * dv],
                )
            )
            for q in range(per):
                st_own[e, h * per + q] = state[:, q * hwidth : (q + 1) * hwidth]
        for q in range(h * per, (h + 1) * per):
            for d in range(1, s):
                later = lax.rem(sp + d, s) > sp
                st[q, d] = send(
                    st_own.at[jnp.where(later, 0, 1), q],
                    st_recv.at[d - 1, q],
                    st_s.at[d - 1, q],
                    st_r.at[d - 1, q],
                    "sp",
                    d,
                )

    queries = proj[0:rows, 0:hk].astype(f32) * DK ** (-0.5)
    blocks = rows // BLK

    def span(b):
        return slice(b * BLK, (b + 1) * BLK)

    inside = [[], []]
    for b in range(blocks):
        f = cum[0][span(b)]
        inside[0].append(f if b == 0 else f - cum[0][b * BLK - 1 : b * BLK])
        f = cum[1][span(b)]
        inside[1].append(
            f if b == blocks - 1 else f - cum[1][(b + 1) * BLK : (b + 1) * BLK + 1]
        )
    ends = [[part[BLK - 1 : BLK] for part in inside[0]], [part[0:1] for part in inside[1]]]
    q_dec = [[short(queries[span(b)] * jnp.exp(inside[e][b])) for b in range(blocks)] for e in range(2)]
    k_dec = [[short(keys[span(b)] * jnp.exp(-inside[e][b])) for b in range(blocks)] for e in range(2)]
    k_end = [
        [short(keys[span(b)] * jnp.exp(ends[e][b] - inside[e][b])) for b in range(blocks)]
        for e in range(2)
    ]
    lower, upper = triangle_of(BLK, False), triangle_of(BLK, True)
    scores = []
    for h in range(heads):
        ch = slice(h * DK, (h + 1) * DK)
        lines = []
        for b in range(blocks):
            strip = []
            for c in range(blocks):
                if b == c:
                    strip.append(
                        jnp.where(lower, nt(q_dec[0][b][:, ch], k_dec[0][b][:, ch]), 0.0)
                        + jnp.where(upper, nt(q_dec[1][b][:, ch], k_dec[1][b][:, ch]), 0.0)
                    )
                    continue
                e = 0 if c < b else 1
                near = q_dec[e][b][:, ch]
                between = range(c + 1, b) if c < b else range(b + 1, c)
                if len(between) > 0:
                    gap = sum(ends[e][m][:, ch] for m in between)
                    near = short(queries[span(b)][:, ch] * jnp.exp(inside[e][b][:, ch] + gap))
                strip.append(nt(near, k_end[e][c][:, ch]))
            lines.append(jnp.concatenate(strip, axis=1) if blocks > 1 else strip[0])
        scores.append(short(jnp.concatenate(lines, axis=0) if blocks > 1 else lines[0]))

    for copy in to:
        copy.wait_recv()
    places = {d: lax.rem(sp - d + s, s) for d in range(1, s)}

    def passed(low_end, high_end, direction):
        result = jnp.zeros((1, hk), f32)
        for d in range(1, s):
            inside_it = jnp.where((places[d] > low_end) & (places[d] < high_end), 1.0, 0.0)
            result = result + inside_it * tot_recv[d - 1][direction : direction + 1]
        return result

    ctx_reach = [
        short(queries * jnp.exp(cum[0] + passed(-1, sp, 0))),
        short(queries * jnp.exp(cum[1] + passed(sp, s, 1))),
    ]
    reach = []
    for d in range(1, s):
        p = places[d]
        before = jnp.where(p < sp, 1.0, 0.0)
        exponent = before * (cum[0] + passed(p, sp, 0)) + (1.0 - before) * (
            cum[1] + passed(sp, p, 1)
        )
        reach.append(short(queries * jnp.exp(exponent)))
    gate_rows = proj[0:rows, 2 * hk + hv :].astype(f32)
    small_gate = gate_rows * lax.logistic(gate_rows) * gain_v[...]

    for copy in kv + lo:
        copy.wait_recv()
    ctx_keys = ctx_kv[:, 0:hk].astype(f32)
    ctx_logs = logs_of(ctx_low[:, 0 : 2 * DECAY_RANK])
    length = s * crows
    ctx_weighted = []
    for e in range(2):
        c = running(ctx_logs, length, e)
        end = c[length - 1 : length] if e == 0 else c[0:1]
        ctx_weighted.append(short(ctx_keys * jnp.exp(end - c)))
    for h in range(heads):
        ch = slice(h * DK, (h + 1) * DK)
        vc = slice(h * dv, (h + 1) * dv)
        ctx_values = ctx_kv[:, hk + h * dv : hk + (h + 1) * dv]
        local_out[:, vc] = nn(
            jnp.concatenate([scores[h]] + [r[:, ch] for r in ctx_reach], axis=1),
            jnp.concatenate(
                [proj[0:rows, 2 * hk + h * dv : 2 * hk + (h + 1) * dv]]
                + [short(tn(w[:, ch], ctx_values)) for w in ctx_weighted],
                axis=0,
            ),
        )
    gi = lax.broadcasted_iota(jnp.int32, (hwidth, hwidth), 0) // VGROUP
    gj = lax.broadcasted_iota(jnp.int32, (hwidth, hwidth), 1) // VGROUP
    group = jnp.where(gi == gj, 1.0, 0.0).astype(jnp.bfloat16)

    def head_piece(q):
        h = q // per
        ch = slice(h * DK, (h + 1) * DK)
        vc = slice(q * hwidth, (q + 1) * hwidth)
        for d in range(1, s):
            st[q, d].wait_recv()
        o = local_out[:, vc] + nn(
            jnp.concatenate([r[:, ch] for r in reach], axis=1),
            jnp.concatenate([st_recv[d - 1, q] for d in range(1, s)], axis=0),
        )
        squares = o * o
        top = short(squares)
        rest = short(squares - top.astype(f32))
        power = (nn(top, group) + nn(rest, group)) * (1.0 / VGROUP)
        ho_all[me * hparts + q] = short(o * lax.rsqrt(power + epsilon) * small_gate[:, vc])
        hg.start(q)

    def ready_out():
        last.wait()
        for copy in held["mg"]:
            copy.wait_recv()
        total_out[...] = jnp.zeros(total_out.shape, f32)

    def add_half(block, half):
        cols = pl.ds(pl.multiple_of(block * feats + half * 2 * hwidth, 2 * hwidth), 2 * hwidth)
        pair = jnp.concatenate(
            [ho_all[block * hparts + 2 * half], ho_all[block * hparts + 2 * half + 1]], axis=1
        )
        total_out[...] += nt(pair, out_w[:, cols])

    def add_column(i, half):
        add_half(block_of(level(i), y), half)

    def add_other(i, half):
        if i > 0:
            hg.arrive(i, 2 * half)
            hg.arrive(i, 2 * half + 1)
        add_half(block_of(level(i), inner - 1 - y), half)

    gap_h, hop_h = 1.4, 2.5
    here = lambda k, q: gap_h * q + hop_h * k
    events = [(here(0, 1) + 0.01, ready_out)]
    for q in range(hparts):
        events.append((here(0, q), functools.partial(head_piece, q)))
        for k in range(1, line):
            events.append((here(k, q), functools.partial(hg.step, k, q)))
        if inner > 1:
            events.append((here(1, q) + 0.02, functools.partial(hg.arrive, 0, q)))
            if q in hg.turned:
                events.append(
                    (here(1, q) + 0.03, functools.partial(hg.side_start, at_end, q))
                )
                if line > 2:
                    events.append(
                        (
                            here(line - 2, q) + 0.03,
                            functools.partial(
                                hg.side_start, jnp.logical_not(at_end), q
                            ),
                        )
                    )
    for i in range(line):
        for half in range(hparts // 2):
            when = here(i, 2 * half + 1) + 0.1
            events.append((when, functools.partial(add_column, i, half)))
            if inner > 1:
                when += hop_h + 0.1
                if i == 1 and 2 * half in hg.turned:
                    when = max(when, here(line - 1, 2 * half + 1) + 0.4)
                events.append((when, functools.partial(add_other, i, half)))
    run(events)
    gates = gate_own[0:1]
    for d in range(1, s):
        gates = gates + gate_recv[d - 1, 0:1]
    for p in range(parts):
        lanes = slice(p * width, (p + 1) * width)
        out_ref[:, lanes] = short(
            x_all[me * parts + p, 0:rows].astype(f32) + gates[:, lanes] * total_out[:, lanes]
        )
    for copy in started:
        copy.wait_send()
    xg.drain()
    hg.drain()


def one_kernel(
    latent,
    context,
    conditioning,
    context_prompt_vector,
    shift_matrix,
    scale_matrix,
    residual_gate_matrix,
    query_matrix,
    key_matrix,
    value_matrix,
    gate_matrix,
    decay_down_factor,
    decay_up_factor,
    decay_key_bias,
    spike_log_decay,
    output_gain,
    output_matrix,
):
    n, s = lax.axis_size("tp"), lax.axis_size("sp")
    rows, feats = latent.shape
    crows = context.shape[0]
    heads = HEADS // n
    hk, hv = query_matrix.shape[0], value_matrix.shape[0]
    dv = hv // heads
    model = n * feats
    both = rows + crows
    inputs = conditioning.shape[0]
    parts = feats // 128
    hparts = hv // 128
    stat_width = -(-both // 128) * 128
    bf, f32 = jnp.bfloat16, jnp.float32
    vmem, dma = pltpu.VMEM, pltpu.SemaphoreType.DMA
    pair = lambda *k: [dma(k), dma(k)]
    scratch = [
        vmem((n * parts, both, 128), bf),
        vmem((both, feats), bf),
        vmem((both, 2 * hk + 2 * hv), f32),
        vmem((both, 2 * DECAY_RANK), f32),
        vmem((3, feats, inputs), bf),
        vmem((2 * hk + 2 * hv, model), bf),
        vmem((output_matrix.shape[0], model), bf),
        vmem((2 * DECAY_RANK, model), bf),
        vmem((2, DECAY_RANK, hk), bf),
        vmem((2, hk), f32),
        vmem((2, HEADS, rows), f32),
        vmem((1, hv), f32),
        vmem((2, inputs // 128, 128), bf),
        vmem((4, feats), f32),
        vmem((s - 1, 4, feats), f32),
        vmem((n, 4, feats), f32),
        vmem((2, feats), f32),
        vmem((s - 1, 2, feats), f32),
        vmem((n, 2, stat_width), f32),
        vmem((rows, 2 * hk), f32),
        vmem((both, 2 * hk + 2 * hv), bf),
        vmem((s * crows, hk + hv), bf),
        vmem((s * crows, 128), f32),
        vmem((2, hk), f32),
        vmem((s - 1, 2, hk), f32),
        vmem((2, hparts, DK, 128), bf),
        vmem((s - 1, hparts, DK, 128), bf),
        vmem((rows, hv), f32),
        vmem((n * hparts, rows, 128), bf),
        vmem((rows, feats), f32),
        dma((15 + 2 * parts,)),
    ]
    for counts in ((s - 1,), (n - 1,), (s - 1,), (n - 1,), (s - 1,), (s - 1,), (s - 1,), (s - 1, hparts)):
        scratch += pair(*counts)
    inner = 2 if n % 2 == 0 else 1
    line = n // inner
    hops = max(line - 1, 1)
    for pieces in (parts, hparts):
        for count in (hops, hops, 2 * line - 1, 1):
            scratch += pair(count, pieces)
    return pl.pallas_call(
        functools.partial(
            layer_kernel, n, s, inner, rows, crows, feats, heads, dv, parts, hparts
        ),
        out_shape=jax.ShapeDtypeStruct((rows, feats), bf),
        in_specs=[pl.BlockSpec(memory_space=pl.ANY)] * 17,
        out_specs=pl.BlockSpec(memory_space=pltpu.VMEM),
        scratch_shapes=scratch,
        compiler_params=pltpu.CompilerParams(
            collective_id=0, has_side_effects=True, vmem_limit_bytes=60 * 1024 * 1024
        ),
        name="layer",
    )(
        latent,
        context,
        conditioning.reshape(-1, 128),
        context_prompt_vector.reshape(-1, 128),
        shift_matrix,
        scale_matrix,
        residual_gate_matrix,
        query_matrix,
        key_matrix,
        value_matrix,
        gate_matrix,
        jnp.swapaxes(decay_down_factor, 1, 2).reshape(2 * DECAY_RANK, model),
        decay_up_factor,
        decay_key_bias,
        jnp.swapaxes(spike_log_decay, 1, 2),
        output_gain.reshape(1, -1),
        output_matrix,
    )


def solution(mesh):
    placed = (
        P("sp", "tp"),
        P("sp", "tp"),
        P("sp"),
        P("sp"),
        P("tp", "sp"),
        P("tp", "sp"),
        P("tp", "sp"),
        P("tp", None),
        P("tp", None),
        P("tp", None),
        P("tp", None),
        P(),
        P(),
        P(),
        P(None, "sp", None),
        P("tp"),
        P("tp", None),
    )
    whole_heads = HEADS % mesh.shape["tp"] == 0
    return jax.shard_map(
        one_kernel if whole_heads else local, mesh=mesh, in_specs=placed, out_specs=P("sp", "tp"), check_vma=False
    )
```

```python
import functools
import math

import jax
import jax.numpy as jnp
from jax import lax
from jax.experimental import pallas as pl
from jax.experimental.pallas import tpu as pltpu
from jax.sharding import PartitionSpec as P

D = 4096
HEADS = 16
DK = 128
DECAY_RANK = 16
BLK = 64
VGROUP = 64
MESH = pl.DeviceIdType.MESH


epsilon = 1e-05
gate_norm = 16.0
precise = lax.Precision.HIGHEST


def for_sending(value):

    def short(part):
        return part.astype(jnp.bfloat16) if part.dtype == jnp.float32 else part

    return jax.tree.map(short, value)


def from_partner(value, axis, distance):
    return lax.ppermute(value, axis, [(i, i ^ 1 << distance) for i in range(lax.axis_size(axis))])


def carried_in(value, axis, combine, identity, reverse):
    peers, index = (lax.axis_size(axis), lax.axis_index(axis))
    everything = jax.tree.map(
        lambda part, kind: lax.all_gather(part.astype(kind), axis),
        value,
        (jnp.bfloat16, jnp.bfloat16),
    )
    start = jax.tree.map(
        lambda part, zero: jnp.broadcast_to(jnp.asarray(zero, part.dtype), part.shape),
        value,
        identity,
    )

    def turn(k, before):
        at = peers - 1 - k if reverse else k
        reached = at > index if reverse else at < index
        new = combine(
            before, jax.tree.map(lambda part, own: part[at].astype(own.dtype), everything, value)
        )
        return jax.tree.map(lambda a, b: jnp.where(reached, a, b), new, before)

    return lax.fori_loop(0, peers, turn, start)


def linear(rows, weight):
    return lax.dot_general(
        rows, weight, (((1,), (1,)), ((), ())), preferred_element_type=jnp.float32
    )


def modulated(rows, row_sum, row_squares, shift_vec, scale_vec):
    rows_f = rows.astype(jnp.float32)
    mean_val = row_sum / D
    variance = row_squares / D - mean_val * mean_val
    return (
        (rows_f - mean_val) * lax.rsqrt(variance + epsilon) * (1.0 + scale_vec) + shift_vec
    ).astype(jnp.bfloat16)


def reverse_rows(array):
    return jnp.flip(array, axis=0)


def end_state(key_rows, value_rows, log_decay):
    cumulative = jnp.cumsum(log_decay, axis=0)
    totals = cumulative[-1]
    weighted = key_rows * jnp.exp(totals - cumulative)
    return (jnp.exp(totals), jnp.einsum("nhd,nhe->hde", weighted, value_rows, precision=precise))


def combine(earlier, later):
    return (earlier[0] * later[0], later[0][..., None] * earlier[1] + later[1])


def blockwise(queries, key_rows, value_rows, log_decay, carried, block_len):
    length, head_count, _ = queries.shape
    value_width = value_rows.shape[-1]
    blocks = length // block_len

    def shaped(array):
        return array.reshape(blocks, block_len, head_count, array.shape[-1])

    triangle = jnp.tril(jnp.ones((block_len, block_len), jnp.float32))

    def advance(state_now, inputs):
        block_q, block_k, block_v, block_a = inputs
        cumulative = jnp.cumsum(block_a, axis=0)
        block_end = cumulative[-1]
        query_dec = block_q * jnp.exp(cumulative)
        scores = (
            jnp.einsum("ihd,jhd->hij", query_dec, block_k * jnp.exp(-cumulative), precision=precise)
            * triangle
        )
        result = jnp.einsum("hij,jhe->ihe", scores, block_v, precision=precise)
        result = result + jnp.einsum("ihd,hde->ihe", query_dec, state_now, precision=precise)
        state_next = state_now * jnp.exp(block_end)[:, :, None] + jnp.einsum(
            "jhd,jhe->hde", block_k * jnp.exp(block_end - cumulative), block_v, precision=precise
        )
        return (state_next, result)

    _, outputs = lax.scan(
        advance, carried, (shaped(queries), shaped(key_rows), shaped(value_rows), shaped(log_decay))
    )
    return outputs.reshape(length, head_count, value_width)


def head_channels(pieces, per_head, tp_index):
    for bit_number in range(per_head.bit_length() - 1):
        partner = from_partner(
            (for_sending(pieces[0]), for_sending(pieces[1]), for_sending(pieces[2])),
            "tp",
            bit_number,
        )
        upper = tp_index // (1 << bit_number) % 2 == 1
        pieces = tuple(
            (
                jnp.where(
                    upper,
                    jnp.concatenate([theirs, mine], axis=1),
                    jnp.concatenate([mine, theirs], axis=1),
                )
                for mine, theirs in zip(pieces, partner)
            )
        )
    return pieces


def context_totals(fwd_growth, fwd_state, bwd_growth, bwd_state, identity):

    def absorb(carried, piece):
        return (combine(carried, piece), None)

    total_fwd, _ = lax.scan(absorb, identity, (fwd_growth, fwd_state))
    total_bwd, _ = lax.scan(absorb, identity, (bwd_growth, bwd_state), reverse=True)
    return (total_fwd, total_bwd)


def stored(array):
    return lax.optimization_barrier(array.astype(jnp.bfloat16))


def local(
    latent,
    context,
    conditioning,
    context_prompt_vector,
    shift_matrix,
    scale_matrix,
    residual_gate_matrix,
    query_matrix,
    key_matrix,
    value_matrix,
    gate_matrix,
    decay_down_factor,
    decay_up_factor,
    decay_key_bias,
    spike_log_decay,
    output_gain,
    output_matrix,
):
    tp_count = lax.axis_size("tp")
    tp_index = lax.axis_index("tp")
    per_head = max(tp_count // HEADS, 1)
    heads_per_shard = max(HEADS // tp_count, 1)
    leading_head = tp_index // per_head * heads_per_shard
    tok_rows = latent.shape[0]
    conds = jax.nn.silu(
        jnp.stack([conditioning, context_prompt_vector]).astype(jnp.float32)
    ).astype(jnp.bfloat16)
    shifts, scales, gates = lax.psum(
        (
            linear(conds, shift_matrix),
            linear(conds, scale_matrix),
            linear(conds, residual_gate_matrix),
        ),
        "sp",
    )
    down_both = jnp.concatenate([decay_down_factor[0].T, decay_down_factor[1].T], axis=0)
    lat_weights = (query_matrix, key_matrix, value_matrix, gate_matrix, down_both)
    ctx_weights = (key_matrix, value_matrix, down_both)
    lat_f = latent.astype(jnp.float32)
    ctx_f = context.astype(jnp.float32)
    lat_sum, lat_squares, ctx_sum, ctx_squares = lax.psum(
        (
            jnp.sum(lat_f, axis=1, keepdims=True),
            jnp.sum(lat_f * lat_f, axis=1, keepdims=True),
            jnp.sum(ctx_f, axis=1, keepdims=True),
            jnp.sum(ctx_f * ctx_f, axis=1, keepdims=True),
        ),
        "tp",
    )
    latent_normalized = modulated(latent, lat_sum, lat_squares, shifts[0], scales[0])
    normed_ctx = modulated(context, ctx_sum, ctx_squares, shifts[1], scales[1])
    lat_piece = lax.all_gather(latent_normalized, "tp", axis=1, tiled=True)
    ctx_piece = lax.all_gather(normed_ctx, "tp", axis=1, tiled=True)
    lat_new = tuple((linear(lat_piece, weight) for weight in lat_weights))
    ctx_new = tuple((linear(ctx_piece, weight) for weight in ctx_weights))
    query_part, key_part, value_part, gate_part, low_rank_part = lat_new
    ctx_key_part, ctx_value_part, ctx_low = ctx_new
    query_full, key_full, ctx_key_full = head_channels(
        (stored(query_part), stored(key_part), stored(ctx_key_part)), per_head, tp_index
    )

    def split_heads(rows, width):
        return rows.astype(jnp.float32).reshape(rows.shape[0], heads_per_shard, width)

    value_cols = value_part.shape[1] // heads_per_shard
    queries = split_heads(query_full, DK) * DK ** (-0.5)
    key_rows = split_heads(key_full, DK)
    ctx_keys = split_heads(ctx_key_full, DK)
    values_lat = split_heads(stored(value_part), value_cols)
    values_ctx = split_heads(stored(ctx_value_part), value_cols)
    gate_rows = stored(gate_part).astype(jnp.float32)

    def per_head_decay(low_rows, direction):
        up_part = lax.dynamic_slice_in_dim(
            decay_up_factor[direction], leading_head * DK, heads_per_shard * DK, 1
        ).astype(jnp.float32)
        bias_part = lax.dynamic_slice_in_dim(
            decay_key_bias[direction], leading_head * DK, heads_per_shard * DK, 0
        )
        pre_act = jnp.dot(low_rows, up_part, precision=precise) + bias_part
        return (jax.nn.log_sigmoid(pre_act) / gate_norm).reshape(
            low_rows.shape[0], heads_per_shard, DK
        )

    decay_spikes = lax.dynamic_slice_in_dim(spike_log_decay, leading_head, heads_per_shard, 2)
    latent_forward = per_head_decay(low_rank_part[:, :DECAY_RANK], 0) + decay_spikes[0][:, :, None]
    latent_backward = per_head_decay(low_rank_part[:, DECAY_RANK:], 1) + decay_spikes[1][:, :, None]
    ctx_fwd = per_head_decay(ctx_low[:, :DECAY_RANK], 0)
    ctx_bwd = per_head_decay(ctx_low[:, DECAY_RANK:], 1)
    cf_growth, cf_state = end_state(ctx_keys, values_ctx, ctx_fwd)
    cb_growth, cb_state = end_state(
        reverse_rows(ctx_keys), reverse_rows(values_ctx), reverse_rows(ctx_bwd)
    )
    lf_growth, lf_state = end_state(key_rows, values_lat, latent_forward)
    lb_growth, lb_state = end_state(
        reverse_rows(key_rows), reverse_rows(values_lat), reverse_rows(latent_backward)
    )
    identity = (
        jnp.ones((heads_per_shard, DK), jnp.float32),
        jnp.zeros((heads_per_shard, DK, value_cols), jnp.float32),
    )
    ctx_gathered = (
        lax.all_gather(cf_growth[None].astype(jnp.bfloat16), "sp", axis=0, tiled=True).astype(
            jnp.float32
        ),
        lax.all_gather(cf_state[None].astype(jnp.bfloat16), "sp", axis=0, tiled=True).astype(
            jnp.float32
        ),
        lax.all_gather(cb_growth[None].astype(jnp.bfloat16), "sp", axis=0, tiled=True).astype(
            jnp.float32
        ),
        lax.all_gather(cb_state[None].astype(jnp.bfloat16), "sp", axis=0, tiled=True).astype(
            jnp.float32
        ),
    )
    total_fwd, total_bwd = context_totals(
        ctx_gathered[0], ctx_gathered[1], ctx_gathered[2], ctx_gathered[3], identity
    )
    prefix = carried_in((lf_growth, lf_state), "sp", combine, identity, False)
    suffix = carried_in((lb_growth, lb_state), "sp", combine, identity, True)
    start_fwd = combine(total_fwd, prefix)[1]
    start_bwd = combine(total_bwd, suffix)[1]
    zero_state = jnp.zeros((heads_per_shard, DK, value_cols), jnp.float32)

    def direction_out(query_rows, key_list, value_list, log_decay, start_state):
        local_part = blockwise(query_rows, key_list, value_list, log_decay, zero_state, BLK)
        reach = query_rows * jnp.exp(jnp.cumsum(log_decay, axis=0))
        return local_part + jnp.einsum("nhd,hde->nhe", reach, start_state, precision=precise)

    out_fwd = direction_out(queries, key_rows, values_lat, latent_forward, start_fwd)
    out_bwd = reverse_rows(
        direction_out(
            reverse_rows(queries),
            reverse_rows(key_rows),
            reverse_rows(values_lat),
            reverse_rows(latent_backward),
            start_bwd,
        )
    )
    grouped = (out_fwd + out_bwd).reshape(tok_rows, -1, VGROUP)
    grouped = grouped * lax.rsqrt(jnp.mean(grouped * grouped, axis=-1, keepdims=True) + epsilon)
    heads_out = (grouped.reshape(tok_rows, -1) * output_gain * jax.nn.silu(gate_rows)).astype(
        jnp.bfloat16
    )
    branch = linear(lax.all_gather(heads_out, "tp", axis=1, tiled=True), output_matrix)
    return (latent.astype(jnp.float32) + gates[0] * branch).astype(jnp.bfloat16)


def exact(a, b):
    return lax.dot_general(
        a, b, (((1,), (0,)), ((), ())), precision=precise, preferred_element_type=jnp.float32
    )


def nt(a, b):
    return lax.dot_general(a, b, (((1,), (1,)), ((), ())), preferred_element_type=jnp.float32)


def nn(a, b):
    return lax.dot_general(a, b, (((1,), (0,)), ((), ())), preferred_element_type=jnp.float32)


def tn(a, b):
    return lax.dot_general(a, b, (((0,), (0,)), ((), ())), preferred_element_type=jnp.float32)


def short(value):
    return value.astype(jnp.bfloat16)


X_STRAIGHT = ()
H_STRAIGHT = ()


def terms(value):
    first = short(value)
    rest = value - first.astype(jnp.float32)
    second = short(rest)
    return first, second, short(rest - second.astype(jnp.float32))


def log_sigmoid(pre):
    return (jnp.minimum(pre, 0.0) - jnp.log1p(jnp.exp(-jnp.abs(pre)))) / gate_norm


def triangle_of(size, upper):
    i = lax.broadcasted_iota(jnp.int32, (size, size), 0)
    j = lax.broadcasted_iota(jnp.int32, (size, size), 1)
    return (j >= i) if upper else (j <= i)


def layer_kernel(
    n,
    s,
    inner,
    rows,
    crows,
    feats,
    heads,
    dv,
    parts,
    hparts,
    latent,
    context,
    conditioning,
    prompt,
    shift_m,
    scale_m,
    gate_m,
    query_m,
    key_m,
    value_m,
    og_m,
    down,
    up,
    bias,
    spike,
    gain,
    out_m,
    out_ref,
    x_all,
    xn,
    acc,
    low_acc,
    mod_w,
    proj_w,
    out_w,
    down_v,
    up_v,
    bias_v,
    spike_v,
    gain_v,
    cond_v,
    mod_own,
    mod_recv,
    mod_all,
    gate_own,
    gate_recv,
    stat_all,
    spike_rows,
    proj,
    ctx_kv,
    ctx_low,
    tot_own,
    tot_recv,
    st_own,
    st_recv,
    local_out,
    ho_all,
    total_out,
    load_sem,
    m1_s,
    m1_r,
    m2_s,
    m2_r,
    mg_s,
    mg_r,
    sa_s,
    sa_r,
    kv_s,
    kv_r,
    lo_s,
    lo_r,
    to_s,
    to_r,
    st_s,
    st_r,
    *gather_sems,
):
    me = lax.axis_index("tp")
    sp = lax.axis_index("sp")
    hk = heads * DK
    hv = heads * dv
    model = n * feats
    both = rows + crows
    width = feats // parts
    hwidth = hv // hparts
    f32 = jnp.float32

    loads = []

    def load(src, dst):
        copy = pltpu.make_async_copy(src, dst, load_sem.at[len(loads)])
        loads.append(copy)
        copy.start()
        return copy

    own_x = []
    for p in range(parts):
        cols = pl.ds(p * width, width)
        own_x.append(
            (
                load(latent.at[:, cols], x_all.at[me * parts + p, pl.ds(0, rows)]),
                load(context.at[:, cols], x_all.at[me * parts + p, pl.ds(rows, crows)]),
            )
        )
    first = [
        load(conditioning, cond_v.at[0]),
        load(prompt, cond_v.at[1]),
        load(shift_m, mod_w.at[0]),
        load(scale_m, mod_w.at[1]),
    ]
    gate_load = load(gate_m, mod_w.at[2])
    head_cols = pl.ds(pl.multiple_of(me * hk, hk), hk)
    small = [
        load(up.at[:, :, head_cols], up_v),
        load(bias.at[:, head_cols], bias_v),
        load(spike, spike_v),
        load(gain, gain_v),
    ]
    weights = [
        load(query_m, proj_w.at[pl.ds(0, hk)]),
        load(key_m, proj_w.at[pl.ds(hk, hk)]),
        load(value_m, proj_w.at[pl.ds(2 * hk, hv)]),
        load(og_m, proj_w.at[pl.ds(2 * hk + hv, hv)]),
        load(down, down_v),
    ]
    last = load(out_m, out_w)

    barrier = pltpu.get_barrier_semaphore()
    for d in range(1, n):
        pl.semaphore_signal(
            barrier, inc=1, device_id={"tp": lax.rem(me + d, n)}, device_id_type=MESH
        )
    for d in range(1, s):
        pl.semaphore_signal(
            barrier, inc=1, device_id={"sp": lax.rem(sp + d, s)}, device_id_type=MESH
        )
    pl.semaphore_wait(barrier, n - 1 + s - 1)

    started = []

    def send(src, dst, send_sem, recv_sem, axis, d):
        index, count = (me, n) if axis == "tp" else (sp, s)
        copy = pltpu.make_async_remote_copy(
            src_ref=src,
            dst_ref=dst,
            send_sem=send_sem,
            recv_sem=recv_sem,
            device_id={axis: lax.rem(index + d, count)},
            device_id_type=MESH,
        )
        copy.start()
        started.append(copy)
        return copy

    line = n // inner
    z, y = lax.div(me, inner), lax.rem(me, inner)
    mate = z + 1 - 2 * lax.rem(z, 2)
    paired = inner > 1 and line % 2 == 0
    at_end = (z == 0) | (z == line - 1)

    def level(i):
        table = []
        for at in range(line):
            order = [at]
            for k in range(1, line):
                order += [b for b in (at - k, at + k) if 0 <= b < line]
            table.append(order[i])
        return sum(jnp.where(z == at, table[at], 0) for at in range(line))

    def block_of(at, column):
        return at * inner + column

    class Gather:
        def __init__(self, ref, pieces, straight, sems):
            self.ref, self.pieces, self.straight = ref, pieces, straight
            self.lanes = {
                lane: (sems[2 * j], sems[2 * j + 1])
                for j, lane in enumerate(("up", "down", "across", "side"))
            }
            self.turned = tuple(range(pieces // 2, pieces)) if paired else ()

        def copy(self, lane, block, piece, slot, target):
            sends, recvs = self.lanes[lane]
            ref = self.ref.at[block * self.pieces + piece]
            return pltpu.make_async_remote_copy(
                src_ref=ref,
                dst_ref=ref,
                send_sem=sends.at[slot, piece],
                recv_sem=recvs.at[slot, piece],
                device_id={"tp": target},
                device_id_type=MESH,
            )

        def hop(self, lane, at, piece, slot):
            target = {
                "up": block_of(jnp.minimum(z + 1, line - 1), y),
                "down": block_of(jnp.maximum(z - 1, 0), y),
                "across": block_of(z, inner - 1 - y),
            }[lane]
            return self.copy(lane, block_of(at, y), piece, slot, target)

        def reach(self, piece, act):
            for k in range(line - 1, 0, -1):
                for lane, has, to in (("up", z + k < line, z + k), ("down", z >= k, z - k)):
                    pl.when(has)(
                        lambda: act(
                            self.copy(lane, block_of(z, y), piece, k - 1, block_of(to, y))
                        )
                    )

        def lane_sends(self, lane, k, piece, act):
            up = lane == "up"
            at, has = (z - k, z >= k) if up else (z + k, z + k < line)
            slot = max(2 * k - 1, 0) if up else 2 * k
            if k < line - 1 and piece not in self.straight:
                onward = z + 1 < line if up else z > 0
                pl.when(has & onward)(lambda: act(self.hop(lane, at, piece, k)))
            if inner > 1 and (k > 0 or up):
                if k == 1 and piece in self.turned:
                    has = has & (lax.rem(z, 2) == (0 if up else 1))
                pl.when(has)(lambda: act(self.hop("across", at, piece, slot)))

        def sends(self, k, piece, act):
            if k == 0 and piece in self.straight:
                self.reach(piece, act)
            for lane in ("up", "down"):
                self.lane_sends(lane, k, piece, act)

        def start(self, piece):
            self.sends(0, piece, lambda c: c.start())

        def take(self, lane, k, piece):
            at, has = (z - k, z >= k) if lane == "up" else (z + k, z + k < line)
            pl.when(has)(lambda: self.hop(lane, at, piece, k - 1).wait_recv())
            self.lane_sends(lane, k, piece, lambda c: c.start())

        def near(self, k, piece):
            pl.when(z >= line // 2)(lambda: self.take("up", k, piece))
            pl.when(z < line // 2)(lambda: self.take("down", k, piece))

        def far(self, k, piece):
            pl.when(z < line // 2)(lambda: self.take("up", k, piece))
            pl.when(z >= line // 2)(lambda: self.take("down", k, piece))

        def side(self, piece):
            return self.copy(
                "side", block_of(z, inner - 1 - y), piece, 0, block_of(mate, y)
            )

        def side_start(self, when, piece):
            pl.when(when)(lambda: self.side(piece).start())

        def arrive(self, i, piece):
            at = level(i)
            block = block_of(at, inner - 1 - y)
            slot = jnp.where(at < z, 2 * (z - at) - 1, 2 * (at - z))

            def plain():
                self.copy("across", block, piece, slot, block).wait_recv()

            if i == 0 or piece not in self.turned:
                plain()
                return
            pl.when(at != mate)(plain)
            pl.when(at == mate)(
                lambda: self.copy("side", block, piece, 0, block).wait_recv()
            )

        def drain(self):
            for piece in range(self.pieces):
                for k in range(line):
                    self.sends(k, piece, lambda c: c.wait_send())
                if piece in self.turned:
                    self.side(piece).wait_send()

    def run(events):
        for _, act in sorted(enumerate(events), key=lambda e: (e[1][0], e[0])):
            act[1]()

    xg = Gather(x_all, parts, X_STRAIGHT, gather_sems[:8])
    hg = Gather(ho_all, hparts, H_STRAIGHT, gather_sems[8:16])

    for copy in own_x[0]:
        copy.wait()
    xg.start(0)
    for pair in own_x[1:]:
        for copy in pair:
            copy.wait()

    ones = jnp.ones((16, width), jnp.bfloat16)
    row_sum = jnp.zeros((16, both), f32)
    row_squares = jnp.zeros((16, both), f32)
    for p in range(parts):
        own = x_all[me * parts + p]
        own_f = own.astype(f32)
        row_sum = row_sum + nt(ones, own)
        for part in terms(own_f * own_f):
            row_squares = row_squares + nt(ones, part)
    stat_all[me] = jnp.zeros(stat_all.shape[1:], f32)
    stat_all[me, 0:1, 0:both] = row_sum[0:1]
    stat_all[me, 1:2, 0:both] = row_squares[0:1]
    sa = [
        send(stat_all.at[me], stat_all.at[me], sa_s.at[d - 1], sa_r.at[d - 1], "tp", d)
        for d in range(1, n)
    ]
    for p in range(1, parts):
        xg.start(p)

    for copy in first:
        copy.wait()

    def one_row(which):
        part = cond_v[which].astype(f32)
        return jnp.concatenate([part[r : r + 1] for r in range(part.shape[0])], axis=1)

    row_of = lax.broadcasted_iota(jnp.int32, (16, shift_m.shape[1]), 0)
    conds = jnp.where(row_of == 0, one_row(0), one_row(1))
    conds = short(conds * lax.logistic(conds))
    for which in range(2):
        mod_own[2 * which : 2 * which + 2, :] = nt(conds, mod_w[which])[0:2]
    m1 = [
        send(mod_own, mod_recv.at[d - 1], m1_s.at[d - 1], m1_r.at[d - 1], "sp", d)
        for d in range(1, s)
    ]

    def exchange_mods():
        for copy in m1:
            copy.wait_recv()
        total = mod_own[...]
        for d in range(1, s):
            total = total + mod_recv[d - 1]
        mod_all[me] = total
        return [
            send(mod_all.at[me], mod_all.at[me], m2_s.at[d - 1], m2_r.at[d - 1], "tp", d)
            for d in range(1, n)
        ]

    held = {}

    def send_mods():
        held["m2"] = exchange_mods()

    def send_gates():
        gate_load.wait()
        gate_own[...] = nt(conds, mod_w[2])[0:2]
        held["mg"] = [
            send(gate_own, gate_recv.at[d - 1], mg_s.at[d - 1], mg_r.at[d - 1], "sp", d)
            for d in range(1, s)
        ]

    def early():
        for copy in small:
            copy.wait()
        slot_head = lax.broadcasted_iota(jnp.int32, (spike_v.shape[1], hk), 0)
        lane_head = lax.broadcasted_iota(jnp.int32, (spike_v.shape[1], hk), 1) // DK
        pick = jnp.where(slot_head == me * heads + lane_head, 1.0, 0.0).astype(jnp.bfloat16)
        for e in range(2):
            spike_rows[:, e * hk : (e + 1) * hk] = sum(
                tn(part, pick) for part in terms(spike_v[e])
            )
        acc[...] = jnp.zeros(acc.shape, f32)
        low_acc[...] = jnp.zeros(low_acc.shape, f32)

    def moments():
        for copy in sa:
            copy.wait_recv()
        stats = sum(stat_all[b] for b in range(n))
        diagonal = lax.broadcasted_iota(jnp.int32, (both, both), 0) == lax.broadcasted_iota(
            jnp.int32, (both, both), 1
        )

        def column_of(row):
            return (
                jnp.sum(
                    jnp.where(diagonal, stats[row : row + 1, 0:both], 0.0), axis=1, keepdims=True
                )
                / model
            )

        mean = column_of(0)
        held["mean"] = mean
        held["spread"] = lax.rsqrt(column_of(1) - mean * mean + epsilon)

    def wait_mods():
        for copy in held["m2"]:
            copy.wait_recv()
        for copy in weights:
            copy.wait()

    tile = math.gcd(2 * hk + 2 * hv, 512)
    columns = acc.shape[1]

    def project_block(block):
        cols = pl.ds(pl.multiple_of(block * feats, feats), feats)
        mean, spread = held["mean"], held["spread"]
        mod = mod_all[block]
        for p in range(parts):
            lanes = slice(p * width, (p + 1) * width)
            x = (x_all[block * parts + p].astype(f32) - mean) * spread
            m = mod[:, lanes]
            xn[0:rows, lanes] = short(x[0:rows] * (1.0 + m[2:3]) + m[0:1])
            xn[rows:, lanes] = short(x[rows:] * (1.0 + m[3:4]) + m[1:2])
        low_acc[...] += nt(xn[...], down_v[:, cols])
        for t in range(columns // tile):
            out = slice(t * tile, (t + 1) * tile)
            acc[:, out] += nt(xn[...], proj_w[out, cols])

    def column_block(i):
        project_block(block_of(level(i), y))

    def other_block(i):
        if i > 0:
            for p in range(parts):
                xg.arrive(i, p)
        project_block(block_of(level(i), inner - 1 - y))

    unit, lag, cost = 0.79, 2.0, 0.6
    arrival = lambda k, p: unit * ((k - 1) * parts + p + 1) + lag
    mods_at = 9.4
    events = [
        (arrival(1, parts // 2 - 1) + 0.01, send_mods),
        (arrival(1, parts // 2 - 1) + 0.02, send_gates),
        (arrival(1, parts - 1) + 0.05, early),
        (arrival(1, parts - 1) + 0.06, moments),
        (mods_at, wait_mods),
    ]
    for k in range(1, line):
        for p in range(parts):
            events.append((arrival(k, p), functools.partial(xg.near, k, p)))
            if 2 * k < line + line % 2:
                events.append((arrival(k, p) + 0.005, functools.partial(xg.far, k, p)))
    if inner > 1:
        for p in range(parts):
            events.append((arrival(1, p) + 0.03, functools.partial(xg.arrive, 0, p)))
            if p in xg.turned:
                events.append(
                    (arrival(1, p) + 0.04, functools.partial(xg.side_start, at_end, p))
                )
                if line > 2:
                    events.append(
                        (
                            arrival(line - 2, parts - 1) + 0.01,
                            functools.partial(
                                xg.side_start, jnp.logical_not(at_end), p
                            ),
                        )
                    )
    tasks = []
    for i in range(line):
        ready = arrival(i, parts - 1) + 0.02 if i else 0.0
        tasks.append((ready, functools.partial(column_block, i)))
        if inner > 1:
            ready = arrival(max(i, 1), parts - 1) + 0.05 + (lag if i else 0)
            if i == 1 and xg.turned:
                ready = max(ready, arrival(line - 1, parts - 1) + unit * len(xg.turned))
            tasks.append((ready, functools.partial(other_block, i)))
    clock = mods_at + 0.01
    for ready, task in sorted(tasks, key=lambda t: t[0]):
        clock = max(clock, ready)
        events.append((clock, task))
        clock += cost
    run(events)
    proj[...] = short(acc[...])

    own_ctx = pl.ds(pl.multiple_of(sp * crows, crows), crows)
    ctx_kv[own_ctx, :] = proj[rows:, hk : 2 * hk + hv]
    ctx_low[own_ctx, :] = jnp.zeros((crows, ctx_low.shape[1]), jnp.bfloat16)
    for i, part in enumerate(terms(low_acc[rows:])):
        ctx_low[own_ctx, i * 2 * DECAY_RANK : (i + 1) * 2 * DECAY_RANK] = part
    lo = [
        send(ctx_low.at[own_ctx], ctx_low.at[own_ctx], lo_s.at[d - 1], lo_r.at[d - 1], "sp", d)
        for d in range(1, s)
    ]
    kv = [
        send(ctx_kv.at[own_ctx], ctx_kv.at[own_ctx], kv_s.at[d - 1], kv_r.at[d - 1], "sp", d)
        for d in range(1, s)
    ]

    none = jnp.zeros((DECAY_RANK, hk), jnp.bfloat16)
    up_both = jnp.concatenate(
        [
            jnp.concatenate([up_v[0], none], axis=1),
            jnp.concatenate([none, up_v[1]], axis=1),
        ],
        axis=0,
    )
    bias_both = jnp.concatenate([bias_v[0:1], bias_v[1:2]], axis=1)

    def logs_of(parts_of_low):
        return log_sigmoid(sum(nn(part, up_both) for part in parts_of_low) + bias_both)

    def running(logs, length, e):
        lanes = slice(e * hk, (e + 1) * hk)
        mask = jnp.where(triangle_of(length, e == 1), 1.0, 0.0).astype(jnp.bfloat16)
        return sum(nn(mask, part) for part in terms(logs[:, lanes]))

    logs = logs_of(terms(low_acc[0:rows])) + spike_rows[...]
    cum = [running(logs, rows, e) for e in range(2)]
    whole = [cum[0][rows - 1 : rows], cum[1][0:1]]
    tot_own[0:1, :] = whole[0]
    tot_own[1:2, :] = whole[1]
    to = [
        send(tot_own, tot_recv.at[d - 1], to_s.at[d - 1], to_r.at[d - 1], "sp", d)
        for d in range(1, s)
    ]

    keys = proj[0:rows, hk : 2 * hk].astype(f32)
    per = hparts // heads
    weighted = [short(keys * jnp.exp(whole[e] - cum[e])) for e in range(2)]
    st = {}
    for h in range(heads):
        for e in range(2):
            state = short(
                tn(
                    weighted[e][:, h * DK : (h + 1) * DK],
                    proj[0:rows, 2 * hk + h * dv : 2 * hk + (h + 1) * dv],
                )
            )
            for q in range(per):
                st_own[e, h * per + q] = state[:, q * hwidth : (q + 1) * hwidth]
        for q in range(h * per, (h + 1) * per):
            for d in range(1, s):
                later = lax.rem(sp + d, s) > sp
                st[q, d] = send(
                    st_own.at[jnp.where(later, 0, 1), q],
                    st_recv.at[d - 1, q],
                    st_s.at[d - 1, q],
                    st_r.at[d - 1, q],
                    "sp",
                    d,
                )

    queries = proj[0:rows, 0:hk].astype(f32) * DK ** (-0.5)
    blocks = rows // BLK

    def span(b):
        return slice(b * BLK, (b + 1) * BLK)

    inside = [[], []]
    for b in range(blocks):
        f = cum[0][span(b)]
        inside[0].append(f if b == 0 else f - cum[0][b * BLK - 1 : b * BLK])
        f = cum[1][span(b)]
        inside[1].append(
            f if b == blocks - 1 else f - cum[1][(b + 1) * BLK : (b + 1) * BLK + 1]
        )
    ends = [[part[BLK - 1 : BLK] for part in inside[0]], [part[0:1] for part in inside[1]]]
    q_dec = [[short(queries[span(b)] * jnp.exp(inside[e][b])) for b in range(blocks)] for e in range(2)]
    k_dec = [[short(keys[span(b)] * jnp.exp(-inside[e][b])) for b in range(blocks)] for e in range(2)]
    k_end = [
        [short(keys[span(b)] * jnp.exp(ends[e][b] - inside[e][b])) for b in range(blocks)]
        for e in range(2)
    ]
    lower, upper = triangle_of(BLK, False), triangle_of(BLK, True)
    scores = []
    for h in range(heads):
        ch = slice(h * DK, (h + 1) * DK)
        lines = []
        for b in range(blocks):
            strip = []
            for c in range(blocks):
                if b == c:
                    strip.append(
                        jnp.where(lower, nt(q_dec[0][b][:, ch], k_dec[0][b][:, ch]), 0.0)
                        + jnp.where(upper, nt(q_dec[1][b][:, ch], k_dec[1][b][:, ch]), 0.0)
                    )
                    continue
                e = 0 if c < b else 1
                near = q_dec[e][b][:, ch]
                between = range(c + 1, b) if c < b else range(b + 1, c)
                if len(between) > 0:
                    gap = sum(ends[e][m][:, ch] for m in between)
                    near = short(queries[span(b)][:, ch] * jnp.exp(inside[e][b][:, ch] + gap))
                strip.append(nt(near, k_end[e][c][:, ch]))
            lines.append(jnp.concatenate(strip, axis=1) if blocks > 1 else strip[0])
        scores.append(short(jnp.concatenate(lines, axis=0) if blocks > 1 else lines[0]))

    for copy in lo:
        copy.wait_recv()
    low_parts = [
        ctx_low[:, i * 2 * DECAY_RANK : (i + 1) * 2 * DECAY_RANK] for i in range(3)
    ]
    ctx_logs = logs_of(low_parts)
    length = s * crows
    ctx_decay = []
    for e in range(2):
        c = running(ctx_logs, length, e)
        end = c[length - 1 : length] if e == 0 else c[0:1]
        ctx_decay.append(jnp.exp(end - c))

    for copy in to:
        copy.wait_recv()
    places = {d: lax.rem(sp - d + s, s) for d in range(1, s)}

    def passed(low_end, high_end, direction):
        result = jnp.zeros((1, hk), f32)
        for d in range(1, s):
            inside_it = jnp.where((places[d] > low_end) & (places[d] < high_end), 1.0, 0.0)
            result = result + inside_it * tot_recv[d - 1][direction : direction + 1]
        return result

    ctx_reach = [
        short(queries * jnp.exp(cum[0] + passed(-1, sp, 0))),
        short(queries * jnp.exp(cum[1] + passed(sp, s, 1))),
    ]
    reach = []
    for d in range(1, s):
        p = places[d]
        before = jnp.where(p < sp, 1.0, 0.0)
        exponent = before * (cum[0] + passed(p, sp, 0)) + (1.0 - before) * (
            cum[1] + passed(sp, p, 1)
        )
        reach.append(short(queries * jnp.exp(exponent)))
    gate_rows = proj[0:rows, 2 * hk + hv :].astype(f32)
    small_gate = gate_rows * lax.logistic(gate_rows) * gain_v[...]

    for copy in kv:
        copy.wait_recv()
    ctx_keys = ctx_kv[:, 0:hk].astype(f32)
    ctx_weighted = [short(ctx_keys * part) for part in ctx_decay]
    for h in range(heads):
        ch = slice(h * DK, (h + 1) * DK)
        vc = slice(h * dv, (h + 1) * dv)
        ctx_values = ctx_kv[:, hk + h * dv : hk + (h + 1) * dv]
        local_out[:, vc] = nn(
            jnp.concatenate([scores[h]] + [r[:, ch] for r in ctx_reach], axis=1),
            jnp.concatenate(
                [proj[0:rows, 2 * hk + h * dv : 2 * hk + (h + 1) * dv]]
                + [short(tn(w[:, ch], ctx_values)) for w in ctx_weighted],
                axis=0,
            ),
        )
    gi = lax.broadcasted_iota(jnp.int32, (hwidth, hwidth), 0) // VGROUP
    gj = lax.broadcasted_iota(jnp.int32, (hwidth, hwidth), 1) // VGROUP
    group = jnp.where(gi == gj, 1.0, 0.0).astype(jnp.bfloat16)

    def head_piece(q):
        h = q // per
        ch = slice(h * DK, (h + 1) * DK)
        vc = slice(q * hwidth, (q + 1) * hwidth)
        for d in range(1, s):
            st[q, d].wait_recv()
        o = local_out[:, vc] + nn(
            jnp.concatenate([r[:, ch] for r in reach], axis=1),
            jnp.concatenate([st_recv[d - 1, q] for d in range(1, s)], axis=0),
        )
        squares = o * o
        top = short(squares)
        rest = short(squares - top.astype(f32))
        power = (nn(top, group) + nn(rest, group)) * (1.0 / VGROUP)
        ho_all[me * hparts + q] = short(o * lax.rsqrt(power + epsilon) * small_gate[:, vc])
        hg.start(q)

    def ready_out():
        last.wait()
        for copy in held["mg"]:
            copy.wait_recv()
        total_out[...] = jnp.zeros(total_out.shape, f32)

    def add_half(block, half):
        cols = pl.ds(pl.multiple_of(block * feats + half * 2 * hwidth, 2 * hwidth), 2 * hwidth)
        pair = jnp.concatenate(
            [ho_all[block * hparts + 2 * half], ho_all[block * hparts + 2 * half + 1]], axis=1
        )
        total_out[...] += nt(pair, out_w[:, cols])

    def add_column(i, half):
        add_half(block_of(level(i), y), half)

    def add_other(i, half):
        if i > 0:
            hg.arrive(i, 2 * half)
            hg.arrive(i, 2 * half + 1)
        add_half(block_of(level(i), inner - 1 - y), half)

    hop_h = 2.6
    here = lambda k, q: 0.4 * q + 0.4 * (q // 2) + hop_h * k
    events = [(here(0, 1) + 0.01, ready_out)]
    for q in range(hparts):
        events.append((here(0, q), functools.partial(head_piece, q)))
        for k in range(1, line):
            events.append((here(k, q), functools.partial(hg.near, k, q)))
            if 2 * k < line + line % 2:
                events.append((here(k, q) + 0.5, functools.partial(hg.far, k, q)))
        if inner > 1:
            events.append((here(1, q) + 0.02, functools.partial(hg.arrive, 0, q)))
            if q in hg.turned:
                events.append(
                    (here(1, q) + 0.03, functools.partial(hg.side_start, at_end, q))
                )
                if line > 2:
                    events.append(
                        (
                            here(line - 2, q) + 0.03,
                            functools.partial(
                                hg.side_start, jnp.logical_not(at_end), q
                            ),
                        )
                    )
    for i in range(line):
        for half in range(hparts // 2):
            when = here(i, 2 * half + 1) + 0.6
            events.append((when, functools.partial(add_column, i, half)))
            if inner > 1:
                when += hop_h + 0.1
                if i == 1 and 2 * half in hg.turned:
                    when = max(when, here(line - 1, 2 * half + 1) + 0.4)
                events.append((when, functools.partial(add_other, i, half)))
    run(events)
    gates = gate_own[0:1]
    for d in range(1, s):
        gates = gates + gate_recv[d - 1, 0:1]
    for p in range(parts):
        lanes = slice(p * width, (p + 1) * width)
        out_ref[:, lanes] = short(
            x_all[me * parts + p, 0:rows].astype(f32) + gates[:, lanes] * total_out[:, lanes]
        )
    for copy in started:
        copy.wait_send()
    xg.drain()
    hg.drain()


def one_kernel(
    latent,
    context,
    conditioning,
    context_prompt_vector,
    shift_matrix,
    scale_matrix,
    residual_gate_matrix,
    query_matrix,
    key_matrix,
    value_matrix,
    gate_matrix,
    decay_down_factor,
    decay_up_factor,
    decay_key_bias,
    spike_log_decay,
    output_gain,
    output_matrix,
):
    n, s = lax.axis_size("tp"), lax.axis_size("sp")
    rows, feats = latent.shape
    crows = context.shape[0]
    heads = HEADS // n
    hk, hv = query_matrix.shape[0], value_matrix.shape[0]
    dv = hv // heads
    model = n * feats
    both = rows + crows
    inputs = conditioning.shape[0]
    parts = feats // 128
    hparts = hv // 128
    stat_width = -(-both // 128) * 128
    bf, f32 = jnp.bfloat16, jnp.float32
    vmem, dma = pltpu.VMEM, pltpu.SemaphoreType.DMA
    pair = lambda *k: [dma(k), dma(k)]
    scratch = [
        vmem((n * parts, both, 128), bf),
        vmem((both, feats), bf),
        vmem((both, 2 * hk + 2 * hv), f32),
        vmem((both, 2 * DECAY_RANK), f32),
        vmem((3, feats, inputs), bf),
        vmem((2 * hk + 2 * hv, model), bf),
        vmem((output_matrix.shape[0], model), bf),
        vmem((2 * DECAY_RANK, model), bf),
        vmem((2, DECAY_RANK, hk), bf),
        vmem((2, hk), f32),
        vmem((2, HEADS, rows), f32),
        vmem((1, hv), f32),
        vmem((2, inputs // 128, 128), bf),
        vmem((4, feats), f32),
        vmem((s - 1, 4, feats), f32),
        vmem((n, 4, feats), f32),
        vmem((2, feats), f32),
        vmem((s - 1, 2, feats), f32),
        vmem((n, 2, stat_width), f32),
        vmem((rows, 2 * hk), f32),
        vmem((both, 2 * hk + 2 * hv), bf),
        vmem((s * crows, hk + hv), bf),
        vmem((s * crows, 128), bf),
        vmem((2, hk), f32),
        vmem((s - 1, 2, hk), f32),
        vmem((2, hparts, DK, 128), bf),
        vmem((s - 1, hparts, DK, 128), bf),
        vmem((rows, hv), f32),
        vmem((n * hparts, rows, 128), bf),
        vmem((rows, feats), f32),
        dma((15 + 2 * parts,)),
    ]
    for counts in ((s - 1,), (n - 1,), (s - 1,), (n - 1,), (s - 1,), (s - 1,), (s - 1,), (s - 1, hparts)):
        scratch += pair(*counts)
    inner = 2 if n % 2 == 0 else 1
    line = n // inner
    hops = max(line - 1, 1)
    for pieces in (parts, hparts):
        for count in (hops, hops, 2 * line - 1, 1):
            scratch += pair(count, pieces)
    return pl.pallas_call(
        functools.partial(
            layer_kernel, n, s, inner, rows, crows, feats, heads, dv, parts, hparts
        ),
        out_shape=jax.ShapeDtypeStruct((rows, feats), bf),
        in_specs=[pl.BlockSpec(memory_space=pl.ANY)] * 17,
        out_specs=pl.BlockSpec(memory_space=pltpu.VMEM),
        scratch_shapes=scratch,
        compiler_params=pltpu.CompilerParams(
            collective_id=0, has_side_effects=True, vmem_limit_bytes=60 * 1024 * 1024
        ),
        name="layer",
    )(
        latent,
        context,
        conditioning.reshape(-1, 128),
        context_prompt_vector.reshape(-1, 128),
        shift_matrix,
        scale_matrix,
        residual_gate_matrix,
        query_matrix,
        key_matrix,
        value_matrix,
        gate_matrix,
        jnp.swapaxes(decay_down_factor, 1, 2).reshape(2 * DECAY_RANK, model),
        decay_up_factor,
        decay_key_bias,
        jnp.swapaxes(spike_log_decay, 1, 2),
        output_gain.reshape(1, -1),
        output_matrix,
    )


def solution(mesh):
    placed = (
        P("sp", "tp"),
        P("sp", "tp"),
        P("sp"),
        P("sp"),
        P("tp", "sp"),
        P("tp", "sp"),
        P("tp", "sp"),
        P("tp", None),
        P("tp", None),
        P("tp", None),
        P("tp", None),
        P(),
        P(),
        P(),
        P(None, "sp", None),
        P("tp"),
        P("tp", None),
    )
    whole_heads = HEADS % mesh.shape["tp"] == 0
    return jax.shard_map(
        one_kernel if whole_heads else local, mesh=mesh, in_specs=placed, out_specs=P("sp", "tp"), check_vma=False
    )
```

```python
import functools
import math

import jax
import jax.numpy as jnp
from jax import lax
from jax.experimental import pallas as pl
from jax.experimental.pallas import tpu as pltpu
from jax.sharding import PartitionSpec as P

D = 4096
HEADS = 16
DK = 128
DECAY_RANK = 16
BLK = 64
VGROUP = 64
MESH = pl.DeviceIdType.MESH


epsilon = 1e-05
gate_norm = 16.0
precise = lax.Precision.HIGHEST


def for_sending(value):

    def short(part):
        return part.astype(jnp.bfloat16) if part.dtype == jnp.float32 else part

    return jax.tree.map(short, value)


def from_partner(value, axis, distance):
    return lax.ppermute(value, axis, [(i, i ^ 1 << distance) for i in range(lax.axis_size(axis))])


def carried_in(value, axis, combine, identity, reverse):
    peers, index = (lax.axis_size(axis), lax.axis_index(axis))
    everything = jax.tree.map(
        lambda part, kind: lax.all_gather(part.astype(kind), axis),
        value,
        (jnp.bfloat16, jnp.bfloat16),
    )
    start = jax.tree.map(
        lambda part, zero: jnp.broadcast_to(jnp.asarray(zero, part.dtype), part.shape),
        value,
        identity,
    )

    def turn(k, before):
        at = peers - 1 - k if reverse else k
        reached = at > index if reverse else at < index
        new = combine(
            before, jax.tree.map(lambda part, own: part[at].astype(own.dtype), everything, value)
        )
        return jax.tree.map(lambda a, b: jnp.where(reached, a, b), new, before)

    return lax.fori_loop(0, peers, turn, start)


def linear(rows, weight):
    return lax.dot_general(
        rows, weight, (((1,), (1,)), ((), ())), preferred_element_type=jnp.float32
    )


def modulated(rows, row_sum, row_squares, shift_vec, scale_vec):
    rows_f = rows.astype(jnp.float32)
    mean_val = row_sum / D
    variance = row_squares / D - mean_val * mean_val
    return (
        (rows_f - mean_val) * lax.rsqrt(variance + epsilon) * (1.0 + scale_vec) + shift_vec
    ).astype(jnp.bfloat16)


def reverse_rows(array):
    return jnp.flip(array, axis=0)


def end_state(key_rows, value_rows, log_decay):
    cumulative = jnp.cumsum(log_decay, axis=0)
    totals = cumulative[-1]
    weighted = key_rows * jnp.exp(totals - cumulative)
    return (jnp.exp(totals), jnp.einsum("nhd,nhe->hde", weighted, value_rows, precision=precise))


def combine(earlier, later):
    return (earlier[0] * later[0], later[0][..., None] * earlier[1] + later[1])


def blockwise(queries, key_rows, value_rows, log_decay, carried, block_len):
    length, head_count, _ = queries.shape
    value_width = value_rows.shape[-1]
    blocks = length // block_len

    def shaped(array):
        return array.reshape(blocks, block_len, head_count, array.shape[-1])

    triangle = jnp.tril(jnp.ones((block_len, block_len), jnp.float32))

    def advance(state_now, inputs):
        block_q, block_k, block_v, block_a = inputs
        cumulative = jnp.cumsum(block_a, axis=0)
        block_end = cumulative[-1]
        query_dec = block_q * jnp.exp(cumulative)
        scores = (
            jnp.einsum("ihd,jhd->hij", query_dec, block_k * jnp.exp(-cumulative), precision=precise)
            * triangle
        )
        result = jnp.einsum("hij,jhe->ihe", scores, block_v, precision=precise)
        result = result + jnp.einsum("ihd,hde->ihe", query_dec, state_now, precision=precise)
        state_next = state_now * jnp.exp(block_end)[:, :, None] + jnp.einsum(
            "jhd,jhe->hde", block_k * jnp.exp(block_end - cumulative), block_v, precision=precise
        )
        return (state_next, result)

    _, outputs = lax.scan(
        advance, carried, (shaped(queries), shaped(key_rows), shaped(value_rows), shaped(log_decay))
    )
    return outputs.reshape(length, head_count, value_width)


def head_channels(pieces, per_head, tp_index):
    for bit_number in range(per_head.bit_length() - 1):
        partner = from_partner(
            (for_sending(pieces[0]), for_sending(pieces[1]), for_sending(pieces[2])),
            "tp",
            bit_number,
        )
        upper = tp_index // (1 << bit_number) % 2 == 1
        pieces = tuple(
            (
                jnp.where(
                    upper,
                    jnp.concatenate([theirs, mine], axis=1),
                    jnp.concatenate([mine, theirs], axis=1),
                )
                for mine, theirs in zip(pieces, partner)
            )
        )
    return pieces


def context_totals(fwd_growth, fwd_state, bwd_growth, bwd_state, identity):

    def absorb(carried, piece):
        return (combine(carried, piece), None)

    total_fwd, _ = lax.scan(absorb, identity, (fwd_growth, fwd_state))
    total_bwd, _ = lax.scan(absorb, identity, (bwd_growth, bwd_state), reverse=True)
    return (total_fwd, total_bwd)


def stored(array):
    return lax.optimization_barrier(array.astype(jnp.bfloat16))


def local(
    latent,
    context,
    conditioning,
    context_prompt_vector,
    shift_matrix,
    scale_matrix,
    residual_gate_matrix,
    query_matrix,
    key_matrix,
    value_matrix,
    gate_matrix,
    decay_down_factor,
    decay_up_factor,
    decay_key_bias,
    spike_log_decay,
    output_gain,
    output_matrix,
):
    tp_count = lax.axis_size("tp")
    tp_index = lax.axis_index("tp")
    per_head = max(tp_count // HEADS, 1)
    heads_per_shard = max(HEADS // tp_count, 1)
    leading_head = tp_index // per_head * heads_per_shard
    tok_rows = latent.shape[0]
    conds = jax.nn.silu(
        jnp.stack([conditioning, context_prompt_vector]).astype(jnp.float32)
    ).astype(jnp.bfloat16)
    shifts, scales, gates = lax.psum(
        (
            linear(conds, shift_matrix),
            linear(conds, scale_matrix),
            linear(conds, residual_gate_matrix),
        ),
        "sp",
    )
    down_both = jnp.concatenate([decay_down_factor[0].T, decay_down_factor[1].T], axis=0)
    lat_weights = (query_matrix, key_matrix, value_matrix, gate_matrix, down_both)
    ctx_weights = (key_matrix, value_matrix, down_both)
    lat_f = latent.astype(jnp.float32)
    ctx_f = context.astype(jnp.float32)
    lat_sum, lat_squares, ctx_sum, ctx_squares = lax.psum(
        (
            jnp.sum(lat_f, axis=1, keepdims=True),
            jnp.sum(lat_f * lat_f, axis=1, keepdims=True),
            jnp.sum(ctx_f, axis=1, keepdims=True),
            jnp.sum(ctx_f * ctx_f, axis=1, keepdims=True),
        ),
        "tp",
    )
    latent_normalized = modulated(latent, lat_sum, lat_squares, shifts[0], scales[0])
    normed_ctx = modulated(context, ctx_sum, ctx_squares, shifts[1], scales[1])
    lat_piece = lax.all_gather(latent_normalized, "tp", axis=1, tiled=True)
    ctx_piece = lax.all_gather(normed_ctx, "tp", axis=1, tiled=True)
    lat_new = tuple((linear(lat_piece, weight) for weight in lat_weights))
    ctx_new = tuple((linear(ctx_piece, weight) for weight in ctx_weights))
    query_part, key_part, value_part, gate_part, low_rank_part = lat_new
    ctx_key_part, ctx_value_part, ctx_low = ctx_new
    query_full, key_full, ctx_key_full = head_channels(
        (stored(query_part), stored(key_part), stored(ctx_key_part)), per_head, tp_index
    )

    def split_heads(rows, width):
        return rows.astype(jnp.float32).reshape(rows.shape[0], heads_per_shard, width)

    value_cols = value_part.shape[1] // heads_per_shard
    queries = split_heads(query_full, DK) * DK ** (-0.5)
    key_rows = split_heads(key_full, DK)
    ctx_keys = split_heads(ctx_key_full, DK)
    values_lat = split_heads(stored(value_part), value_cols)
    values_ctx = split_heads(stored(ctx_value_part), value_cols)
    gate_rows = stored(gate_part).astype(jnp.float32)

    def per_head_decay(low_rows, direction):
        up_part = lax.dynamic_slice_in_dim(
            decay_up_factor[direction], leading_head * DK, heads_per_shard * DK, 1
        ).astype(jnp.float32)
        bias_part = lax.dynamic_slice_in_dim(
            decay_key_bias[direction], leading_head * DK, heads_per_shard * DK, 0
        )
        pre_act = jnp.dot(low_rows, up_part, precision=precise) + bias_part
        return (jax.nn.log_sigmoid(pre_act) / gate_norm).reshape(
            low_rows.shape[0], heads_per_shard, DK
        )

    decay_spikes = lax.dynamic_slice_in_dim(spike_log_decay, leading_head, heads_per_shard, 2)
    latent_forward = per_head_decay(low_rank_part[:, :DECAY_RANK], 0) + decay_spikes[0][:, :, None]
    latent_backward = per_head_decay(low_rank_part[:, DECAY_RANK:], 1) + decay_spikes[1][:, :, None]
    ctx_fwd = per_head_decay(ctx_low[:, :DECAY_RANK], 0)
    ctx_bwd = per_head_decay(ctx_low[:, DECAY_RANK:], 1)
    cf_growth, cf_state = end_state(ctx_keys, values_ctx, ctx_fwd)
    cb_growth, cb_state = end_state(
        reverse_rows(ctx_keys), reverse_rows(values_ctx), reverse_rows(ctx_bwd)
    )
    lf_growth, lf_state = end_state(key_rows, values_lat, latent_forward)
    lb_growth, lb_state = end_state(
        reverse_rows(key_rows), reverse_rows(values_lat), reverse_rows(latent_backward)
    )
    identity = (
        jnp.ones((heads_per_shard, DK), jnp.float32),
        jnp.zeros((heads_per_shard, DK, value_cols), jnp.float32),
    )
    ctx_gathered = (
        lax.all_gather(cf_growth[None].astype(jnp.bfloat16), "sp", axis=0, tiled=True).astype(
            jnp.float32
        ),
        lax.all_gather(cf_state[None].astype(jnp.bfloat16), "sp", axis=0, tiled=True).astype(
            jnp.float32
        ),
        lax.all_gather(cb_growth[None].astype(jnp.bfloat16), "sp", axis=0, tiled=True).astype(
            jnp.float32
        ),
        lax.all_gather(cb_state[None].astype(jnp.bfloat16), "sp", axis=0, tiled=True).astype(
            jnp.float32
        ),
    )
    total_fwd, total_bwd = context_totals(
        ctx_gathered[0], ctx_gathered[1], ctx_gathered[2], ctx_gathered[3], identity
    )
    prefix = carried_in((lf_growth, lf_state), "sp", combine, identity, False)
    suffix = carried_in((lb_growth, lb_state), "sp", combine, identity, True)
    start_fwd = combine(total_fwd, prefix)[1]
    start_bwd = combine(total_bwd, suffix)[1]
    zero_state = jnp.zeros((heads_per_shard, DK, value_cols), jnp.float32)

    def direction_out(query_rows, key_list, value_list, log_decay, start_state):
        local_part = blockwise(query_rows, key_list, value_list, log_decay, zero_state, BLK)
        reach = query_rows * jnp.exp(jnp.cumsum(log_decay, axis=0))
        return local_part + jnp.einsum("nhd,hde->nhe", reach, start_state, precision=precise)

    out_fwd = direction_out(queries, key_rows, values_lat, latent_forward, start_fwd)
    out_bwd = reverse_rows(
        direction_out(
            reverse_rows(queries),
            reverse_rows(key_rows),
            reverse_rows(values_lat),
            reverse_rows(latent_backward),
            start_bwd,
        )
    )
    grouped = (out_fwd + out_bwd).reshape(tok_rows, -1, VGROUP)
    grouped = grouped * lax.rsqrt(jnp.mean(grouped * grouped, axis=-1, keepdims=True) + epsilon)
    heads_out = (grouped.reshape(tok_rows, -1) * output_gain * jax.nn.silu(gate_rows)).astype(
        jnp.bfloat16
    )
    branch = linear(lax.all_gather(heads_out, "tp", axis=1, tiled=True), output_matrix)
    return (latent.astype(jnp.float32) + gates[0] * branch).astype(jnp.bfloat16)


def exact(a, b):
    return lax.dot_general(
        a, b, (((1,), (0,)), ((), ())), precision=precise, preferred_element_type=jnp.float32
    )


def nt(a, b):
    return lax.dot_general(a, b, (((1,), (1,)), ((), ())), preferred_element_type=jnp.float32)


def nn(a, b):
    return lax.dot_general(a, b, (((1,), (0,)), ((), ())), preferred_element_type=jnp.float32)


def tn(a, b):
    return lax.dot_general(a, b, (((0,), (0,)), ((), ())), preferred_element_type=jnp.float32)


def short(value):
    return value.astype(jnp.bfloat16)


def terms(value):
    first = short(value)
    rest = value - first.astype(jnp.float32)
    second = short(rest)
    return first, second, short(rest - second.astype(jnp.float32))


def log_sigmoid(pre):
    return (jnp.minimum(pre, 0.0) - jnp.log1p(jnp.exp(-jnp.abs(pre)))) / gate_norm


def triangle_of(size, upper):
    i = lax.broadcasted_iota(jnp.int32, (size, size), 0)
    j = lax.broadcasted_iota(jnp.int32, (size, size), 1)
    return (j >= i) if upper else (j <= i)


def layer_kernel(
    n,
    s,
    inner,
    rows,
    crows,
    feats,
    heads,
    dv,
    parts,
    hparts,
    latent,
    context,
    conditioning,
    prompt,
    shift_m,
    scale_m,
    gate_m,
    query_m,
    key_m,
    value_m,
    og_m,
    down,
    up,
    bias,
    spike,
    gain,
    out_m,
    out_ref,
    x_all,
    xn,
    acc,
    low_acc,
    mod_w,
    proj_w,
    out_w,
    down_v,
    up_v,
    bias_v,
    spike_v,
    gain_v,
    cond_v,
    mod_own,
    mod_recv,
    mod_all,
    gate_own,
    gate_recv,
    stat_all,
    spike_rows,
    proj,
    ctx_kv,
    ctx_low,
    tot_own,
    tot_recv,
    st_own,
    st_recv,
    local_out,
    ho_all,
    total_out,
    load_sem,
    x_send,
    x_recv,
    *gather_sems,
):
    me = lax.axis_index("tp")
    sp = lax.axis_index("sp")
    hk = heads * DK
    hv = heads * dv
    model = n * feats
    both = rows + crows
    width = feats // parts
    hwidth = hv // hparts
    f32 = jnp.float32

    used = [0]

    def load(*pairs, whole):
        sem = load_sem.at[used[0]]
        used[0] += 1
        for src, dst in pairs:
            pltpu.make_async_copy(src, dst, sem).start()
        return pltpu.make_async_copy(whole, whole, sem)

    def own_piece(p):
        cols = pl.ds(p * width, width)
        return (
            (latent.at[:, cols], x_all.at[me * parts + p, pl.ds(0, rows)]),
            (context.at[:, cols], x_all.at[me * parts + p, pl.ds(rows, crows)]),
        )

    own_x = [load(*own_piece(0), whole=x_all.at[pl.ds(me * parts, 1)])]
    if parts > 1:
        own_x.append(
            load(
                *[c for p in range(1, parts) for c in own_piece(p)],
                whole=x_all.at[pl.ds(me * parts + 1, parts - 1)],
            )
        )
    first = [
        load((conditioning, cond_v.at[0]), (prompt, cond_v.at[1]), whole=cond_v),
        load((shift_m, mod_w.at[0]), (scale_m, mod_w.at[1]), whole=mod_w.at[pl.ds(0, 2)]),
    ]
    gate_load = load((gate_m, mod_w.at[2]), whole=mod_w.at[2])
    head_cols = pl.ds(pl.multiple_of(me * hk, hk), hk)
    small = [
        load((up.at[:, :, head_cols], up_v), whole=up_v),
        load((bias.at[:, head_cols], bias_v), whole=bias_v),
        load((spike, spike_v), whole=spike_v),
        load((gain, gain_v), whole=gain_v),
    ]
    weights = [
        load(
            (query_m, proj_w.at[pl.ds(0, hk)]),
            (key_m, proj_w.at[pl.ds(hk, hk)]),
            (value_m, proj_w.at[pl.ds(2 * hk, hv)]),
            (og_m, proj_w.at[pl.ds(2 * hk + hv, hv)]),
            whole=proj_w,
        ),
        load((down, down_v), whole=down_v),
    ]
    last = load((out_m, out_w), whole=out_w)

    barrier = pltpu.get_barrier_semaphore()
    for d in range(1, n):
        pl.semaphore_signal(
            barrier, inc=1, device_id={"tp": lax.rem(me + d, n)}, device_id_type=MESH
        )
    for d in range(1, s):
        pl.semaphore_signal(
            barrier, inc=1, device_id={"sp": lax.rem(sp + d, s)}, device_id_type=MESH
        )
    pl.semaphore_wait(barrier, n - 1 + s - 1)

    started = []

    class Exchange:
        def __init__(self, axis, index, src, dst, landed, send_index=None, sent=True):
            at, count = (me, n) if axis == "tp" else (sp, s)
            self.some = count > 1

            def copy(source, target, d):
                return pltpu.make_async_remote_copy(
                    src_ref=source,
                    dst_ref=target,
                    send_sem=x_send.at[index if send_index is None else send_index],
                    recv_sem=x_recv.at[index],
                    device_id={axis: lax.rem(at + d, count)},
                    device_id_type=MESH,
                )

            for d in range(1, count):
                copy(src(d), dst(d), d).start()
            if self.some:
                self.all = copy(landed, landed, 1)
                if sent:
                    started.append(self.all)

        def wait_recv(self):
            if self.some:
                self.all.wait_recv()

    line = n // inner
    z, y = lax.div(me, inner), lax.rem(me, inner)
    mate = z + 1 - 2 * lax.rem(z, 2)
    paired = inner > 1 and line % 2 == 0
    at_end = (z == 0) | (z == line - 1)

    def level(i):
        table = []
        for at in range(line):
            order = [at]
            for k in range(1, line):
                order += [b for b in (at - k, at + k) if 0 <= b < line]
            table.append(order[i])
        return sum(jnp.where(z == at, table[at], 0) for at in range(line))

    def block_of(at, column):
        return at * inner + column

    class Gather:
        def __init__(self, ref, pieces, sems):
            self.ref, self.pieces = ref, pieces
            self.column_send, self.across_send, self.column_recv, self.across_recv = sems
            self.half = max(pieces // 2, 1)
            self.turned = tuple(range(pieces // 2, pieces)) if paired else ()

        def remote(self, ref, send_sem, recv_sem, target):
            return pltpu.make_async_remote_copy(
                src_ref=ref,
                dst_ref=ref,
                send_sem=send_sem,
                recv_sem=recv_sem,
                device_id={"tp": target},
                device_id_type=MESH,
            )

        def along(self, at, piece, to):
            return self.remote(
                self.ref.at[block_of(at, y) * self.pieces + piece],
                self.column_send.at[0],
                self.column_recv.at[lax.rem(at - to + line, line) - 1, piece],
                block_of(to, y),
            )

        def across(self, at, column, piece, target):
            return self.remote(
                self.ref.at[block_of(at, column) * self.pieces + piece],
                self.across_send.at[0],
                self.across_recv.at[at, piece // self.half],
                target,
            )

        def lane_sends(self, lane, k, piece, act):
            up = lane == "up"
            at, has = (z - k, z >= k) if up else (z + k, z + k < line)
            if k < line - 1:
                onward, to = (z + 1 < line, z + 1) if up else (z > 0, z - 1)
                pl.when(has & onward)(lambda: act(self.along(at, piece, to)))
            if inner > 1 and (k > 0 or up):
                if k == 1 and piece in self.turned:
                    has = has & (lax.rem(z, 2) == (0 if up else 1))
                pl.when(has)(
                    lambda: act(self.across(at, y, piece, block_of(z, inner - 1 - y)))
                )

        def start(self, piece):
            for lane in ("up", "down"):
                self.lane_sends(lane, 0, piece, lambda c: c.start())

        def take(self, lane, k, piece):
            at, has = (z - k, z >= k) if lane == "up" else (z + k, z + k < line)
            pl.when(has)(lambda: self.along(at, piece, z).wait_recv())
            self.lane_sends(lane, k, piece, lambda c: c.start())

        def near(self, k, piece):
            pl.when(z >= line // 2)(lambda: self.take("up", k, piece))
            pl.when(z < line // 2)(lambda: self.take("down", k, piece))

        def far(self, k, piece):
            pl.when(z < line // 2)(lambda: self.take("up", k, piece))
            pl.when(z >= line // 2)(lambda: self.take("down", k, piece))

        def side_start(self, when, piece):
            pl.when(when)(
                lambda: self.across(z, inner - 1 - y, piece, block_of(mate, y)).start()
            )

        def arrive(self, i, half):
            at = level(i)
            block = block_of(at, inner - 1 - y)
            self.remote(
                self.ref.at[pl.ds(block * self.pieces + half * self.half, self.half)],
                self.across_send.at[0],
                self.across_recv.at[at, half],
                block,
            ).wait_recv()

        def drain(self):
            def sent(count, sem):
                self.remote(
                    self.ref.at[pl.ds(0, count * self.pieces)],
                    sem.at[0],
                    self.across_recv.at[0, 0],
                    block_of(z, inner - 1 - y),
                ).wait_send()

            if line > 1:
                pl.when(at_end)(lambda: sent(1, self.column_send))
            if line > 2:
                pl.when(jnp.logical_not(at_end))(lambda: sent(line + 1, self.column_send))
            if inner > 1:
                sent(line, self.across_send)

    def run(events):
        for _, act in sorted(enumerate(events), key=lambda e: (e[1][0], e[0])):
            act[1]()

    xg = Gather(x_all, parts, gather_sems[:4])
    hg = Gather(ho_all, hparts, gather_sems[4:])

    own_x[0].wait()
    xg.start(0)
    for copy in own_x[1:]:
        copy.wait()

    ones = jnp.ones((16, width), jnp.bfloat16)
    row_sum = jnp.zeros((16, both), f32)
    row_squares = jnp.zeros((16, both), f32)
    for p in range(parts):
        own = x_all[me * parts + p]
        own_f = own.astype(f32)
        row_sum = row_sum + nt(ones, own)
        for part in terms(own_f * own_f):
            row_squares = row_squares + nt(ones, part)
    stat_all[me] = jnp.zeros(stat_all.shape[1:], f32)
    stat_all[me, 0:1, 0:both] = row_sum[0:1]
    stat_all[me, 1:2, 0:both] = row_squares[0:1]
    sa = Exchange(
        "tp",
        3,
        lambda d: stat_all.at[me],
        lambda d: stat_all.at[me],
        stat_all.at[pl.ds(0, n - 1)],
    )
    for p in range(1, parts):
        xg.start(p)

    for copy in first:
        copy.wait()

    def one_row(which):
        part = cond_v[which].astype(f32)
        return jnp.concatenate([part[r : r + 1] for r in range(part.shape[0])], axis=1)

    row_of = lax.broadcasted_iota(jnp.int32, (16, shift_m.shape[1]), 0)
    conds = jnp.where(row_of == 0, one_row(0), one_row(1))
    conds = short(conds * lax.logistic(conds))
    for which in range(2):
        mod_own[2 * which : 2 * which + 2, :] = nt(conds, mod_w[which])[0:2]
    m1 = Exchange("sp", 0, lambda d: mod_own, lambda d: mod_recv.at[d - 1], mod_recv)
    held = {}

    def send_mods():
        m1.wait_recv()
        total = mod_own[...]
        for d in range(1, s):
            total = total + mod_recv[d - 1]
        mod_all[me] = total
        held["m2"] = Exchange(
            "tp",
            1,
            lambda d: mod_all.at[me],
            lambda d: mod_all.at[me],
            mod_all.at[pl.ds(0, n - 1)],
        )

    def send_gates():
        gate_load.wait()
        gate_own[...] = nt(conds, mod_w[2])[0:2]
        held["mg"] = Exchange(
            "sp", 2, lambda d: gate_own, lambda d: gate_recv.at[d - 1], gate_recv
        )

    def early():
        for copy in small:
            copy.wait()
        slot_head = lax.broadcasted_iota(jnp.int32, (spike_v.shape[1], hk), 0)
        lane_head = lax.broadcasted_iota(jnp.int32, (spike_v.shape[1], hk), 1) // DK
        pick = jnp.where(slot_head == me * heads + lane_head, 1.0, 0.0).astype(jnp.bfloat16)
        for e in range(2):
            spike_rows[:, e * hk : (e + 1) * hk] = sum(
                tn(part, pick) for part in terms(spike_v[e])
            )
        acc[...] = jnp.zeros(acc.shape, f32)
        low_acc[...] = jnp.zeros(low_acc.shape, f32)

    def moments():
        sa.wait_recv()
        stats = sum(stat_all[b] for b in range(n))
        diagonal = lax.broadcasted_iota(jnp.int32, (both, both), 0) == lax.broadcasted_iota(
            jnp.int32, (both, both), 1
        )

        def column_of(row):
            return (
                jnp.sum(
                    jnp.where(diagonal, stats[row : row + 1, 0:both], 0.0), axis=1, keepdims=True
                )
                / model
            )

        mean = column_of(0)
        held["mean"] = mean
        held["spread"] = lax.rsqrt(column_of(1) - mean * mean + epsilon)

    def wait_mods():
        held["m2"].wait_recv()
        for copy in weights:
            copy.wait()

    tile = math.gcd(2 * hk + 2 * hv, 512)
    columns = acc.shape[1]

    def project_block(block):
        cols = pl.ds(pl.multiple_of(block * feats, feats), feats)
        mean, spread = held["mean"], held["spread"]
        mod = mod_all[block]
        for p in range(parts):
            lanes = slice(p * width, (p + 1) * width)
            x = (x_all[block * parts + p].astype(f32) - mean) * spread
            m = mod[:, lanes]
            xn[0:rows, lanes] = short(x[0:rows] * (1.0 + m[2:3]) + m[0:1])
            xn[rows:, lanes] = short(x[rows:] * (1.0 + m[3:4]) + m[1:2])
        low_acc[...] += nt(xn[...], down_v[:, cols])
        for t in range(columns // tile):
            out = slice(t * tile, (t + 1) * tile)
            acc[:, out] += nt(xn[...], proj_w[out, cols])

    def column_block(i):
        project_block(block_of(level(i), y))

    def other_block(i):
        if i > 0:
            for half in range(min(parts, 2)):
                xg.arrive(i, half)
        project_block(block_of(level(i), inner - 1 - y))

    unit, lag, cost = 0.79, 2.0, 0.6
    arrival = lambda k, p: unit * ((k - 1) * parts + p + 1) + lag
    mods_at = 9.4
    events = [
        (arrival(1, parts // 2 - 1) + 0.01, send_mods),
        (arrival(1, parts // 2 - 1) + 0.02, send_gates),
        (arrival(1, parts - 1) + 0.05, early),
        (arrival(1, parts - 1) + 0.06, moments),
        (mods_at, wait_mods),
    ]
    for k in range(1, line):
        for p in range(parts):
            events.append((arrival(k, p), functools.partial(xg.near, k, p)))
            if 2 * k < line + line % 2:
                events.append((arrival(k, p) + 0.005, functools.partial(xg.far, k, p)))
    if inner > 1:
        for half in range(min(parts, 2)):
            when = arrival(1, (half + 1) * xg.half - 1)
            events.append((when + 0.03, functools.partial(xg.arrive, 0, half)))
        for p in xg.turned:
            when = arrival(1, parts - 1)
            events.append((when + 0.04, functools.partial(xg.side_start, at_end, p)))
            if line > 2:
                when = arrival(line - 2, parts - 1)
                events.append(
                    (
                        when + 0.01,
                        functools.partial(xg.side_start, jnp.logical_not(at_end), p),
                    )
                )
    tasks = []
    for i in range(line):
        ready = arrival(i, parts - 1) + 0.02 if i else 0.0
        tasks.append((ready, functools.partial(column_block, i)))
        if inner > 1:
            ready = arrival(max(i, 1), parts - 1) + 0.05 + (lag if i else 0)
            if i == 1 and xg.turned:
                ready = max(ready, arrival(line - 1, parts - 1) + unit * len(xg.turned))
            tasks.append((ready, functools.partial(other_block, i)))
    clock = mods_at + 0.01
    for ready, task in sorted(tasks, key=lambda t: t[0]):
        clock = max(clock, ready)
        events.append((clock, task))
        clock += cost
    run(events)
    proj[...] = short(acc[...])

    own_ctx = pl.ds(pl.multiple_of(sp * crows, crows), crows)
    ctx_kv[own_ctx, :] = proj[rows:, hk : 2 * hk + hv]
    ctx_low[own_ctx, :] = jnp.zeros((crows, ctx_low.shape[1]), jnp.bfloat16)
    for i, part in enumerate(terms(low_acc[rows:])):
        ctx_low[own_ctx, i * 2 * DECAY_RANK : (i + 1) * 2 * DECAY_RANK] = part
    lo = Exchange(
        "sp",
        5,
        lambda d: ctx_low.at[own_ctx],
        lambda d: ctx_low.at[own_ctx],
        ctx_low.at[pl.ds(0, (s - 1) * crows)],
    )
    kv = Exchange(
        "sp",
        4,
        lambda d: ctx_kv.at[own_ctx],
        lambda d: ctx_kv.at[own_ctx],
        ctx_kv.at[pl.ds(0, (s - 1) * crows)],
    )

    none = jnp.zeros((DECAY_RANK, hk), jnp.bfloat16)
    up_both = jnp.concatenate(
        [
            jnp.concatenate([up_v[0], none], axis=1),
            jnp.concatenate([none, up_v[1]], axis=1),
        ],
        axis=0,
    )
    bias_both = jnp.concatenate([bias_v[0:1], bias_v[1:2]], axis=1)

    def logs_of(parts_of_low):
        return log_sigmoid(sum(nn(part, up_both) for part in parts_of_low) + bias_both)

    def running(logs, length, e):
        lanes = slice(e * hk, (e + 1) * hk)
        mask = jnp.where(triangle_of(length, e == 1), 1.0, 0.0).astype(jnp.bfloat16)
        return sum(nn(mask, part) for part in terms(logs[:, lanes]))

    logs = logs_of(terms(low_acc[0:rows])) + spike_rows[...]
    cum = [running(logs, rows, e) for e in range(2)]
    whole = [cum[0][rows - 1 : rows], cum[1][0:1]]
    tot_own[0:1, :] = whole[0]
    tot_own[1:2, :] = whole[1]
    to = Exchange("sp", 6, lambda d: tot_own, lambda d: tot_recv.at[d - 1], tot_recv)

    keys = proj[0:rows, hk : 2 * hk].astype(f32)
    per = hparts // heads
    weighted = [short(keys * jnp.exp(whole[e] - cum[e])) for e in range(2)]
    st = []
    for h in range(heads):
        for e in range(2):
            state = short(
                tn(
                    weighted[e][:, h * DK : (h + 1) * DK],
                    proj[0:rows, 2 * hk + h * dv : 2 * hk + (h + 1) * dv],
                )
            )
            for q in range(per):
                st_own[e, h * per + q] = state[:, q * hwidth : (q + 1) * hwidth]
        for q in range(h * per, (h + 1) * per):
            st.append(
                Exchange(
                    "sp",
                    7 + q,
                    lambda d: st_own.at[jnp.where(lax.rem(sp + d, s) > sp, 0, 1), q],
                    lambda d: st_recv.at[d - 1, q],
                    st_recv.at[:, q],
                    7,
                    False,
                )
            )

    queries = proj[0:rows, 0:hk].astype(f32) * DK ** (-0.5)
    blocks = rows // BLK

    def span(b):
        return slice(b * BLK, (b + 1) * BLK)

    inside = [[], []]
    for b in range(blocks):
        f = cum[0][span(b)]
        inside[0].append(f if b == 0 else f - cum[0][b * BLK - 1 : b * BLK])
        f = cum[1][span(b)]
        inside[1].append(
            f if b == blocks - 1 else f - cum[1][(b + 1) * BLK : (b + 1) * BLK + 1]
        )
    ends = [[part[BLK - 1 : BLK] for part in inside[0]], [part[0:1] for part in inside[1]]]
    q_dec = [[short(queries[span(b)] * jnp.exp(inside[e][b])) for b in range(blocks)] for e in range(2)]
    k_dec = [[short(keys[span(b)] * jnp.exp(-inside[e][b])) for b in range(blocks)] for e in range(2)]
    k_end = [
        [short(keys[span(b)] * jnp.exp(ends[e][b] - inside[e][b])) for b in range(blocks)]
        for e in range(2)
    ]
    lower, upper = triangle_of(BLK, False), triangle_of(BLK, True)
    scores = []
    for h in range(heads):
        ch = slice(h * DK, (h + 1) * DK)
        lines = []
        for b in range(blocks):
            strip = []
            for c in range(blocks):
                if b == c:
                    strip.append(
                        jnp.where(lower, nt(q_dec[0][b][:, ch], k_dec[0][b][:, ch]), 0.0)
                        + jnp.where(upper, nt(q_dec[1][b][:, ch], k_dec[1][b][:, ch]), 0.0)
                    )
                    continue
                e = 0 if c < b else 1
                near = q_dec[e][b][:, ch]
                between = range(c + 1, b) if c < b else range(b + 1, c)
                if len(between) > 0:
                    gap = sum(ends[e][m][:, ch] for m in between)
                    near = short(queries[span(b)][:, ch] * jnp.exp(inside[e][b][:, ch] + gap))
                strip.append(nt(near, k_end[e][c][:, ch]))
            lines.append(jnp.concatenate(strip, axis=1) if blocks > 1 else strip[0])
        scores.append(short(jnp.concatenate(lines, axis=0) if blocks > 1 else lines[0]))

    lo.wait_recv()
    low_parts = [
        ctx_low[:, i * 2 * DECAY_RANK : (i + 1) * 2 * DECAY_RANK] for i in range(3)
    ]
    ctx_logs = logs_of(low_parts)
    length = s * crows
    ctx_decay = []
    for e in range(2):
        c = running(ctx_logs, length, e)
        end = c[length - 1 : length] if e == 0 else c[0:1]
        ctx_decay.append(jnp.exp(end - c))

    kv.wait_recv()
    ctx_keys = ctx_kv[:, 0:hk].astype(f32)
    ctx_weighted = [short(ctx_keys * part) for part in ctx_decay]
    ctx_states = [
        [
            short(tn(w[:, h * DK : (h + 1) * DK], ctx_kv[:, hk + h * dv : hk + (h + 1) * dv]))
            for w in ctx_weighted
        ]
        for h in range(heads)
    ]
    to.wait_recv()
    places = {d: lax.rem(sp - d + s, s) for d in range(1, s)}

    def passed(low_end, high_end, direction):
        result = jnp.zeros((1, hk), f32)
        for d in range(1, s):
            inside_it = jnp.where((places[d] > low_end) & (places[d] < high_end), 1.0, 0.0)
            result = result + inside_it * tot_recv[d - 1][direction : direction + 1]
        return result

    ctx_reach = [
        short(queries * jnp.exp(cum[0] + passed(-1, sp, 0))),
        short(queries * jnp.exp(cum[1] + passed(sp, s, 1))),
    ]
    reach = []
    for d in range(1, s):
        p = places[d]
        before = jnp.where(p < sp, 1.0, 0.0)
        exponent = before * (cum[0] + passed(p, sp, 0)) + (1.0 - before) * (
            cum[1] + passed(sp, p, 1)
        )
        reach.append(short(queries * jnp.exp(exponent)))
    gate_rows = proj[0:rows, 2 * hk + hv :].astype(f32)
    small_gate = gate_rows * lax.logistic(gate_rows) * gain_v[...]

    for h in range(heads):
        ch = slice(h * DK, (h + 1) * DK)
        vc = slice(h * dv, (h + 1) * dv)
        local_out[:, vc] = nn(
            jnp.concatenate([scores[h]] + [r[:, ch] for r in ctx_reach], axis=1),
            jnp.concatenate(
                [proj[0:rows, 2 * hk + h * dv : 2 * hk + (h + 1) * dv]]
                + ctx_states[h],
                axis=0,
            ),
        )
    gi = lax.broadcasted_iota(jnp.int32, (hwidth, hwidth), 0) // VGROUP
    gj = lax.broadcasted_iota(jnp.int32, (hwidth, hwidth), 1) // VGROUP
    group = jnp.where(gi == gj, 1.0, 0.0).astype(jnp.bfloat16)

    def head_piece(q):
        h = q // per
        ch = slice(h * DK, (h + 1) * DK)
        vc = slice(q * hwidth, (q + 1) * hwidth)
        st[q].wait_recv()
        o = local_out[:, vc] + nn(
            jnp.concatenate([r[:, ch] for r in reach], axis=1),
            jnp.concatenate([st_recv[d - 1, q] for d in range(1, s)], axis=0),
        )
        squares = o * o
        top = short(squares)
        rest = short(squares - top.astype(f32))
        power = (nn(top, group) + nn(rest, group)) * (1.0 / VGROUP)
        ho_all[me * hparts + q] = short(o * lax.rsqrt(power + epsilon) * small_gate[:, vc])
        hg.start(q)

    def ready_out():
        last.wait()
        held["mg"].wait_recv()
        total_out[...] = jnp.zeros(total_out.shape, f32)

    def add_half(block, half):
        cols = pl.ds(pl.multiple_of(block * feats + half * 2 * hwidth, 2 * hwidth), 2 * hwidth)
        pair = jnp.concatenate(
            [ho_all[block * hparts + 2 * half], ho_all[block * hparts + 2 * half + 1]], axis=1
        )
        total_out[...] += nt(pair, out_w[:, cols])

    def add_column(i, half):
        add_half(block_of(level(i), y), half)

    def add_other(i, half):
        if i > 0:
            hg.arrive(i, half)
        add_half(block_of(level(i), inner - 1 - y), half)

    hop_h = 2.6
    here = lambda k, q: 0.4 * q + 0.4 * (q // 2) + hop_h * k
    events = [(here(0, 1) + 0.01, ready_out)]
    for q in range(hparts):
        events.append((here(0, q), functools.partial(head_piece, q)))
        for k in range(1, line):
            events.append((here(k, q), functools.partial(hg.near, k, q)))
            if 2 * k < line + line % 2:
                events.append((here(k, q) + 0.5, functools.partial(hg.far, k, q)))
        if q in hg.turned:
            when = here(1, hparts - 1) + 0.03
            events.append((when, functools.partial(hg.side_start, at_end, q)))
            if line > 2:
                when = here(line - 2, q) + 0.03
                events.append(
                    (when, functools.partial(hg.side_start, jnp.logical_not(at_end), q))
                )
    if inner > 1:
        for half in range(2):
            when = here(1, (half + 1) * hg.half - 1) + 0.02
            events.append((when, functools.partial(hg.arrive, 0, half)))
    for i in range(line):
        for half in range(hparts // 2):
            when = here(i, 2 * half + 1) + 0.6
            events.append((when, functools.partial(add_column, i, half)))
            if inner > 1:
                when += hop_h + 0.1
                if i == 1 and 2 * half in hg.turned:
                    when = max(when, here(line - 1, 2 * half + 1) + 0.4)
                events.append((when, functools.partial(add_other, i, half)))
    run(events)
    gates = gate_own[0:1]
    for d in range(1, s):
        gates = gates + gate_recv[d - 1, 0:1]
    for p in range(parts):
        lanes = slice(p * width, (p + 1) * width)
        out_ref[:, lanes] = short(
            x_all[me * parts + p, 0:rows].astype(f32) + gates[:, lanes] * total_out[:, lanes]
        )
    for copy in started:
        copy.wait_send()
    if s > 1:
        pltpu.make_async_remote_copy(
            src_ref=st_recv,
            dst_ref=st_recv,
            send_sem=x_send.at[7],
            recv_sem=x_recv.at[7],
            device_id={"sp": lax.rem(sp + 1, s)},
            device_id_type=MESH,
        ).wait_send()
    xg.drain()
    hg.drain()


def one_kernel(
    latent,
    context,
    conditioning,
    context_prompt_vector,
    shift_matrix,
    scale_matrix,
    residual_gate_matrix,
    query_matrix,
    key_matrix,
    value_matrix,
    gate_matrix,
    decay_down_factor,
    decay_up_factor,
    decay_key_bias,
    spike_log_decay,
    output_gain,
    output_matrix,
):
    n, s = lax.axis_size("tp"), lax.axis_size("sp")
    rows, feats = latent.shape
    crows = context.shape[0]
    heads = HEADS // n
    hk, hv = query_matrix.shape[0], value_matrix.shape[0]
    dv = hv // heads
    model = n * feats
    both = rows + crows
    inputs = conditioning.shape[0]
    parts = feats // 128
    hparts = hv // 128
    stat_width = -(-both // 128) * 128
    bf, f32 = jnp.bfloat16, jnp.float32
    vmem, dma = pltpu.VMEM, pltpu.SemaphoreType.DMA
    scratch = [
        vmem((n * parts, both, 128), bf),
        vmem((both, feats), bf),
        vmem((both, 2 * hk + 2 * hv), f32),
        vmem((both, 2 * DECAY_RANK), f32),
        vmem((3, feats, inputs), bf),
        vmem((2 * hk + 2 * hv, model), bf),
        vmem((output_matrix.shape[0], model), bf),
        vmem((2 * DECAY_RANK, model), bf),
        vmem((2, DECAY_RANK, hk), bf),
        vmem((2, hk), f32),
        vmem((2, HEADS, rows), f32),
        vmem((1, hv), f32),
        vmem((2, inputs // 128, 128), bf),
        vmem((4, feats), f32),
        vmem((s - 1, 4, feats), f32),
        vmem((n, 4, feats), f32),
        vmem((2, feats), f32),
        vmem((s - 1, 2, feats), f32),
        vmem((n, 2, stat_width), f32),
        vmem((rows, 2 * hk), f32),
        vmem((both, 2 * hk + 2 * hv), bf),
        vmem((s * crows, hk + hv), bf),
        vmem((s * crows, 128), bf),
        vmem((2, hk), f32),
        vmem((s - 1, 2, hk), f32),
        vmem((2, hparts, DK, 128), bf),
        vmem((s - 1, hparts, DK, 128), bf),
        vmem((rows, hv), f32),
        vmem((n * hparts, rows, 128), bf),
        vmem((rows, feats), f32),
        dma((12,)),
        dma((8,)),
        dma((7 + hparts,)),
    ]
    inner = 2 if n % 2 == 0 else 1
    line = n // inner
    hops = max(line - 1, 1)
    for pieces in (parts, hparts):
        scratch += [dma((1,)), dma((1,)), dma((hops, pieces)), dma((line, min(pieces, 2)))]
    return pl.pallas_call(
        functools.partial(
            layer_kernel, n, s, inner, rows, crows, feats, heads, dv, parts, hparts
        ),
        out_shape=pltpu.VMEM((rows, feats), bf),
        in_specs=[pl.BlockSpec(memory_space=pl.ANY)] * 17,
        out_specs=pl.BlockSpec(memory_space=pltpu.VMEM),
        scratch_shapes=scratch,
        compiler_params=pltpu.CompilerParams(
            collective_id=0, has_side_effects=True, vmem_limit_bytes=60 * 1024 * 1024
        ),
        name="layer",
    )(
        latent,
        context,
        conditioning.reshape(-1, 128),
        context_prompt_vector.reshape(-1, 128),
        shift_matrix,
        scale_matrix,
        residual_gate_matrix,
        query_matrix,
        key_matrix,
        value_matrix,
        gate_matrix,
        jnp.swapaxes(decay_down_factor, 1, 2).reshape(2 * DECAY_RANK, model),
        decay_up_factor,
        decay_key_bias,
        jnp.swapaxes(spike_log_decay, 1, 2),
        output_gain.reshape(1, -1),
        output_matrix,
    )


def solution(mesh):
    placed = (
        P("sp", "tp"),
        P("sp", "tp"),
        P("sp"),
        P("sp"),
        P("tp", "sp"),
        P("tp", "sp"),
        P("tp", "sp"),
        P("tp", None),
        P("tp", None),
        P("tp", None),
        P("tp", None),
        P(),
        P(),
        P(),
        P(None, "sp", None),
        P("tp"),
        P("tp", None),
    )
    whole_heads = HEADS == 2 * mesh.shape["tp"]
    return jax.shard_map(
        one_kernel if whole_heads else local, mesh=mesh, in_specs=placed, out_specs=P("sp", "tp"), check_vma=False
    )
```

```python
import functools
import math

import jax
import jax.numpy as jnp
from jax import lax
from jax.experimental import pallas as pl
from jax.experimental.pallas import tpu as pltpu
from jax.sharding import PartitionSpec as P

D = 4096
HEADS = 16
DK = 128
DECAY_RANK = 16
BLK = 64
VGROUP = 64
MESH = pl.DeviceIdType.MESH


epsilon = 1e-05
gate_norm = 16.0
precise = lax.Precision.HIGHEST


def for_sending(value):

    def short(part):
        return part.astype(jnp.bfloat16) if part.dtype == jnp.float32 else part

    return jax.tree.map(short, value)


def from_partner(value, axis, distance):
    return lax.ppermute(value, axis, [(i, i ^ 1 << distance) for i in range(lax.axis_size(axis))])


def carried_in(value, axis, combine, identity, reverse):
    peers, index = (lax.axis_size(axis), lax.axis_index(axis))
    everything = jax.tree.map(
        lambda part, kind: lax.all_gather(part.astype(kind), axis),
        value,
        (jnp.bfloat16, jnp.bfloat16),
    )
    start = jax.tree.map(
        lambda part, zero: jnp.broadcast_to(jnp.asarray(zero, part.dtype), part.shape),
        value,
        identity,
    )

    def turn(k, before):
        at = peers - 1 - k if reverse else k
        reached = at > index if reverse else at < index
        new = combine(
            before, jax.tree.map(lambda part, own: part[at].astype(own.dtype), everything, value)
        )
        return jax.tree.map(lambda a, b: jnp.where(reached, a, b), new, before)

    return lax.fori_loop(0, peers, turn, start)


def linear(rows, weight):
    return lax.dot_general(
        rows, weight, (((1,), (1,)), ((), ())), preferred_element_type=jnp.float32
    )


def modulated(rows, row_sum, row_squares, shift_vec, scale_vec):
    rows_f = rows.astype(jnp.float32)
    mean_val = row_sum / D
    variance = row_squares / D - mean_val * mean_val
    return (
        (rows_f - mean_val) * lax.rsqrt(variance + epsilon) * (1.0 + scale_vec) + shift_vec
    ).astype(jnp.bfloat16)


def reverse_rows(array):
    return jnp.flip(array, axis=0)


def end_state(key_rows, value_rows, log_decay):
    cumulative = jnp.cumsum(log_decay, axis=0)
    totals = cumulative[-1]
    weighted = key_rows * jnp.exp(totals - cumulative)
    return (jnp.exp(totals), jnp.einsum("nhd,nhe->hde", weighted, value_rows, precision=precise))


def combine(earlier, later):
    return (earlier[0] * later[0], later[0][..., None] * earlier[1] + later[1])


def blockwise(queries, key_rows, value_rows, log_decay, carried, block_len):
    length, head_count, _ = queries.shape
    value_width = value_rows.shape[-1]
    blocks = length // block_len

    def shaped(array):
        return array.reshape(blocks, block_len, head_count, array.shape[-1])

    triangle = jnp.tril(jnp.ones((block_len, block_len), jnp.float32))

    def advance(state_now, inputs):
        block_q, block_k, block_v, block_a = inputs
        cumulative = jnp.cumsum(block_a, axis=0)
        block_end = cumulative[-1]
        query_dec = block_q * jnp.exp(cumulative)
        scores = (
            jnp.einsum("ihd,jhd->hij", query_dec, block_k * jnp.exp(-cumulative), precision=precise)
            * triangle
        )
        result = jnp.einsum("hij,jhe->ihe", scores, block_v, precision=precise)
        result = result + jnp.einsum("ihd,hde->ihe", query_dec, state_now, precision=precise)
        state_next = state_now * jnp.exp(block_end)[:, :, None] + jnp.einsum(
            "jhd,jhe->hde", block_k * jnp.exp(block_end - cumulative), block_v, precision=precise
        )
        return (state_next, result)

    _, outputs = lax.scan(
        advance, carried, (shaped(queries), shaped(key_rows), shaped(value_rows), shaped(log_decay))
    )
    return outputs.reshape(length, head_count, value_width)


def head_channels(pieces, per_head, tp_index):
    for bit_number in range(per_head.bit_length() - 1):
        partner = from_partner(
            (for_sending(pieces[0]), for_sending(pieces[1]), for_sending(pieces[2])),
            "tp",
            bit_number,
        )
        upper = tp_index // (1 << bit_number) % 2 == 1
        pieces = tuple(
            (
                jnp.where(
                    upper,
                    jnp.concatenate([theirs, mine], axis=1),
                    jnp.concatenate([mine, theirs], axis=1),
                )
                for mine, theirs in zip(pieces, partner)
            )
        )
    return pieces


def context_totals(fwd_growth, fwd_state, bwd_growth, bwd_state, identity):

    def absorb(carried, piece):
        return (combine(carried, piece), None)

    total_fwd, _ = lax.scan(absorb, identity, (fwd_growth, fwd_state))
    total_bwd, _ = lax.scan(absorb, identity, (bwd_growth, bwd_state), reverse=True)
    return (total_fwd, total_bwd)


def stored(array):
    return lax.optimization_barrier(array.astype(jnp.bfloat16))


def local(
    latent,
    context,
    conditioning,
    context_prompt_vector,
    shift_matrix,
    scale_matrix,
    residual_gate_matrix,
    query_matrix,
    key_matrix,
    value_matrix,
    gate_matrix,
    decay_down_factor,
    decay_up_factor,
    decay_key_bias,
    spike_log_decay,
    output_gain,
    output_matrix,
):
    tp_count = lax.axis_size("tp")
    tp_index = lax.axis_index("tp")
    per_head = max(tp_count // HEADS, 1)
    heads_per_shard = max(HEADS // tp_count, 1)
    leading_head = tp_index // per_head * heads_per_shard
    tok_rows = latent.shape[0]
    conds = jax.nn.silu(
        jnp.stack([conditioning, context_prompt_vector]).astype(jnp.float32)
    ).astype(jnp.bfloat16)
    shifts, scales, gates = lax.psum(
        (
            linear(conds, shift_matrix),
            linear(conds, scale_matrix),
            linear(conds, residual_gate_matrix),
        ),
        "sp",
    )
    down_both = jnp.concatenate([decay_down_factor[0].T, decay_down_factor[1].T], axis=0)
    lat_weights = (query_matrix, key_matrix, value_matrix, gate_matrix, down_both)
    ctx_weights = (key_matrix, value_matrix, down_both)
    lat_f = latent.astype(jnp.float32)
    ctx_f = context.astype(jnp.float32)
    lat_sum, lat_squares, ctx_sum, ctx_squares = lax.psum(
        (
            jnp.sum(lat_f, axis=1, keepdims=True),
            jnp.sum(lat_f * lat_f, axis=1, keepdims=True),
            jnp.sum(ctx_f, axis=1, keepdims=True),
            jnp.sum(ctx_f * ctx_f, axis=1, keepdims=True),
        ),
        "tp",
    )
    latent_normalized = modulated(latent, lat_sum, lat_squares, shifts[0], scales[0])
    normed_ctx = modulated(context, ctx_sum, ctx_squares, shifts[1], scales[1])
    lat_piece = lax.all_gather(latent_normalized, "tp", axis=1, tiled=True)
    ctx_piece = lax.all_gather(normed_ctx, "tp", axis=1, tiled=True)
    lat_new = tuple((linear(lat_piece, weight) for weight in lat_weights))
    ctx_new = tuple((linear(ctx_piece, weight) for weight in ctx_weights))
    query_part, key_part, value_part, gate_part, low_rank_part = lat_new
    ctx_key_part, ctx_value_part, ctx_low = ctx_new
    query_full, key_full, ctx_key_full = head_channels(
        (stored(query_part), stored(key_part), stored(ctx_key_part)), per_head, tp_index
    )

    def split_heads(rows, width):
        return rows.astype(jnp.float32).reshape(rows.shape[0], heads_per_shard, width)

    value_cols = value_part.shape[1] // heads_per_shard
    queries = split_heads(query_full, DK) * DK ** (-0.5)
    key_rows = split_heads(key_full, DK)
    ctx_keys = split_heads(ctx_key_full, DK)
    values_lat = split_heads(stored(value_part), value_cols)
    values_ctx = split_heads(stored(ctx_value_part), value_cols)
    gate_rows = stored(gate_part).astype(jnp.float32)

    def per_head_decay(low_rows, direction):
        up_part = lax.dynamic_slice_in_dim(
            decay_up_factor[direction], leading_head * DK, heads_per_shard * DK, 1
        ).astype(jnp.float32)
        bias_part = lax.dynamic_slice_in_dim(
            decay_key_bias[direction], leading_head * DK, heads_per_shard * DK, 0
        )
        pre_act = jnp.dot(low_rows, up_part, precision=precise) + bias_part
        return (jax.nn.log_sigmoid(pre_act) / gate_norm).reshape(
            low_rows.shape[0], heads_per_shard, DK
        )

    decay_spikes = lax.dynamic_slice_in_dim(spike_log_decay, leading_head, heads_per_shard, 2)
    latent_forward = per_head_decay(low_rank_part[:, :DECAY_RANK], 0) + decay_spikes[0][:, :, None]
    latent_backward = per_head_decay(low_rank_part[:, DECAY_RANK:], 1) + decay_spikes[1][:, :, None]
    ctx_fwd = per_head_decay(ctx_low[:, :DECAY_RANK], 0)
    ctx_bwd = per_head_decay(ctx_low[:, DECAY_RANK:], 1)
    cf_growth, cf_state = end_state(ctx_keys, values_ctx, ctx_fwd)
    cb_growth, cb_state = end_state(
        reverse_rows(ctx_keys), reverse_rows(values_ctx), reverse_rows(ctx_bwd)
    )
    lf_growth, lf_state = end_state(key_rows, values_lat, latent_forward)
    lb_growth, lb_state = end_state(
        reverse_rows(key_rows), reverse_rows(values_lat), reverse_rows(latent_backward)
    )
    identity = (
        jnp.ones((heads_per_shard, DK), jnp.float32),
        jnp.zeros((heads_per_shard, DK, value_cols), jnp.float32),
    )
    ctx_gathered = (
        lax.all_gather(cf_growth[None].astype(jnp.bfloat16), "sp", axis=0, tiled=True).astype(
            jnp.float32
        ),
        lax.all_gather(cf_state[None].astype(jnp.bfloat16), "sp", axis=0, tiled=True).astype(
            jnp.float32
        ),
        lax.all_gather(cb_growth[None].astype(jnp.bfloat16), "sp", axis=0, tiled=True).astype(
            jnp.float32
        ),
        lax.all_gather(cb_state[None].astype(jnp.bfloat16), "sp", axis=0, tiled=True).astype(
            jnp.float32
        ),
    )
    total_fwd, total_bwd = context_totals(
        ctx_gathered[0], ctx_gathered[1], ctx_gathered[2], ctx_gathered[3], identity
    )
    prefix = carried_in((lf_growth, lf_state), "sp", combine, identity, False)
    suffix = carried_in((lb_growth, lb_state), "sp", combine, identity, True)
    start_fwd = combine(total_fwd, prefix)[1]
    start_bwd = combine(total_bwd, suffix)[1]
    zero_state = jnp.zeros((heads_per_shard, DK, value_cols), jnp.float32)

    def direction_out(query_rows, key_list, value_list, log_decay, start_state):
        local_part = blockwise(query_rows, key_list, value_list, log_decay, zero_state, BLK)
        reach = query_rows * jnp.exp(jnp.cumsum(log_decay, axis=0))
        return local_part + jnp.einsum("nhd,hde->nhe", reach, start_state, precision=precise)

    out_fwd = direction_out(queries, key_rows, values_lat, latent_forward, start_fwd)
    out_bwd = reverse_rows(
        direction_out(
            reverse_rows(queries),
            reverse_rows(key_rows),
            reverse_rows(values_lat),
            reverse_rows(latent_backward),
            start_bwd,
        )
    )
    grouped = (out_fwd + out_bwd).reshape(tok_rows, -1, VGROUP)
    grouped = grouped * lax.rsqrt(jnp.mean(grouped * grouped, axis=-1, keepdims=True) + epsilon)
    heads_out = (grouped.reshape(tok_rows, -1) * output_gain * jax.nn.silu(gate_rows)).astype(
        jnp.bfloat16
    )
    branch = linear(lax.all_gather(heads_out, "tp", axis=1, tiled=True), output_matrix)
    return (latent.astype(jnp.float32) + gates[0] * branch).astype(jnp.bfloat16)


def exact(a, b):
    return lax.dot_general(
        a, b, (((1,), (0,)), ((), ())), precision=precise, preferred_element_type=jnp.float32
    )


def nt(a, b):
    return lax.dot_general(a, b, (((1,), (1,)), ((), ())), preferred_element_type=jnp.float32)


def nn(a, b):
    return lax.dot_general(a, b, (((1,), (0,)), ((), ())), preferred_element_type=jnp.float32)


def tn(a, b):
    return lax.dot_general(a, b, (((0,), (0,)), ((), ())), preferred_element_type=jnp.float32)


def short(value):
    return value.astype(jnp.bfloat16)


def terms(value):
    first = short(value)
    rest = value - first.astype(jnp.float32)
    second = short(rest)
    return first, second, short(rest - second.astype(jnp.float32))


def log_sigmoid(pre):
    return (jnp.minimum(pre, 0.0) - jnp.log1p(jnp.exp(-jnp.abs(pre)))) / gate_norm


def triangle_of(size, upper):
    i = lax.broadcasted_iota(jnp.int32, (size, size), 0)
    j = lax.broadcasted_iota(jnp.int32, (size, size), 1)
    return (j >= i) if upper else (j <= i)


def layer_kernel(
    n,
    s,
    inner,
    rows,
    crows,
    feats,
    heads,
    dv,
    parts,
    hparts,
    latent,
    context,
    conditioning,
    prompt,
    shift_m,
    scale_m,
    gate_m,
    query_m,
    key_m,
    value_m,
    og_m,
    down,
    up,
    bias,
    spike,
    gain,
    out_m,
    out_ref,
    x_all,
    xn,
    acc,
    low_acc,
    mod_w,
    proj_w,
    out_w,
    down_v,
    up_v,
    bias_v,
    spike_v,
    gain_v,
    cond_v,
    mod_own,
    mod_recv,
    mod_all,
    gate_own,
    gate_recv,
    stat_all,
    spike_rows,
    proj,
    ctx_kv,
    ctx_low,
    tot_own,
    tot_recv,
    st_own,
    st_recv,
    local_out,
    ho_all,
    total_out,
    load_sem,
    x_send,
    x_recv,
    waves,
    *gather_sems,
):
    me = lax.axis_index("tp")
    sp = lax.axis_index("sp")
    hk = heads * DK
    hv = heads * dv
    model = n * feats
    both = rows + crows
    width = feats // parts
    hwidth = hv // hparts
    f32 = jnp.float32

    used = [0]

    def load(*pairs, whole):
        sem = load_sem.at[used[0]]
        used[0] += 1
        for src, dst in pairs:
            pltpu.make_async_copy(src, dst, sem).start()
        return pltpu.make_async_copy(whole, whole, sem)

    def own_piece(p):
        cols = pl.ds(p * width, width)
        return (
            (latent.at[:, cols], x_all.at[me * parts + p, pl.ds(0, rows)]),
            (context.at[:, cols], x_all.at[me * parts + p, pl.ds(rows, crows)]),
        )

    own_x = [load(*own_piece(0), whole=x_all.at[pl.ds(me * parts, 1)])]
    if parts > 1:
        own_x.append(
            load(
                *[c for p in range(1, parts) for c in own_piece(p)],
                whole=x_all.at[pl.ds(me * parts + 1, parts - 1)],
            )
        )
    first = [
        load((conditioning, cond_v.at[0]), (prompt, cond_v.at[1]), whole=cond_v),
        load((shift_m, mod_w.at[0]), (scale_m, mod_w.at[1]), whole=mod_w.at[pl.ds(0, 2)]),
    ]
    gate_load = load((gate_m, mod_w.at[2]), whole=mod_w.at[2])
    head_cols = pl.ds(pl.multiple_of(me * hk, hk), hk)
    small = [
        load((up.at[:, :, head_cols], up_v), whole=up_v),
        load((bias.at[:, head_cols], bias_v), whole=bias_v),
        load((spike, spike_v), whole=spike_v),
        load((gain, gain_v), whole=gain_v),
    ]
    weights = [
        load(
            (query_m, proj_w.at[pl.ds(0, hk)]),
            (key_m, proj_w.at[pl.ds(hk, hk)]),
            (value_m, proj_w.at[pl.ds(2 * hk, hv)]),
            (og_m, proj_w.at[pl.ds(2 * hk + hv, hv)]),
            whole=proj_w,
        ),
        load((down, down_v), whole=down_v),
    ]
    last = load((out_m, out_w), whole=out_w)

    line = n // inner
    z, y = lax.div(me, inner), lax.rem(me, inner)
    mate = z + 1 - 2 * lax.rem(z, 2)
    paired = inner > 1 and line % 2 == 0
    at_end = (z == 0) | (z == line - 1)

    def block_of(at, column):
        return at * inner + column

    barrier = pltpu.get_barrier_semaphore()

    def greet(**where):
        pl.semaphore_signal(barrier, inc=1, device_id=where, device_id_type=MESH)

    pl.when(z + 1 < line)(lambda: greet(tp=block_of(z + 1, y)))
    pl.when(z > 0)(lambda: greet(tp=block_of(z - 1, y)))
    if inner > 1:
        greet(tp=block_of(z, inner - 1 - y))
    for d in range(1, s):
        greet(sp=lax.rem(sp + d, s))
    beside = jnp.where(z > 0, 1, 0) + jnp.where(z + 1 < line, 1, 0)
    pl.semaphore_wait(barrier, beside + (inner - 1) + (s - 1))

    def pass_on(way):
        pl.semaphore_signal(
            waves.at[way],
            inc=1,
            device_id={"tp": block_of(z + 1 - 2 * way, y)},
            device_id_type=MESH,
        )

    def relay(way):
        pl.semaphore_wait(waves.at[way], 1)
        pass_on(way)

    if line > 1:
        pl.when(z == 0)(lambda: pass_on(0))
        pl.when(z == line - 1)(lambda: pass_on(1))

    started = []

    class Exchange:
        def __init__(self, axis, index, src, dst, landed, send_index=None, sent=True):
            at, count = (me, n) if axis == "tp" else (sp, s)
            self.some = count > 1

            def copy(source, target, d):
                return pltpu.make_async_remote_copy(
                    src_ref=source,
                    dst_ref=target,
                    send_sem=x_send.at[index if send_index is None else send_index],
                    recv_sem=x_recv.at[index],
                    device_id={axis: lax.rem(at + d, count)},
                    device_id_type=MESH,
                )

            for d in range(1, count):
                copy(src(d), dst(d), d).start()
            if self.some:
                self.all = copy(landed, landed, 1)
                if sent:
                    started.append(self.all)

        def wait_recv(self):
            if self.some:
                self.all.wait_recv()

    def level(i):
        table = []
        for at in range(line):
            order = [at]
            for k in range(1, line):
                order += [b for b in (at - k, at + k) if 0 <= b < line]
            table.append(order[i])
        return sum(jnp.where(z == at, table[at], 0) for at in range(line))

    class Gather:
        def __init__(self, ref, pieces, sems):
            self.ref, self.pieces = ref, pieces
            self.column_send, self.across_send, self.column_recv, self.across_recv = sems
            self.half = max(pieces // 2, 1)
            self.turned = tuple(range(pieces // 2, pieces)) if paired else ()

        def remote(self, ref, send_sem, recv_sem, target):
            return pltpu.make_async_remote_copy(
                src_ref=ref,
                dst_ref=ref,
                send_sem=send_sem,
                recv_sem=recv_sem,
                device_id={"tp": target},
                device_id_type=MESH,
            )

        def along(self, at, piece, to):
            return self.remote(
                self.ref.at[block_of(at, y) * self.pieces + piece],
                self.column_send.at[0],
                self.column_recv.at[lax.rem(at - to + line, line) - 1, piece],
                block_of(to, y),
            )

        def across(self, at, column, piece, target):
            return self.remote(
                self.ref.at[block_of(at, column) * self.pieces + piece],
                self.across_send.at[0],
                self.across_recv.at[at, piece // self.half],
                target,
            )

        def lane_sends(self, lane, k, piece, act):
            up = lane == "up"
            at, has = (z - k, z >= k) if up else (z + k, z + k < line)
            if k < line - 1:
                onward, to = (z + 1 < line, z + 1) if up else (z > 0, z - 1)
                pl.when(has & onward)(lambda: act(self.along(at, piece, to)))
            if inner > 1 and (k > 0 or up):
                if k == 1 and piece in self.turned:
                    has = has & (lax.rem(z, 2) == (0 if up else 1))
                pl.when(has)(
                    lambda: act(self.across(at, y, piece, block_of(z, inner - 1 - y)))
                )

        def start(self, piece):
            for lane in ("up", "down"):
                self.lane_sends(lane, 0, piece, lambda c: c.start())

        def take(self, lane, k, piece):
            at, has = (z - k, z >= k) if lane == "up" else (z + k, z + k < line)
            pl.when(has)(lambda: self.along(at, piece, z).wait_recv())
            self.lane_sends(lane, k, piece, lambda c: c.start())

        def near(self, k, piece):
            pl.when(z >= line // 2)(lambda: self.take("up", k, piece))
            pl.when(z < line // 2)(lambda: self.take("down", k, piece))

        def far(self, k, piece):
            pl.when(z < line // 2)(lambda: self.take("up", k, piece))
            pl.when(z >= line // 2)(lambda: self.take("down", k, piece))

        def side_start(self, when, piece):
            pl.when(when)(
                lambda: self.across(z, inner - 1 - y, piece, block_of(mate, y)).start()
            )

        def arrive(self, i, half):
            at = level(i)
            block = block_of(at, inner - 1 - y)
            self.remote(
                self.ref.at[pl.ds(block * self.pieces + half * self.half, self.half)],
                self.across_send.at[0],
                self.across_recv.at[at, half],
                block,
            ).wait_recv()

        def drain(self):
            def sent(count, sem):
                self.remote(
                    self.ref.at[pl.ds(0, count * self.pieces)],
                    sem.at[0],
                    self.across_recv.at[0, 0],
                    block_of(z, inner - 1 - y),
                ).wait_send()

            if line > 1:
                pl.when(at_end)(lambda: sent(1, self.column_send))
            if line > 2:
                pl.when(jnp.logical_not(at_end))(lambda: sent(line + 1, self.column_send))
            if inner > 1:
                sent(line, self.across_send)

    def run(events):
        for _, act in sorted(enumerate(events), key=lambda e: (e[1][0], e[0])):
            act[1]()

    xg = Gather(x_all, parts, gather_sems[:4])
    hg = Gather(ho_all, hparts, gather_sems[4:])

    for p in range(parts):
        if p < 2:
            own_x[p].wait()
        xg.start(p)
    if line > 2:
        pl.when((z > 0) & (z < line - 1))(lambda: relay(0))
        pl.when(z == line - 2)(lambda: relay(1))

    first[0].wait()

    def one_row(which):
        part = cond_v[which].astype(f32)
        return jnp.concatenate([part[r : r + 1] for r in range(part.shape[0])], axis=1)

    row_of = lax.broadcasted_iota(jnp.int32, (16, shift_m.shape[1]), 0)
    conds = jnp.where(row_of == 0, one_row(0), one_row(1))
    conds = short(conds * lax.logistic(conds))
    first[1].wait()
    for which in range(2):
        mod_own[2 * which : 2 * which + 2, :] = nt(conds, mod_w[which])[0:2]
    m1 = Exchange("sp", 0, lambda d: mod_own, lambda d: mod_recv.at[d - 1], mod_recv)

    ones = jnp.ones((16, width), jnp.bfloat16)
    row_sum = jnp.zeros((16, both), f32)
    row_squares = jnp.zeros((16, both), f32)
    for p in range(parts):
        own = x_all[me * parts + p]
        own_f = own.astype(f32)
        row_sum = row_sum + nt(ones, own)
        for part in terms(own_f * own_f):
            row_squares = row_squares + nt(ones, part)
    stat_all[me] = jnp.zeros(stat_all.shape[1:], f32)
    stat_all[me, 0:1, 0:both] = row_sum[0:1]
    stat_all[me, 1:2, 0:both] = row_squares[0:1]

    held = {}

    def send_stats():
        if line > 1:
            pl.when(z == line - 1)(lambda: pl.semaphore_wait(waves.at[0], 1))
            pl.when(z == 0)(lambda: pl.semaphore_wait(waves.at[1], 1))
        if line > 2:
            pl.when((z > 0) & (z < line - 2))(lambda: relay(1))
        held["sa"] = Exchange(
            "tp",
            3,
            lambda d: stat_all.at[me],
            lambda d: stat_all.at[me],
            stat_all.at[pl.ds(0, n - 1)],
        )

    def send_mods():
        m1.wait_recv()
        total = mod_own[...]
        for d in range(1, s):
            total = total + mod_recv[d - 1]
        mod_all[me] = total
        held["m2"] = Exchange(
            "tp",
            1,
            lambda d: mod_all.at[me],
            lambda d: mod_all.at[me],
            mod_all.at[pl.ds(0, n - 1)],
        )

    def send_gates():
        gate_load.wait()
        gate_own[...] = nt(conds, mod_w[2])[0:2]
        held["mg"] = Exchange(
            "sp", 2, lambda d: gate_own, lambda d: gate_recv.at[d - 1], gate_recv
        )

    def early():
        for copy in small:
            copy.wait()
        slot_head = lax.broadcasted_iota(jnp.int32, (spike_v.shape[1], hk), 0)
        lane_head = lax.broadcasted_iota(jnp.int32, (spike_v.shape[1], hk), 1) // DK
        pick = jnp.where(slot_head == me * heads + lane_head, 1.0, 0.0).astype(jnp.bfloat16)
        for e in range(2):
            spike_rows[:, e * hk : (e + 1) * hk] = sum(
                tn(part, pick) for part in terms(spike_v[e])
            )
        acc[...] = jnp.zeros(acc.shape, f32)
        low_acc[...] = jnp.zeros(low_acc.shape, f32)

    def moments():
        held["sa"].wait_recv()
        stats = sum(stat_all[b] for b in range(n))
        diagonal = lax.broadcasted_iota(jnp.int32, (both, both), 0) == lax.broadcasted_iota(
            jnp.int32, (both, both), 1
        )

        def column_of(row):
            return (
                jnp.sum(
                    jnp.where(diagonal, stats[row : row + 1, 0:both], 0.0), axis=1, keepdims=True
                )
                / model
            )

        mean = column_of(0)
        held["mean"] = mean
        held["spread"] = lax.rsqrt(column_of(1) - mean * mean + epsilon)

    def wait_mods():
        held["m2"].wait_recv()
        for copy in weights:
            copy.wait()

    tile = math.gcd(2 * hk + 2 * hv, 512)
    columns = acc.shape[1]

    def project_block(block):
        cols = pl.ds(pl.multiple_of(block * feats, feats), feats)
        mean, spread = held["mean"], held["spread"]
        mod = mod_all[block]
        for p in range(parts):
            lanes = slice(p * width, (p + 1) * width)
            x = (x_all[block * parts + p].astype(f32) - mean) * spread
            m = mod[:, lanes]
            xn[0:rows, lanes] = short(x[0:rows] * (1.0 + m[2:3]) + m[0:1])
            xn[rows:, lanes] = short(x[rows:] * (1.0 + m[3:4]) + m[1:2])
        low_acc[...] += nt(xn[...], down_v[:, cols])
        for t in range(columns // tile):
            out = slice(t * tile, (t + 1) * tile)
            acc[:, out] += nt(xn[...], proj_w[out, cols])

    def column_block(i):
        project_block(block_of(level(i), y))

    def other_block(i):
        if i > 0:
            for half in range(min(parts, 2)):
                xg.arrive(i, half)
        project_block(block_of(level(i), inner - 1 - y))

    unit, lag, cost = 0.79, 2.0, 0.6
    arrival = lambda k, p: unit * ((k - 1) * parts + p + 1) + lag
    mods_at = 9.4
    events = [
        (arrival(1, 0) - 0.1, send_stats),
        (arrival(1, parts // 2 - 1) + 0.01, send_mods),
        (arrival(1, parts // 2 - 1) + 0.02, send_gates),
        (arrival(1, parts - 1) + 0.05, early),
        (arrival(1, parts - 1) + 0.06, moments),
        (mods_at, wait_mods),
    ]
    for k in range(1, line):
        for p in range(parts):
            events.append((arrival(k, p), functools.partial(xg.take, "up", k, p)))
            events.append((arrival(k, p) + 0.005, functools.partial(xg.take, "down", k, p)))
    if inner > 1:
        for half in range(min(parts, 2)):
            when = arrival(1, (half + 1) * xg.half - 1)
            events.append((when + 0.03, functools.partial(xg.arrive, 0, half)))
        for p in xg.turned:
            when = arrival(1, parts - 1)
            events.append((when + 0.04, functools.partial(xg.side_start, at_end, p)))
            if line > 2:
                when = arrival(line - 2, parts - 1)
                events.append(
                    (
                        when + 0.01,
                        functools.partial(xg.side_start, jnp.logical_not(at_end), p),
                    )
                )
    tasks = []
    for i in range(line):
        ready = arrival(i, parts - 1) + 0.02 if i else 0.0
        tasks.append((ready, functools.partial(column_block, i)))
        if inner > 1:
            ready = arrival(max(i, 1), parts - 1) + 0.05 + (lag if i else 0)
            if i == 1 and xg.turned:
                ready = max(ready, arrival(line - 1, parts - 1) + unit * len(xg.turned))
            tasks.append((ready, functools.partial(other_block, i)))
    clock = mods_at + 0.01
    for ready, task in sorted(tasks, key=lambda t: t[0]):
        clock = max(clock, ready)
        events.append((clock, task))
        clock += cost
    run(events)
    proj[...] = short(acc[...])

    own_ctx = pl.ds(pl.multiple_of(sp * crows, crows), crows)
    ctx_kv[own_ctx, :] = proj[rows:, hk : 2 * hk + hv]
    ctx_low[own_ctx, :] = jnp.zeros((crows, ctx_low.shape[1]), jnp.bfloat16)
    for i, part in enumerate(terms(low_acc[rows:])):
        ctx_low[own_ctx, i * 2 * DECAY_RANK : (i + 1) * 2 * DECAY_RANK] = part
    lo = Exchange(
        "sp",
        5,
        lambda d: ctx_low.at[own_ctx],
        lambda d: ctx_low.at[own_ctx],
        ctx_low.at[pl.ds(0, (s - 1) * crows)],
    )
    kv = Exchange(
        "sp",
        4,
        lambda d: ctx_kv.at[own_ctx],
        lambda d: ctx_kv.at[own_ctx],
        ctx_kv.at[pl.ds(0, (s - 1) * crows)],
    )

    none = jnp.zeros((DECAY_RANK, hk), jnp.bfloat16)
    up_both = jnp.concatenate(
        [
            jnp.concatenate([up_v[0], none], axis=1),
            jnp.concatenate([none, up_v[1]], axis=1),
        ],
        axis=0,
    )
    bias_both = jnp.concatenate([bias_v[0:1], bias_v[1:2]], axis=1)

    def logs_of(parts_of_low):
        return log_sigmoid(sum(nn(part, up_both) for part in parts_of_low) + bias_both)

    def running(logs, length, e):
        lanes = slice(e * hk, (e + 1) * hk)
        mask = jnp.where(triangle_of(length, e == 1), 1.0, 0.0).astype(jnp.bfloat16)
        return sum(nn(mask, part) for part in terms(logs[:, lanes]))

    logs = logs_of(terms(low_acc[0:rows])) + spike_rows[...]
    cum = [running(logs, rows, e) for e in range(2)]
    whole = [cum[0][rows - 1 : rows], cum[1][0:1]]
    tot_own[0:1, :] = whole[0]
    tot_own[1:2, :] = whole[1]
    to = Exchange("sp", 6, lambda d: tot_own, lambda d: tot_recv.at[d - 1], tot_recv)

    keys = proj[0:rows, hk : 2 * hk].astype(f32)
    per = hparts // heads
    weighted = [short(keys * jnp.exp(whole[e] - cum[e])) for e in range(2)]
    st = []
    for h in range(heads):
        for e in range(2):
            state = short(
                tn(
                    weighted[e][:, h * DK : (h + 1) * DK],
                    proj[0:rows, 2 * hk + h * dv : 2 * hk + (h + 1) * dv],
                )
            )
            for q in range(per):
                st_own[e, h * per + q] = state[:, q * hwidth : (q + 1) * hwidth]
        for q in range(h * per, (h + 1) * per):
            st.append(
                Exchange(
                    "sp",
                    7 + q,
                    lambda d: st_own.at[jnp.where(lax.rem(sp + d, s) > sp, 0, 1), q],
                    lambda d: st_recv.at[d - 1, q],
                    st_recv.at[:, q],
                    7,
                    False,
                )
            )

    queries = proj[0:rows, 0:hk].astype(f32) * DK ** (-0.5)
    blocks = rows // BLK

    def span(b):
        return slice(b * BLK, (b + 1) * BLK)

    inside = [[], []]
    for b in range(blocks):
        f = cum[0][span(b)]
        inside[0].append(f if b == 0 else f - cum[0][b * BLK - 1 : b * BLK])
        f = cum[1][span(b)]
        inside[1].append(
            f if b == blocks - 1 else f - cum[1][(b + 1) * BLK : (b + 1) * BLK + 1]
        )
    ends = [[part[BLK - 1 : BLK] for part in inside[0]], [part[0:1] for part in inside[1]]]
    q_dec = [[short(queries[span(b)] * jnp.exp(inside[e][b])) for b in range(blocks)] for e in range(2)]
    k_dec = [[short(keys[span(b)] * jnp.exp(-inside[e][b])) for b in range(blocks)] for e in range(2)]
    k_end = [
        [short(keys[span(b)] * jnp.exp(ends[e][b] - inside[e][b])) for b in range(blocks)]
        for e in range(2)
    ]
    lower, upper = triangle_of(BLK, False), triangle_of(BLK, True)
    scores = []
    for h in range(heads):
        ch = slice(h * DK, (h + 1) * DK)
        lines = []
        for b in range(blocks):
            strip = []
            for c in range(blocks):
                if b == c:
                    strip.append(
                        jnp.where(lower, nt(q_dec[0][b][:, ch], k_dec[0][b][:, ch]), 0.0)
                        + jnp.where(upper, nt(q_dec[1][b][:, ch], k_dec[1][b][:, ch]), 0.0)
                    )
                    continue
                e = 0 if c < b else 1
                near = q_dec[e][b][:, ch]
                between = range(c + 1, b) if c < b else range(b + 1, c)
                if len(between) > 0:
                    gap = sum(ends[e][m][:, ch] for m in between)
                    near = short(queries[span(b)][:, ch] * jnp.exp(inside[e][b][:, ch] + gap))
                strip.append(nt(near, k_end[e][c][:, ch]))
            lines.append(jnp.concatenate(strip, axis=1) if blocks > 1 else strip[0])
        scores.append(short(jnp.concatenate(lines, axis=0) if blocks > 1 else lines[0]))

    lo.wait_recv()
    low_parts = [
        ctx_low[:, i * 2 * DECAY_RANK : (i + 1) * 2 * DECAY_RANK] for i in range(3)
    ]
    ctx_logs = logs_of(low_parts)
    length = s * crows
    ctx_decay = []
    for e in range(2):
        c = running(ctx_logs, length, e)
        end = c[length - 1 : length] if e == 0 else c[0:1]
        ctx_decay.append(jnp.exp(end - c))

    kv.wait_recv()
    ctx_keys = ctx_kv[:, 0:hk].astype(f32)
    ctx_weighted = [short(ctx_keys * part) for part in ctx_decay]
    ctx_states = [
        [
            short(tn(w[:, h * DK : (h + 1) * DK], ctx_kv[:, hk + h * dv : hk + (h + 1) * dv]))
            for w in ctx_weighted
        ]
        for h in range(heads)
    ]
    to.wait_recv()
    places = {d: lax.rem(sp - d + s, s) for d in range(1, s)}

    def passed(low_end, high_end, direction):
        result = jnp.zeros((1, hk), f32)
        for d in range(1, s):
            inside_it = jnp.where((places[d] > low_end) & (places[d] < high_end), 1.0, 0.0)
            result = result + inside_it * tot_recv[d - 1][direction : direction + 1]
        return result

    ctx_reach = [
        short(queries * jnp.exp(cum[0] + passed(-1, sp, 0))),
        short(queries * jnp.exp(cum[1] + passed(sp, s, 1))),
    ]
    reach = []
    for d in range(1, s):
        p = places[d]
        before = jnp.where(p < sp, 1.0, 0.0)
        exponent = before * (cum[0] + passed(p, sp, 0)) + (1.0 - before) * (
            cum[1] + passed(sp, p, 1)
        )
        reach.append(short(queries * jnp.exp(exponent)))
    gate_rows = proj[0:rows, 2 * hk + hv :].astype(f32)
    small_gate = gate_rows * lax.logistic(gate_rows) * gain_v[...]

    for h in range(heads):
        ch = slice(h * DK, (h + 1) * DK)
        vc = slice(h * dv, (h + 1) * dv)
        local_out[:, vc] = nn(
            jnp.concatenate([scores[h]] + [r[:, ch] for r in ctx_reach], axis=1),
            jnp.concatenate(
                [proj[0:rows, 2 * hk + h * dv : 2 * hk + (h + 1) * dv]]
                + ctx_states[h],
                axis=0,
            ),
        )
    gi = lax.broadcasted_iota(jnp.int32, (hwidth, hwidth), 0) // VGROUP
    gj = lax.broadcasted_iota(jnp.int32, (hwidth, hwidth), 1) // VGROUP
    group = jnp.where(gi == gj, 1.0, 0.0).astype(jnp.bfloat16)

    def head_piece(q):
        h = q // per
        ch = slice(h * DK, (h + 1) * DK)
        vc = slice(q * hwidth, (q + 1) * hwidth)
        st[q].wait_recv()
        o = local_out[:, vc] + nn(
            jnp.concatenate([r[:, ch] for r in reach], axis=1),
            jnp.concatenate([st_recv[d - 1, q] for d in range(1, s)], axis=0),
        )
        squares = o * o
        top = short(squares)
        rest = short(squares - top.astype(f32))
        power = (nn(top, group) + nn(rest, group)) * (1.0 / VGROUP)
        ho_all[me * hparts + q] = short(o * lax.rsqrt(power + epsilon) * small_gate[:, vc])
        hg.start(q)

    def ready_out():
        last.wait()
        held["mg"].wait_recv()
        total_out[...] = jnp.zeros(total_out.shape, f32)

    def add_half(block, half):
        cols = pl.ds(pl.multiple_of(block * feats + half * 2 * hwidth, 2 * hwidth), 2 * hwidth)
        pair = jnp.concatenate(
            [ho_all[block * hparts + 2 * half], ho_all[block * hparts + 2 * half + 1]], axis=1
        )
        total_out[...] += nt(pair, out_w[:, cols])

    def add_column(i, half):
        add_half(block_of(level(i), y), half)

    def add_other(i, half):
        if i > 0:
            hg.arrive(i, half)
        add_half(block_of(level(i), inner - 1 - y), half)

    hop_h = 2.6
    here = lambda k, q: 0.4 * q + 0.4 * (q // 2) + hop_h * k
    events = [(here(0, 1) + 0.01, ready_out)]
    for q in range(hparts):
        events.append((here(0, q), functools.partial(head_piece, q)))
        for k in range(1, line):
            events.append((here(k, q), functools.partial(hg.near, k, q)))
            if 2 * k < line + line % 2:
                events.append((here(k, q) + 0.5, functools.partial(hg.far, k, q)))
        if q in hg.turned:
            when = here(1, hparts - 1) + 0.03
            events.append((when, functools.partial(hg.side_start, at_end, q)))
            if line > 2:
                when = here(line - 2, q) + 0.03
                events.append(
                    (when, functools.partial(hg.side_start, jnp.logical_not(at_end), q))
                )
    if inner > 1:
        for half in range(2):
            when = here(1, (half + 1) * hg.half - 1) + 0.02
            events.append((when, functools.partial(hg.arrive, 0, half)))
    for i in range(line):
        for half in range(hparts // 2):
            when = here(i, 2 * half + 1) + 0.6
            events.append((when, functools.partial(add_column, i, half)))
            if inner > 1:
                when += hop_h + 0.1
                if i == 1 and 2 * half in hg.turned:
                    when = max(when, here(line - 1, 2 * half + 1) + 0.4)
                events.append((when, functools.partial(add_other, i, half)))
    run(events)
    gates = gate_own[0:1]
    for d in range(1, s):
        gates = gates + gate_recv[d - 1, 0:1]
    for p in range(parts):
        lanes = slice(p * width, (p + 1) * width)
        out_ref[:, lanes] = short(
            x_all[me * parts + p, 0:rows].astype(f32) + gates[:, lanes] * total_out[:, lanes]
        )
    for copy in started:
        copy.wait_send()
    if s > 1:
        pltpu.make_async_remote_copy(
            src_ref=st_recv,
            dst_ref=st_recv,
            send_sem=x_send.at[7],
            recv_sem=x_recv.at[7],
            device_id={"sp": lax.rem(sp + 1, s)},
            device_id_type=MESH,
        ).wait_send()
    xg.drain()
    hg.drain()


def one_kernel(
    latent,
    context,
    conditioning,
    context_prompt_vector,
    shift_matrix,
    scale_matrix,
    residual_gate_matrix,
    query_matrix,
    key_matrix,
    value_matrix,
    gate_matrix,
    decay_down_factor,
    decay_up_factor,
    decay_key_bias,
    spike_log_decay,
    output_gain,
    output_matrix,
):
    n, s = lax.axis_size("tp"), lax.axis_size("sp")
    rows, feats = latent.shape
    crows = context.shape[0]
    heads = HEADS // n
    hk, hv = query_matrix.shape[0], value_matrix.shape[0]
    dv = hv // heads
    model = n * feats
    both = rows + crows
    inputs = conditioning.shape[0]
    parts = feats // 128
    hparts = hv // 128
    stat_width = -(-both // 128) * 128
    bf, f32 = jnp.bfloat16, jnp.float32
    vmem, dma = pltpu.VMEM, pltpu.SemaphoreType.DMA
    scratch = [
        vmem((n * parts, both, 128), bf),
        vmem((both, feats), bf),
        vmem((both, 2 * hk + 2 * hv), f32),
        vmem((both, 2 * DECAY_RANK), f32),
        vmem((3, feats, inputs), bf),
        vmem((2 * hk + 2 * hv, model), bf),
        vmem((output_matrix.shape[0], model), bf),
        vmem((2 * DECAY_RANK, model), bf),
        vmem((2, DECAY_RANK, hk), bf),
        vmem((2, hk), f32),
        vmem((2, HEADS, rows), f32),
        vmem((1, hv), f32),
        vmem((2, inputs // 128, 128), bf),
        vmem((4, feats), f32),
        vmem((s - 1, 4, feats), f32),
        vmem((n, 4, feats), f32),
        vmem((2, feats), f32),
        vmem((s - 1, 2, feats), f32),
        vmem((n, 2, stat_width), f32),
        vmem((rows, 2 * hk), f32),
        vmem((both, 2 * hk + 2 * hv), bf),
        vmem((s * crows, hk + hv), bf),
        vmem((s * crows, 128), bf),
        vmem((2, hk), f32),
        vmem((s - 1, 2, hk), f32),
        vmem((2, hparts, DK, 128), bf),
        vmem((s - 1, hparts, DK, 128), bf),
        vmem((rows, hv), f32),
        vmem((n * hparts, rows, 128), bf),
        vmem((rows, feats), f32),
        dma((12,)),
        dma((8,)),
        dma((7 + hparts,)),
        pltpu.SemaphoreType.REGULAR((2,)),
    ]
    inner = 2 if n % 2 == 0 else 1
    line = n // inner
    hops = max(line - 1, 1)
    for pieces in (parts, hparts):
        scratch += [dma((1,)), dma((1,)), dma((hops, pieces)), dma((line, min(pieces, 2)))]
    return pl.pallas_call(
        functools.partial(
            layer_kernel, n, s, inner, rows, crows, feats, heads, dv, parts, hparts
        ),
        out_shape=pltpu.VMEM((rows, feats), bf),
        in_specs=[pl.BlockSpec(memory_space=pl.ANY)] * 17,
        out_specs=pl.BlockSpec(memory_space=pltpu.VMEM),
        scratch_shapes=scratch,
        compiler_params=pltpu.CompilerParams(
            collective_id=0, has_side_effects=True, vmem_limit_bytes=60 * 1024 * 1024
        ),
        name="layer",
    )(
        latent,
        context,
        conditioning.reshape(-1, 128),
        context_prompt_vector.reshape(-1, 128),
        shift_matrix,
        scale_matrix,
        residual_gate_matrix,
        query_matrix,
        key_matrix,
        value_matrix,
        gate_matrix,
        jnp.swapaxes(decay_down_factor, 1, 2).reshape(2 * DECAY_RANK, model),
        decay_up_factor,
        decay_key_bias,
        jnp.swapaxes(spike_log_decay, 1, 2),
        output_gain.reshape(1, -1),
        output_matrix,
    )


def solution(mesh):
    placed = (
        P("sp", "tp"),
        P("sp", "tp"),
        P("sp"),
        P("sp"),
        P("tp", "sp"),
        P("tp", "sp"),
        P("tp", "sp"),
        P("tp", None),
        P("tp", None),
        P("tp", None),
        P("tp", None),
        P(),
        P(),
        P(),
        P(None, "sp", None),
        P("tp"),
        P("tp", None),
    )
    whole_heads = HEADS == 2 * mesh.shape["tp"]
    return jax.shard_map(
        one_kernel if whole_heads else local, mesh=mesh, in_specs=placed, out_specs=P("sp", "tp"), check_vma=False
    )
```

```python
import functools
import math

import jax
import jax.numpy as jnp
from jax import lax
from jax.experimental import pallas as pl
from jax.experimental.pallas import tpu as pltpu
from jax.sharding import PartitionSpec as P

D = 4096
HEADS = 16
DK = 128
DECAY_RANK = 16
BLK = 64
VGROUP = 64
MESH = pl.DeviceIdType.MESH


epsilon = 1e-05
gate_norm = 16.0
precise = lax.Precision.HIGHEST


def for_sending(value):

    def short(part):
        return part.astype(jnp.bfloat16) if part.dtype == jnp.float32 else part

    return jax.tree.map(short, value)


def from_partner(value, axis, distance):
    return lax.ppermute(value, axis, [(i, i ^ 1 << distance) for i in range(lax.axis_size(axis))])


def carried_in(value, axis, combine, identity, reverse):
    peers, index = (lax.axis_size(axis), lax.axis_index(axis))
    everything = jax.tree.map(
        lambda part, kind: lax.all_gather(part.astype(kind), axis),
        value,
        (jnp.bfloat16, jnp.bfloat16),
    )
    start = jax.tree.map(
        lambda part, zero: jnp.broadcast_to(jnp.asarray(zero, part.dtype), part.shape),
        value,
        identity,
    )

    def turn(k, before):
        at = peers - 1 - k if reverse else k
        reached = at > index if reverse else at < index
        new = combine(
            before, jax.tree.map(lambda part, own: part[at].astype(own.dtype), everything, value)
        )
        return jax.tree.map(lambda a, b: jnp.where(reached, a, b), new, before)

    return lax.fori_loop(0, peers, turn, start)


def linear(rows, weight):
    return lax.dot_general(
        rows, weight, (((1,), (1,)), ((), ())), preferred_element_type=jnp.float32
    )


def modulated(rows, row_sum, row_squares, shift_vec, scale_vec):
    rows_f = rows.astype(jnp.float32)
    mean_val = row_sum / D
    variance = row_squares / D - mean_val * mean_val
    return (
        (rows_f - mean_val) * lax.rsqrt(variance + epsilon) * (1.0 + scale_vec) + shift_vec
    ).astype(jnp.bfloat16)


def reverse_rows(array):
    return jnp.flip(array, axis=0)


def end_state(key_rows, value_rows, log_decay):
    cumulative = jnp.cumsum(log_decay, axis=0)
    totals = cumulative[-1]
    weighted = key_rows * jnp.exp(totals - cumulative)
    return (jnp.exp(totals), jnp.einsum("nhd,nhe->hde", weighted, value_rows, precision=precise))


def combine(earlier, later):
    return (earlier[0] * later[0], later[0][..., None] * earlier[1] + later[1])


def blockwise(queries, key_rows, value_rows, log_decay, carried, block_len):
    length, head_count, _ = queries.shape
    value_width = value_rows.shape[-1]
    blocks = length // block_len

    def shaped(array):
        return array.reshape(blocks, block_len, head_count, array.shape[-1])

    triangle = jnp.tril(jnp.ones((block_len, block_len), jnp.float32))

    def advance(state_now, inputs):
        block_q, block_k, block_v, block_a = inputs
        cumulative = jnp.cumsum(block_a, axis=0)
        block_end = cumulative[-1]
        query_dec = block_q * jnp.exp(cumulative)
        scores = (
            jnp.einsum("ihd,jhd->hij", query_dec, block_k * jnp.exp(-cumulative), precision=precise)
            * triangle
        )
        result = jnp.einsum("hij,jhe->ihe", scores, block_v, precision=precise)
        result = result + jnp.einsum("ihd,hde->ihe", query_dec, state_now, precision=precise)
        state_next = state_now * jnp.exp(block_end)[:, :, None] + jnp.einsum(
            "jhd,jhe->hde", block_k * jnp.exp(block_end - cumulative), block_v, precision=precise
        )
        return (state_next, result)

    _, outputs = lax.scan(
        advance, carried, (shaped(queries), shaped(key_rows), shaped(value_rows), shaped(log_decay))
    )
    return outputs.reshape(length, head_count, value_width)


def head_channels(pieces, per_head, tp_index):
    for bit_number in range(per_head.bit_length() - 1):
        partner = from_partner(
            (for_sending(pieces[0]), for_sending(pieces[1]), for_sending(pieces[2])),
            "tp",
            bit_number,
        )
        upper = tp_index // (1 << bit_number) % 2 == 1
        pieces = tuple(
            (
                jnp.where(
                    upper,
                    jnp.concatenate([theirs, mine], axis=1),
                    jnp.concatenate([mine, theirs], axis=1),
                )
                for mine, theirs in zip(pieces, partner)
            )
        )
    return pieces


def context_totals(fwd_growth, fwd_state, bwd_growth, bwd_state, identity):

    def absorb(carried, piece):
        return (combine(carried, piece), None)

    total_fwd, _ = lax.scan(absorb, identity, (fwd_growth, fwd_state))
    total_bwd, _ = lax.scan(absorb, identity, (bwd_growth, bwd_state), reverse=True)
    return (total_fwd, total_bwd)


def stored(array):
    return lax.optimization_barrier(array.astype(jnp.bfloat16))


def local(
    latent,
    context,
    conditioning,
    context_prompt_vector,
    shift_matrix,
    scale_matrix,
    residual_gate_matrix,
    query_matrix,
    key_matrix,
    value_matrix,
    gate_matrix,
    decay_down_factor,
    decay_up_factor,
    decay_key_bias,
    spike_log_decay,
    output_gain,
    output_matrix,
):
    tp_count = lax.axis_size("tp")
    tp_index = lax.axis_index("tp")
    per_head = max(tp_count // HEADS, 1)
    heads_per_shard = max(HEADS // tp_count, 1)
    leading_head = tp_index // per_head * heads_per_shard
    tok_rows = latent.shape[0]
    conds = jax.nn.silu(
        jnp.stack([conditioning, context_prompt_vector]).astype(jnp.float32)
    ).astype(jnp.bfloat16)
    shifts, scales, gates = lax.psum(
        (
            linear(conds, shift_matrix),
            linear(conds, scale_matrix),
            linear(conds, residual_gate_matrix),
        ),
        "sp",
    )
    down_both = jnp.concatenate([decay_down_factor[0].T, decay_down_factor[1].T], axis=0)
    lat_weights = (query_matrix, key_matrix, value_matrix, gate_matrix, down_both)
    ctx_weights = (key_matrix, value_matrix, down_both)
    lat_f = latent.astype(jnp.float32)
    ctx_f = context.astype(jnp.float32)
    lat_sum, lat_squares, ctx_sum, ctx_squares = lax.psum(
        (
            jnp.sum(lat_f, axis=1, keepdims=True),
            jnp.sum(lat_f * lat_f, axis=1, keepdims=True),
            jnp.sum(ctx_f, axis=1, keepdims=True),
            jnp.sum(ctx_f * ctx_f, axis=1, keepdims=True),
        ),
        "tp",
    )
    latent_normalized = modulated(latent, lat_sum, lat_squares, shifts[0], scales[0])
    normed_ctx = modulated(context, ctx_sum, ctx_squares, shifts[1], scales[1])
    lat_piece = lax.all_gather(latent_normalized, "tp", axis=1, tiled=True)
    ctx_piece = lax.all_gather(normed_ctx, "tp", axis=1, tiled=True)
    lat_new = tuple((linear(lat_piece, weight) for weight in lat_weights))
    ctx_new = tuple((linear(ctx_piece, weight) for weight in ctx_weights))
    query_part, key_part, value_part, gate_part, low_rank_part = lat_new
    ctx_key_part, ctx_value_part, ctx_low = ctx_new
    query_full, key_full, ctx_key_full = head_channels(
        (stored(query_part), stored(key_part), stored(ctx_key_part)), per_head, tp_index
    )

    def split_heads(rows, width):
        return rows.astype(jnp.float32).reshape(rows.shape[0], heads_per_shard, width)

    value_cols = value_part.shape[1] // heads_per_shard
    queries = split_heads(query_full, DK) * DK ** (-0.5)
    key_rows = split_heads(key_full, DK)
    ctx_keys = split_heads(ctx_key_full, DK)
    values_lat = split_heads(stored(value_part), value_cols)
    values_ctx = split_heads(stored(ctx_value_part), value_cols)
    gate_rows = stored(gate_part).astype(jnp.float32)

    def per_head_decay(low_rows, direction):
        up_part = lax.dynamic_slice_in_dim(
            decay_up_factor[direction], leading_head * DK, heads_per_shard * DK, 1
        ).astype(jnp.float32)
        bias_part = lax.dynamic_slice_in_dim(
            decay_key_bias[direction], leading_head * DK, heads_per_shard * DK, 0
        )
        pre_act = jnp.dot(low_rows, up_part, precision=precise) + bias_part
        return (jax.nn.log_sigmoid(pre_act) / gate_norm).reshape(
            low_rows.shape[0], heads_per_shard, DK
        )

    decay_spikes = lax.dynamic_slice_in_dim(spike_log_decay, leading_head, heads_per_shard, 2)
    latent_forward = per_head_decay(low_rank_part[:, :DECAY_RANK], 0) + decay_spikes[0][:, :, None]
    latent_backward = per_head_decay(low_rank_part[:, DECAY_RANK:], 1) + decay_spikes[1][:, :, None]
    ctx_fwd = per_head_decay(ctx_low[:, :DECAY_RANK], 0)
    ctx_bwd = per_head_decay(ctx_low[:, DECAY_RANK:], 1)
    cf_growth, cf_state = end_state(ctx_keys, values_ctx, ctx_fwd)
    cb_growth, cb_state = end_state(
        reverse_rows(ctx_keys), reverse_rows(values_ctx), reverse_rows(ctx_bwd)
    )
    lf_growth, lf_state = end_state(key_rows, values_lat, latent_forward)
    lb_growth, lb_state = end_state(
        reverse_rows(key_rows), reverse_rows(values_lat), reverse_rows(latent_backward)
    )
    identity = (
        jnp.ones((heads_per_shard, DK), jnp.float32),
        jnp.zeros((heads_per_shard, DK, value_cols), jnp.float32),
    )
    ctx_gathered = (
        lax.all_gather(cf_growth[None].astype(jnp.bfloat16), "sp", axis=0, tiled=True).astype(
            jnp.float32
        ),
        lax.all_gather(cf_state[None].astype(jnp.bfloat16), "sp", axis=0, tiled=True).astype(
            jnp.float32
        ),
        lax.all_gather(cb_growth[None].astype(jnp.bfloat16), "sp", axis=0, tiled=True).astype(
            jnp.float32
        ),
        lax.all_gather(cb_state[None].astype(jnp.bfloat16), "sp", axis=0, tiled=True).astype(
            jnp.float32
        ),
    )
    total_fwd, total_bwd = context_totals(
        ctx_gathered[0], ctx_gathered[1], ctx_gathered[2], ctx_gathered[3], identity
    )
    prefix = carried_in((lf_growth, lf_state), "sp", combine, identity, False)
    suffix = carried_in((lb_growth, lb_state), "sp", combine, identity, True)
    start_fwd = combine(total_fwd, prefix)[1]
    start_bwd = combine(total_bwd, suffix)[1]
    zero_state = jnp.zeros((heads_per_shard, DK, value_cols), jnp.float32)

    def direction_out(query_rows, key_list, value_list, log_decay, start_state):
        local_part = blockwise(query_rows, key_list, value_list, log_decay, zero_state, BLK)
        reach = query_rows * jnp.exp(jnp.cumsum(log_decay, axis=0))
        return local_part + jnp.einsum("nhd,hde->nhe", reach, start_state, precision=precise)

    out_fwd = direction_out(queries, key_rows, values_lat, latent_forward, start_fwd)
    out_bwd = reverse_rows(
        direction_out(
            reverse_rows(queries),
            reverse_rows(key_rows),
            reverse_rows(values_lat),
            reverse_rows(latent_backward),
            start_bwd,
        )
    )
    grouped = (out_fwd + out_bwd).reshape(tok_rows, -1, VGROUP)
    grouped = grouped * lax.rsqrt(jnp.mean(grouped * grouped, axis=-1, keepdims=True) + epsilon)
    heads_out = (grouped.reshape(tok_rows, -1) * output_gain * jax.nn.silu(gate_rows)).astype(
        jnp.bfloat16
    )
    branch = linear(lax.all_gather(heads_out, "tp", axis=1, tiled=True), output_matrix)
    return (latent.astype(jnp.float32) + gates[0] * branch).astype(jnp.bfloat16)


def exact(a, b):
    return lax.dot_general(
        a, b, (((1,), (0,)), ((), ())), precision=precise, preferred_element_type=jnp.float32
    )


def nt(a, b):
    return lax.dot_general(a, b, (((1,), (1,)), ((), ())), preferred_element_type=jnp.float32)


def nn(a, b):
    return lax.dot_general(a, b, (((1,), (0,)), ((), ())), preferred_element_type=jnp.float32)


def tn(a, b):
    return lax.dot_general(a, b, (((0,), (0,)), ((), ())), preferred_element_type=jnp.float32)


def short(value):
    return value.astype(jnp.bfloat16)


H_CUTS = 2


def terms(value):
    first = short(value)
    rest = value - first.astype(jnp.float32)
    second = short(rest)
    return first, second, short(rest - second.astype(jnp.float32))


def log_sigmoid(pre):
    return (jnp.minimum(pre, 0.0) - jnp.log1p(jnp.exp(-jnp.abs(pre)))) / gate_norm


def triangle_of(size, upper):
    i = lax.broadcasted_iota(jnp.int32, (size, size), 0)
    j = lax.broadcasted_iota(jnp.int32, (size, size), 1)
    return (j >= i) if upper else (j <= i)


def layer_kernel(
    n,
    s,
    inner,
    rows,
    crows,
    feats,
    heads,
    dv,
    parts,
    hparts,
    latent,
    context,
    conditioning,
    prompt,
    shift_m,
    scale_m,
    gate_m,
    query_m,
    key_m,
    value_m,
    og_m,
    down,
    up,
    bias,
    spike,
    gain,
    out_m,
    out_ref,
    x_all,
    xn,
    acc,
    low_acc,
    mod_w,
    proj_w,
    out_w,
    down_v,
    up_v,
    bias_v,
    spike_v,
    gain_v,
    cond_v,
    mod_own,
    mod_recv,
    mod_all,
    gate_own,
    gate_recv,
    stat_all,
    spike_rows,
    proj,
    ctx_kv,
    ctx_low,
    tot_own,
    tot_recv,
    st_own,
    st_recv,
    local_out,
    ho_all,
    total_out,
    load_sem,
    x_send,
    x_recv,
    waves,
    *gather_sems,
):
    me = lax.axis_index("tp")
    sp = lax.axis_index("sp")
    hk = heads * DK
    hv = heads * dv
    model = n * feats
    both = rows + crows
    width = feats // parts
    hwidth = hv // hparts
    f32 = jnp.float32

    used = [0]

    def load(*pairs, whole):
        sem = load_sem.at[used[0]]
        used[0] += 1
        for src, dst in pairs:
            pltpu.make_async_copy(src, dst, sem).start()
        return pltpu.make_async_copy(whole, whole, sem)

    def own_piece(p):
        cols = pl.ds(p * width, width)
        return (
            (latent.at[:, cols], x_all.at[me * parts + p, pl.ds(0, rows)]),
            (context.at[:, cols], x_all.at[me * parts + p, pl.ds(rows, crows)]),
        )

    own_x = [load(*own_piece(0), whole=x_all.at[pl.ds(me * parts, 1)])]
    if parts > 1:
        own_x.append(
            load(
                *[c for p in range(1, parts) for c in own_piece(p)],
                whole=x_all.at[pl.ds(me * parts + 1, parts - 1)],
            )
        )
    first = [
        load((conditioning, cond_v.at[0]), (prompt, cond_v.at[1]), whole=cond_v),
        load((shift_m, mod_w.at[0]), (scale_m, mod_w.at[1]), whole=mod_w.at[pl.ds(0, 2)]),
    ]
    gate_load = load((gate_m, mod_w.at[2]), whole=mod_w.at[2])
    head_cols = pl.ds(pl.multiple_of(me * hk, hk), hk)
    small = [
        load((up.at[:, :, head_cols], up_v), whole=up_v),
        load((bias.at[:, head_cols], bias_v), whole=bias_v),
        load((spike, spike_v), whole=spike_v),
        load((gain, gain_v), whole=gain_v),
    ]
    weights = [
        load(
            (query_m, proj_w.at[pl.ds(0, hk)]),
            (key_m, proj_w.at[pl.ds(hk, hk)]),
            (value_m, proj_w.at[pl.ds(2 * hk, hv)]),
            (og_m, proj_w.at[pl.ds(2 * hk + hv, hv)]),
            whole=proj_w,
        ),
        load((down, down_v), whole=down_v),
    ]
    last = load((out_m, out_w), whole=out_w)

    line = n // inner
    z, y = lax.div(me, inner), lax.rem(me, inner)
    mate = z + 1 - 2 * lax.rem(z, 2)
    paired = inner > 1 and line % 2 == 0
    at_end = (z == 0) | (z == line - 1)

    def block_of(at, column):
        return at * inner + column

    barrier = pltpu.get_barrier_semaphore()

    def greet(**where):
        pl.semaphore_signal(barrier, inc=1, device_id=where, device_id_type=MESH)

    pl.when(z + 1 < line)(lambda: greet(tp=block_of(z + 1, y)))
    pl.when(z > 0)(lambda: greet(tp=block_of(z - 1, y)))
    if inner > 1:
        greet(tp=block_of(z, inner - 1 - y))
    for d in range(1, s):
        greet(sp=lax.rem(sp + d, s))
    beside = jnp.where(z > 0, 1, 0) + jnp.where(z + 1 < line, 1, 0)
    pl.semaphore_wait(barrier, beside + (inner - 1) + (s - 1))

    def pass_on(way):
        pl.semaphore_signal(
            waves.at[way],
            inc=1,
            device_id={"tp": block_of(z + 1 - 2 * way, y)},
            device_id_type=MESH,
        )

    def relay(way):
        pl.semaphore_wait(waves.at[way], 1)
        pass_on(way)

    if line > 1:
        pl.when(z == 0)(lambda: pass_on(0))
        pl.when(z == line - 1)(lambda: pass_on(1))

    started = []

    class Exchange:
        def __init__(self, axis, index, src, dst, landed, send_index=None, sent=True):
            at, count = (me, n) if axis == "tp" else (sp, s)
            self.some = count > 1

            def copy(source, target, d):
                return pltpu.make_async_remote_copy(
                    src_ref=source,
                    dst_ref=target,
                    send_sem=x_send.at[index if send_index is None else send_index],
                    recv_sem=x_recv.at[index],
                    device_id={axis: lax.rem(at + d, count)},
                    device_id_type=MESH,
                )

            for d in range(1, count):
                copy(src(d), dst(d), d).start()
            if self.some:
                self.all = copy(landed, landed, 1)
                if sent:
                    started.append(self.all)

        def wait_recv(self):
            if self.some:
                self.all.wait_recv()

    def level(i):
        table = []
        for at in range(line):
            order = [at]
            for k in range(1, line):
                order += [b for b in (at - k, at + k) if 0 <= b < line]
            table.append(order[i])
        return sum(jnp.where(z == at, table[at], 0) for at in range(line))

    class Gather:
        def __init__(self, ref, pieces, sems):
            self.ref, self.pieces = ref, pieces
            self.column_send, self.across_send, self.column_recv, self.across_recv = sems
            self.half = max(pieces // 2, 1)
            self.turned = tuple(range(pieces // 2, pieces)) if paired else ()

        def remote(self, ref, send_sem, recv_sem, target):
            return pltpu.make_async_remote_copy(
                src_ref=ref,
                dst_ref=ref,
                send_sem=send_sem,
                recv_sem=recv_sem,
                device_id={"tp": target},
                device_id_type=MESH,
            )

        def along(self, at, piece, to):
            return self.remote(
                self.ref.at[block_of(at, y) * self.pieces + piece],
                self.column_send.at[0],
                self.column_recv.at[lax.rem(at - to + line, line) - 1, piece],
                block_of(to, y),
            )

        def across(self, at, column, piece, target):
            return self.remote(
                self.ref.at[block_of(at, column) * self.pieces + piece],
                self.across_send.at[0],
                self.across_recv.at[at, piece // self.half],
                target,
            )

        def lane_sends(self, lane, k, piece, act):
            up = lane == "up"
            at, has = (z - k, z >= k) if up else (z + k, z + k < line)
            if k < line - 1:
                onward, to = (z + 1 < line, z + 1) if up else (z > 0, z - 1)
                pl.when(has & onward)(lambda: act(self.along(at, piece, to)))
            if inner > 1 and (k > 0 or up):
                if k == 1 and piece in self.turned:
                    has = has & (lax.rem(z, 2) == (0 if up else 1))
                pl.when(has)(
                    lambda: act(self.across(at, y, piece, block_of(z, inner - 1 - y)))
                )

        def start(self, piece):
            for lane in ("up", "down"):
                self.lane_sends(lane, 0, piece, lambda c: c.start())

        def take(self, lane, k, piece):
            at, has = (z - k, z >= k) if lane == "up" else (z + k, z + k < line)
            pl.when(has)(lambda: self.along(at, piece, z).wait_recv())
            self.lane_sends(lane, k, piece, lambda c: c.start())

        def near(self, k, piece):
            pl.when(z >= line // 2)(lambda: self.take("up", k, piece))
            pl.when(z < line // 2)(lambda: self.take("down", k, piece))

        def far(self, k, piece):
            pl.when(z < line // 2)(lambda: self.take("up", k, piece))
            pl.when(z >= line // 2)(lambda: self.take("down", k, piece))

        def side_start(self, when, piece):
            pl.when(when)(
                lambda: self.across(z, inner - 1 - y, piece, block_of(mate, y)).start()
            )

        def arrive(self, i, half):
            at = level(i)
            block = block_of(at, inner - 1 - y)
            self.remote(
                self.ref.at[pl.ds(block * self.pieces + half * self.half, self.half)],
                self.across_send.at[0],
                self.across_recv.at[at, half],
                block,
            ).wait_recv()

        def drain(self):
            def sent(count, sem):
                self.remote(
                    self.ref.at[pl.ds(0, count * self.pieces)],
                    sem.at[0],
                    self.across_recv.at[0, 0],
                    block_of(z, inner - 1 - y),
                ).wait_send()

            if line > 1:
                pl.when(at_end)(lambda: sent(1, self.column_send))
            if line > 2:
                pl.when(jnp.logical_not(at_end))(lambda: sent(line + 1, self.column_send))
            if inner > 1:
                sent(line, self.across_send)

    def run(events):
        for _, act in sorted(enumerate(events), key=lambda e: (e[1][0], e[0])):
            act[1]()

    xg = Gather(x_all, parts, gather_sems[:4])
    hg = Gather(ho_all, hparts * H_CUTS, gather_sems[4:])
    strip_rows = rows // H_CUTS

    for p in range(parts):
        if p < 2:
            own_x[p].wait()
        xg.start(p)
    if line > 2:
        pl.when((z > 0) & (z < line - 1))(lambda: relay(0))
        pl.when(z == line - 2)(lambda: relay(1))

    first[0].wait()

    def one_row(which):
        part = cond_v[which].astype(f32)
        return jnp.concatenate([part[r : r + 1] for r in range(part.shape[0])], axis=1)

    row_of = lax.broadcasted_iota(jnp.int32, (16, shift_m.shape[1]), 0)
    conds = jnp.where(row_of == 0, one_row(0), one_row(1))
    conds = short(conds * lax.logistic(conds))
    first[1].wait()
    for which in range(2):
        mod_own[2 * which : 2 * which + 2, :] = nt(conds, mod_w[which])[0:2]
    m1 = Exchange("sp", 0, lambda d: mod_own, lambda d: mod_recv.at[d - 1], mod_recv)

    ones = jnp.ones((16, width), jnp.bfloat16)
    row_sum = jnp.zeros((16, both), f32)
    row_squares = jnp.zeros((16, both), f32)
    for p in range(parts):
        own = x_all[me * parts + p]
        own_f = own.astype(f32)
        row_sum = row_sum + nt(ones, own)
        for part in terms(own_f * own_f):
            row_squares = row_squares + nt(ones, part)
    stat_all[me] = jnp.zeros(stat_all.shape[1:], f32)
    stat_all[me, 0:1, 0:both] = row_sum[0:1]
    stat_all[me, 1:2, 0:both] = row_squares[0:1]

    held = {}

    def send_stats():
        if line > 1:
            pl.when(z == line - 1)(lambda: pl.semaphore_wait(waves.at[0], 1))
            pl.when(z == 0)(lambda: pl.semaphore_wait(waves.at[1], 1))
        if line > 2:
            pl.when((z > 0) & (z < line - 2))(lambda: relay(1))
        held["sa"] = Exchange(
            "tp",
            3,
            lambda d: stat_all.at[me],
            lambda d: stat_all.at[me],
            stat_all.at[pl.ds(0, n - 1)],
        )

    def send_mods():
        m1.wait_recv()
        total = mod_own[...]
        for d in range(1, s):
            total = total + mod_recv[d - 1]
        mod_all[me] = total
        held["m2"] = Exchange(
            "tp",
            1,
            lambda d: mod_all.at[me],
            lambda d: mod_all.at[me],
            mod_all.at[pl.ds(0, n - 1)],
        )

    def send_gates():
        gate_load.wait()
        gate_own[...] = nt(conds, mod_w[2])[0:2]
        held["mg"] = Exchange(
            "sp", 2, lambda d: gate_own, lambda d: gate_recv.at[d - 1], gate_recv
        )

    def early():
        for copy in small:
            copy.wait()
        slot_head = lax.broadcasted_iota(jnp.int32, (spike_v.shape[1], hk), 0)
        lane_head = lax.broadcasted_iota(jnp.int32, (spike_v.shape[1], hk), 1) // DK
        pick = jnp.where(slot_head == me * heads + lane_head, 1.0, 0.0).astype(jnp.bfloat16)
        for e in range(2):
            spike_rows[:, e * hk : (e + 1) * hk] = sum(
                tn(part, pick) for part in terms(spike_v[e])
            )
        acc[...] = jnp.zeros(acc.shape, f32)
        low_acc[...] = jnp.zeros(low_acc.shape, f32)

    def moments():
        held["sa"].wait_recv()
        stats = sum(stat_all[b] for b in range(n))
        diagonal = lax.broadcasted_iota(jnp.int32, (both, both), 0) == lax.broadcasted_iota(
            jnp.int32, (both, both), 1
        )

        def column_of(row):
            return (
                jnp.sum(
                    jnp.where(diagonal, stats[row : row + 1, 0:both], 0.0), axis=1, keepdims=True
                )
                / model
            )

        mean = column_of(0)
        held["mean"] = mean
        held["spread"] = lax.rsqrt(column_of(1) - mean * mean + epsilon)

    def wait_mods():
        held["m2"].wait_recv()
        for copy in weights:
            copy.wait()

    tile = math.gcd(2 * hk + 2 * hv, 512)
    columns = acc.shape[1]

    def project_block(block):
        cols = pl.ds(pl.multiple_of(block * feats, feats), feats)
        mean, spread = held["mean"], held["spread"]
        mod = mod_all[block]
        for p in range(parts):
            lanes = slice(p * width, (p + 1) * width)
            x = (x_all[block * parts + p].astype(f32) - mean) * spread
            m = mod[:, lanes]
            xn[0:rows, lanes] = short(x[0:rows] * (1.0 + m[2:3]) + m[0:1])
            xn[rows:, lanes] = short(x[rows:] * (1.0 + m[3:4]) + m[1:2])
        low_acc[...] += nt(xn[...], down_v[:, cols])
        for t in range(columns // tile):
            out = slice(t * tile, (t + 1) * tile)
            acc[:, out] += nt(xn[...], proj_w[out, cols])

    def column_block(i):
        project_block(block_of(level(i), y))

    def other_block(i):
        if i > 0:
            for half in range(min(parts, 2)):
                xg.arrive(i, half)
        project_block(block_of(level(i), inner - 1 - y))

    unit, lag, cost = 0.79, 2.0, 0.6
    arrival = lambda k, p: unit * ((k - 1) * parts + p + 1) + lag
    mods_at = 9.4
    events = [
        (arrival(1, 0) - 0.1, send_stats),
        (arrival(1, parts // 2 - 1) + 0.01, send_mods),
        (arrival(1, parts // 2 - 1) + 0.02, send_gates),
        (arrival(1, parts - 1) + 0.05, early),
        (arrival(1, parts - 1) + 0.06, moments),
        (mods_at, wait_mods),
    ]
    for k in range(1, line):
        for p in range(parts):
            events.append((arrival(k, p), functools.partial(xg.take, "up", k, p)))
            events.append((arrival(k, p) + 0.005, functools.partial(xg.take, "down", k, p)))
    if inner > 1:
        for half in range(min(parts, 2)):
            when = arrival(1, (half + 1) * xg.half - 1)
            events.append((when + 0.03, functools.partial(xg.arrive, 0, half)))
        for p in xg.turned:
            when = arrival(1, parts - 1)
            events.append((when + 0.04, functools.partial(xg.side_start, at_end, p)))
            if line > 2:
                when = arrival(line - 2, parts - 1)
                events.append(
                    (
                        when + 0.01,
                        functools.partial(xg.side_start, jnp.logical_not(at_end), p),
                    )
                )
    tasks = []
    for i in range(line):
        ready = arrival(i, parts - 1) + 0.02 if i else 0.0
        tasks.append((ready, functools.partial(column_block, i)))
        if inner > 1:
            ready = arrival(max(i, 1), parts - 1) + 0.05 + (lag if i else 0)
            if i == 1 and xg.turned:
                ready = max(ready, arrival(line - 1, parts - 1) + unit * len(xg.turned))
            tasks.append((ready, functools.partial(other_block, i)))
    clock = mods_at + 0.01
    for ready, task in sorted(tasks, key=lambda t: t[0]):
        clock = max(clock, ready)
        events.append((clock, task))
        clock += cost
    run(events)
    proj[...] = short(acc[...])

    own_ctx = pl.ds(pl.multiple_of(sp * crows, crows), crows)
    ctx_kv[own_ctx, :] = proj[rows:, hk : 2 * hk + hv]
    ctx_low[own_ctx, :] = jnp.zeros((crows, ctx_low.shape[1]), jnp.bfloat16)
    for i, part in enumerate(terms(low_acc[rows:])):
        ctx_low[own_ctx, i * 2 * DECAY_RANK : (i + 1) * 2 * DECAY_RANK] = part
    lo = Exchange(
        "sp",
        5,
        lambda d: ctx_low.at[own_ctx],
        lambda d: ctx_low.at[own_ctx],
        ctx_low.at[pl.ds(0, (s - 1) * crows)],
    )
    mate_core = sp + 1 - 2 * lax.rem(sp, 2)
    opposite = lax.rem(sp + 2, s)
    even = lax.rem(sp, 2) == 0
    toward_mate = jnp.where(mate_core > sp, 0, 1)
    toward_opposite = jnp.where(opposite > sp, 0, 1)

    def push(src, dst, send_index, recv_index, target):
        return pltpu.make_async_remote_copy(
            src_ref=src,
            dst_ref=dst,
            send_sem=x_send.at[send_index],
            recv_sem=x_recv.at[recv_index],
            device_id={"sp": target},
            device_id_type=MESH,
        )

    def kv_rows(source):
        return ctx_kv.at[pl.ds(pl.multiple_of(source * crows, crows), crows)]

    push(kv_rows(sp), kv_rows(sp), 4, 4, opposite).start()
    push(kv_rows(sp), kv_rows(sp), 4, 15, mate_core).start()

    def pass_kv():
        push(kv_rows(opposite), kv_rows(opposite), 4, 4, opposite).wait_recv()
        push(kv_rows(opposite), kv_rows(opposite), 4, 15, mate_core).start()

    def wait_kv():
        rest = ctx_kv.at[pl.ds(0, 2 * crows)]
        push(rest, rest, 4, 15, mate_core).wait_recv()

    none = jnp.zeros((DECAY_RANK, hk), jnp.bfloat16)
    up_both = jnp.concatenate(
        [
            jnp.concatenate([up_v[0], none], axis=1),
            jnp.concatenate([none, up_v[1]], axis=1),
        ],
        axis=0,
    )
    bias_both = jnp.concatenate([bias_v[0:1], bias_v[1:2]], axis=1)

    def logs_of(parts_of_low):
        return log_sigmoid(sum(nn(part, up_both) for part in parts_of_low) + bias_both)

    def running(logs, length, e):
        lanes = slice(e * hk, (e + 1) * hk)
        mask = jnp.where(triangle_of(length, e == 1), 1.0, 0.0).astype(jnp.bfloat16)
        return sum(nn(mask, part) for part in terms(logs[:, lanes]))

    logs = logs_of(terms(low_acc[0:rows])) + spike_rows[...]
    cum = [running(logs, rows, e) for e in range(2)]
    whole = [cum[0][rows - 1 : rows], cum[1][0:1]]
    tot_own[0:1, :] = whole[0]
    tot_own[1:2, :] = whole[1]
    to = Exchange("sp", 6, lambda d: tot_own, lambda d: tot_recv.at[d - 1], tot_recv)

    keys = proj[0:rows, hk : 2 * hk].astype(f32)
    per = hparts // heads
    weighted = [short(keys * jnp.exp(whole[e] - cum[e])) for e in range(2)]
    for h in range(heads):
        for e in range(2):
            state = short(
                tn(
                    weighted[e][:, h * DK : (h + 1) * DK],
                    proj[0:rows, 2 * hk + h * dv : 2 * hk + (h + 1) * dv],
                )
            )
            for q in range(per):
                st_own[e, h * per + q] = state[:, q * hwidth : (q + 1) * hwidth]
        for q in range(h * per, (h + 1) * per):
            push(
                st_own.at[toward_opposite, q], st_recv.at[1, q], 7, 7 + q, opposite
            ).start()
            push(
                st_own.at[toward_mate, q],
                st_recv.at[jnp.where(even, 0, 2), q],
                7,
                11 + q,
                mate_core,
            ).start()

    def pass_state(q):
        mine = st_recv.at[1, q]
        push(mine, mine, 7, 7 + q, opposite).wait_recv()
        push(mine, st_recv.at[jnp.where(even, 2, 0), q], 7, 11 + q, mate_core).start()

    def wait_state(q):
        rest = st_recv.at[pl.ds(0, 2), q]
        push(rest, rest, 7, 11 + q, mate_core).wait_recv()

    queries = proj[0:rows, 0:hk].astype(f32) * DK ** (-0.5)
    blocks = rows // BLK

    def span(b):
        return slice(b * BLK, (b + 1) * BLK)

    inside = [[], []]
    for b in range(blocks):
        f = cum[0][span(b)]
        inside[0].append(f if b == 0 else f - cum[0][b * BLK - 1 : b * BLK])
        f = cum[1][span(b)]
        inside[1].append(
            f if b == blocks - 1 else f - cum[1][(b + 1) * BLK : (b + 1) * BLK + 1]
        )
    ends = [[part[BLK - 1 : BLK] for part in inside[0]], [part[0:1] for part in inside[1]]]
    q_dec = [[short(queries[span(b)] * jnp.exp(inside[e][b])) for b in range(blocks)] for e in range(2)]
    k_dec = [[short(keys[span(b)] * jnp.exp(-inside[e][b])) for b in range(blocks)] for e in range(2)]
    k_end = [
        [short(keys[span(b)] * jnp.exp(ends[e][b] - inside[e][b])) for b in range(blocks)]
        for e in range(2)
    ]
    lower, upper = triangle_of(BLK, False), triangle_of(BLK, True)
    scores = []
    for h in range(heads):
        ch = slice(h * DK, (h + 1) * DK)
        lines = []
        for b in range(blocks):
            strip = []
            for c in range(blocks):
                if b == c:
                    strip.append(
                        jnp.where(lower, nt(q_dec[0][b][:, ch], k_dec[0][b][:, ch]), 0.0)
                        + jnp.where(upper, nt(q_dec[1][b][:, ch], k_dec[1][b][:, ch]), 0.0)
                    )
                    continue
                e = 0 if c < b else 1
                near = q_dec[e][b][:, ch]
                between = range(c + 1, b) if c < b else range(b + 1, c)
                if len(between) > 0:
                    gap = sum(ends[e][m][:, ch] for m in between)
                    near = short(queries[span(b)][:, ch] * jnp.exp(inside[e][b][:, ch] + gap))
                strip.append(nt(near, k_end[e][c][:, ch]))
            lines.append(jnp.concatenate(strip, axis=1) if blocks > 1 else strip[0])
        scores.append(short(jnp.concatenate(lines, axis=0) if blocks > 1 else lines[0]))

    lo.wait_recv()
    pass_kv()
    low_parts = [
        ctx_low[:, i * 2 * DECAY_RANK : (i + 1) * 2 * DECAY_RANK] for i in range(3)
    ]
    ctx_logs = logs_of(low_parts)
    length = s * crows
    ctx_decay = []
    for e in range(2):
        c = running(ctx_logs, length, e)
        end = c[length - 1 : length] if e == 0 else c[0:1]
        ctx_decay.append(jnp.exp(end - c))

    to.wait_recv()
    places = {d: lax.rem(sp - d + s, s) for d in range(1, s)}

    def passed(low_end, high_end, direction):
        result = jnp.zeros((1, hk), f32)
        for d in range(1, s):
            inside_it = jnp.where((places[d] > low_end) & (places[d] < high_end), 1.0, 0.0)
            result = result + inside_it * tot_recv[d - 1][direction : direction + 1]
        return result

    ctx_reach = [
        short(queries * jnp.exp(cum[0] + passed(-1, sp, 0))),
        short(queries * jnp.exp(cum[1] + passed(sp, s, 1))),
    ]
    reach = []
    for d in range(1, s):
        p = places[d]
        before = jnp.where(p < sp, 1.0, 0.0)
        exponent = before * (cum[0] + passed(p, sp, 0)) + (1.0 - before) * (
            cum[1] + passed(sp, p, 1)
        )
        reach.append(short(queries * jnp.exp(exponent)))
    gate_rows = proj[0:rows, 2 * hk + hv :].astype(f32)
    small_gate = gate_rows * lax.logistic(gate_rows) * gain_v[...]

    pass_state(0)
    wait_kv()
    ctx_keys = ctx_kv[:, 0:hk].astype(f32)
    ctx_weighted = [short(ctx_keys * part) for part in ctx_decay]
    ctx_states = [
        [
            short(tn(w[:, h * DK : (h + 1) * DK], ctx_kv[:, hk + h * dv : hk + (h + 1) * dv]))
            for w in ctx_weighted
        ]
        for h in range(heads)
    ]
    for h in range(heads):
        ch = slice(h * DK, (h + 1) * DK)
        vc = slice(h * dv, (h + 1) * dv)
        local_out[:, vc] = nn(
            jnp.concatenate([scores[h]] + [r[:, ch] for r in ctx_reach], axis=1),
            jnp.concatenate(
                [proj[0:rows, 2 * hk + h * dv : 2 * hk + (h + 1) * dv]]
                + ctx_states[h],
                axis=0,
            ),
        )
    gi = lax.broadcasted_iota(jnp.int32, (hwidth, hwidth), 0) // VGROUP
    gj = lax.broadcasted_iota(jnp.int32, (hwidth, hwidth), 1) // VGROUP
    group = jnp.where(gi == gj, 1.0, 0.0).astype(jnp.bfloat16)

    def head_piece(q):
        h = q // per
        ch = slice(h * DK, (h + 1) * DK)
        vc = slice(q * hwidth, (q + 1) * hwidth)
        if q + 1 < hparts:
            pass_state(q + 1)
        wait_state(q)
        o = local_out[:, vc] + nn(
            jnp.concatenate([r[:, ch] for r in reach], axis=1),
            jnp.concatenate([st_recv[d - 1, q] for d in range(1, s)], axis=0),
        )
        squares = o * o
        top = short(squares)
        rest = short(squares - top.astype(f32))
        power = (nn(top, group) + nn(rest, group)) * (1.0 / VGROUP)
        result = short(o * lax.rsqrt(power + epsilon) * small_gate[:, vc])
        for r in range(H_CUTS):
            p = q * H_CUTS + r
            ho_all[me * hg.pieces + p] = result[r * strip_rows : (r + 1) * strip_rows]
            hg.start(p)

    def ready_out():
        last.wait()
        held["mg"].wait_recv()
        total_out[...] = jnp.zeros(total_out.shape, f32)

    def add_half(block, half):
        cols = pl.ds(pl.multiple_of(block * feats + half * 2 * hwidth, 2 * hwidth), 2 * hwidth)
        first_piece = block * hg.pieces + 2 * half * H_CUTS
        pair = jnp.concatenate(
            [
                jnp.concatenate(
                    [ho_all[first_piece + r], ho_all[first_piece + H_CUTS + r]], axis=1
                )
                for r in range(H_CUTS)
            ],
            axis=0,
        )
        total_out[...] += nt(pair, out_w[:, cols])

    def add_column(i, half):
        add_half(block_of(level(i), y), half)

    def add_other(i, half):
        if i > 0:
            hg.arrive(i, half)
        add_half(block_of(level(i), inner - 1 - y), half)

    hop_h = 2.6
    here = lambda k, q: 0.4 * q + 0.4 * (q // 2) + hop_h * k
    events = [(here(0, 1) + 0.01, ready_out)]
    for q in range(hparts):
        events.append((here(0, q), functools.partial(head_piece, q)))
        for r in range(H_CUTS):
            p = q * H_CUTS + r
            for k in range(1, line):
                events.append((here(k, q) + 0.01 * r, functools.partial(hg.near, k, p)))
                if 2 * k < line + line % 2:
                    when = here(k, q) + 0.5 + 0.01 * r
                    events.append((when, functools.partial(hg.far, k, p)))
            if p in hg.turned:
                when = here(1, hparts - 1) + 0.03
                events.append((when, functools.partial(hg.side_start, at_end, p)))
                if line > 2:
                    when = here(line - 2, hparts - 1) + 0.03
                    events.append(
                        (when, functools.partial(hg.side_start, jnp.logical_not(at_end), p))
                    )
    if inner > 1:
        for half in range(2):
            when = here(1, (half + 1) * hparts // 2 - 1) + 0.02
            events.append((when, functools.partial(hg.arrive, 0, half)))
    for i in range(line):
        for half in range(hparts // 2):
            when = here(i, 2 * half + 1) + 0.6
            events.append((when, functools.partial(add_column, i, half)))
            if inner > 1:
                when += hop_h + 0.1
                if i == 1 and 2 * half * H_CUTS in hg.turned:
                    when = max(when, here(line - 1, 2 * half + 1) + 0.4)
                events.append((when, functools.partial(add_other, i, half)))
    run(events)
    gates = gate_own[0:1]
    for d in range(1, s):
        gates = gates + gate_recv[d - 1, 0:1]
    for p in range(parts):
        lanes = slice(p * width, (p + 1) * width)
        out_ref[:, lanes] = short(
            x_all[me * parts + p, 0:rows].astype(f32) + gates[:, lanes] * total_out[:, lanes]
        )
    for copy in started:
        copy.wait_send()
    push(st_recv, st_recv, 7, 7, opposite).wait_send()
    sent_kv = ctx_kv.at[pl.ds(0, (s - 1) * crows)]
    push(sent_kv, sent_kv, 4, 4, opposite).wait_send()
    xg.drain()
    hg.drain()


def one_kernel(
    latent,
    context,
    conditioning,
    context_prompt_vector,
    shift_matrix,
    scale_matrix,
    residual_gate_matrix,
    query_matrix,
    key_matrix,
    value_matrix,
    gate_matrix,
    decay_down_factor,
    decay_up_factor,
    decay_key_bias,
    spike_log_decay,
    output_gain,
    output_matrix,
):
    n, s = lax.axis_size("tp"), lax.axis_size("sp")
    rows, feats = latent.shape
    crows = context.shape[0]
    heads = HEADS // n
    hk, hv = query_matrix.shape[0], value_matrix.shape[0]
    dv = hv // heads
    model = n * feats
    both = rows + crows
    inputs = conditioning.shape[0]
    parts = feats // 128
    hparts = hv // 128
    stat_width = -(-both // 128) * 128
    bf, f32 = jnp.bfloat16, jnp.float32
    vmem, dma = pltpu.VMEM, pltpu.SemaphoreType.DMA
    scratch = [
        vmem((n * parts, both, 128), bf),
        vmem((both, feats), bf),
        vmem((both, 2 * hk + 2 * hv), f32),
        vmem((both, 2 * DECAY_RANK), f32),
        vmem((3, feats, inputs), bf),
        vmem((2 * hk + 2 * hv, model), bf),
        vmem((output_matrix.shape[0], model), bf),
        vmem((2 * DECAY_RANK, model), bf),
        vmem((2, DECAY_RANK, hk), bf),
        vmem((2, hk), f32),
        vmem((2, HEADS, rows), f32),
        vmem((1, hv), f32),
        vmem((2, inputs // 128, 128), bf),
        vmem((4, feats), f32),
        vmem((s - 1, 4, feats), f32),
        vmem((n, 4, feats), f32),
        vmem((2, feats), f32),
        vmem((s - 1, 2, feats), f32),
        vmem((n, 2, stat_width), f32),
        vmem((rows, 2 * hk), f32),
        vmem((both, 2 * hk + 2 * hv), bf),
        vmem((s * crows, hk + hv), bf),
        vmem((s * crows, 128), bf),
        vmem((2, hk), f32),
        vmem((s - 1, 2, hk), f32),
        vmem((2, hparts, DK, 128), bf),
        vmem((s - 1, hparts, DK, 128), bf),
        vmem((rows, hv), f32),
        vmem((n * hparts * H_CUTS, rows // H_CUTS, 128), bf),
        vmem((rows, feats), f32),
        dma((12,)),
        dma((8,)),
        dma((8 + 2 * hparts,)),
        pltpu.SemaphoreType.REGULAR((2,)),
    ]
    inner = 2 if n % 2 == 0 else 1
    line = n // inner
    hops = max(line - 1, 1)
    for pieces in (parts, hparts * H_CUTS):
        scratch += [dma((1,)), dma((1,)), dma((hops, pieces)), dma((line, min(pieces, 2)))]
    return pl.pallas_call(
        functools.partial(
            layer_kernel, n, s, inner, rows, crows, feats, heads, dv, parts, hparts
        ),
        out_shape=pltpu.VMEM((rows, feats), bf),
        in_specs=[pl.BlockSpec(memory_space=pl.ANY)] * 17,
        out_specs=pl.BlockSpec(memory_space=pltpu.VMEM),
        scratch_shapes=scratch,
        compiler_params=pltpu.CompilerParams(
            collective_id=0, has_side_effects=True, vmem_limit_bytes=60 * 1024 * 1024
        ),
        name="layer",
    )(
        latent,
        context,
        conditioning.reshape(-1, 128),
        context_prompt_vector.reshape(-1, 128),
        shift_matrix,
        scale_matrix,
        residual_gate_matrix,
        query_matrix,
        key_matrix,
        value_matrix,
        gate_matrix,
        jnp.swapaxes(decay_down_factor, 1, 2).reshape(2 * DECAY_RANK, model),
        decay_up_factor,
        decay_key_bias,
        jnp.swapaxes(spike_log_decay, 1, 2),
        output_gain.reshape(1, -1),
        output_matrix,
    )


def solution(mesh):
    placed = (
        P("sp", "tp"),
        P("sp", "tp"),
        P("sp"),
        P("sp"),
        P("tp", "sp"),
        P("tp", "sp"),
        P("tp", "sp"),
        P("tp", None),
        P("tp", None),
        P("tp", None),
        P("tp", None),
        P(),
        P(),
        P(),
        P(None, "sp", None),
        P("tp"),
        P("tp", None),
    )
    whole_heads = HEADS == 2 * mesh.shape["tp"] and mesh.shape["sp"] == 4
    return jax.shard_map(
        one_kernel if whole_heads else local, mesh=mesh, in_specs=placed, out_specs=P("sp", "tp"), check_vma=False
    )
```
